128 devices in a mesh: sp: 64 (over z, y, x), tp: 2 (over core).
Axes of the slice: x: 4, y: 4, z: 4, core: 2. Of those that a mesh axis runs over, the one named last changes fastest.
Arguments:
- projected_queries: bfloat16 [32768, 1024], P('sp', 'tp'), may hold values from -6 to 6
- projected_keys: bfloat16 [32768, 1024], P('sp', 'tp'), may hold values from -6 to 6
- projected_values: bfloat16 [32768, 1024], P('sp', 'tp'), may hold values from -6 to 6
- output_gate_values: bfloat16 [32768, 1024], P('sp', 'tp'), may hold values from -6 to 6
- write_strength_logits: bfloat16 [32768, 8], P('sp', 'tp'), may hold values from -6.5 to 3
- decay_input_logits: bfloat16 [32768, 8], P('sp', 'tp'), may hold values from -5 to 5
- head_rate_logarithm: float32 [8], P('tp'), may hold values from -8 to 2.3
- extra_log_decay: float32 [32768, 8], P('sp', 'tp'), may hold values from -0.7 to 0
- per_head_norm_gain: float32 [128], replicated, may hold values from 0.1 to 1.9
- output_matrix: bfloat16 [1024, 2048], replicated, may hold values from -0.1875 to 0.1875
- residual: bfloat16 [32768, 2048], P(('sp', 'tp')), may hold values from -6 to 6
- mixture_norm_gain: float32 [2048], replicated, may hold values from 0.1 to 1.9
- selected_expert_index: int32 [32768, 4], P(('sp', 'tp')), may hold values from 0 to 127, all different within a row; in each aligned block of 256 rows (0 to 255, 256 to 511, ...) at most 12 rows name the same one
- routing_weight: float32 [32768, 4], P(('sp', 'tp')), may hold values from 0.1 to 0.9
- routed_gate_weight: bfloat16 [128, 2048, 512], P(('sp', 'tp')), may hold values from -0.125 to 0.125
- routed_up_weight: bfloat16 [128, 2048, 512], P(('sp', 'tp')), may hold values from -0.125 to 0.125
- routed_down_weight: bfloat16 [128, 512, 2048], P(('sp', 'tp')), may hold values from -0.25 to 0.25
- common_gate_weight: bfloat16 [2048, 512], replicated, may hold values from -0.125 to 0.125
- common_up_weight: bfloat16 [2048, 512], replicated, may hold values from -0.125 to 0.125
- common_down_weight: bfloat16 [512, 2048], replicated, may hold values from -0.25 to 0.25
Outputs:
- block_out: bfloat16 [32768, 2048], P(('sp', 'tp'))
The draws below stay inside these ranges and needn't reach their ends.
Inputs may be any that keep to these rules, and one draw needn't show every extreme that they name: `selected_expert_index`: each row names 4 different experts. Among the rows that one device holds, no expert is named more than 12 times.
All inputs are finite; a program needn't handle non-finite values.
Results may differ from the reference program's by a relative error of at most 0.008.
Values may be sent and summed in bfloat16 or wider, within the bound.
A program may use at most 192 MiB of HBM per device.

```python
import math
import jax
import jax.numpy as jnp
import numpy as np
from jax import lax

D = 2048
HEADS = 8
HD = 128
EFF = 512
SFF = 512
TOP_K = 4
SPAN = 64
TOK_DEV = 512
TOKENS = 32768
EXPERTS = 128
CAP = 12
N_SP = 64
N_TP = 2


def head_order(key):
    return jax.random.permutation(jax.random.fold_in(key, 11), HEADS)


def draw_head_rate_logarithm(key, part):
    order = head_order(key)
    jitter = jax.random.uniform(jax.random.fold_in(key, 12), (HEADS,), jnp.float32, -0.4, 0.4)
    fast = order < HEADS // 2
    slow_level = math.log(244.0 / TOKENS)
    return jnp.where(fast, 1.8, slow_level).astype(jnp.float32) + jitter


def draw_write_strength_logits(key, part):
    order = head_order(key)
    fast = order < HEADS // 2
    blocks = TOKENS // TOK_DEV
    level = jax.random.uniform(jax.random.fold_in(key, 41), (blocks, 1, HEADS), jnp.float32, -5.5, -4.5)
    jiggle = jax.random.uniform(jax.random.fold_in(key, 42), (blocks, TOK_DEV, HEADS), jnp.float32, -1.0, 1.0)
    wide = jax.random.uniform(jax.random.fold_in(key, 43), (blocks, TOK_DEV, HEADS), jnp.float32, -3.0, 3.0)
    picked = jnp.where(fast[None, None, :], wide, level + jiggle)
    return picked.reshape(TOKENS, HEADS).astype(jnp.bfloat16)


def draw_decay_input_logits(key, part):
    shifts = jax.random.uniform(jax.random.fold_in(key, 21), (TOKENS // TOK_DEV, 1, HEADS), jnp.float32, -0.8, 0.8)
    noise = jnp.clip(jax.random.normal(jax.random.fold_in(key, 22), (TOKENS // TOK_DEV, TOK_DEV, HEADS), jnp.float32), -3.5, 3.5)
    return (noise + shifts).reshape(TOKENS, HEADS).astype(jnp.bfloat16)


def draw_extra_log_decay(key, part):
    chance = jax.random.uniform(jax.random.fold_in(key, 31), (TOKENS, HEADS), jnp.float32)
    depth = jax.random.uniform(jax.random.fold_in(key, 32), (TOKENS, HEADS), jnp.float32, 0.22, 0.69)
    return jnp.where(chance < 6.0 / TOKENS, -depth, 0.0).astype(jnp.float32)


def steps_of(stream_key, dims, shards, low, largest):
    def one(dim, blocks):
        draws = jax.random.uniform(jax.random.fold_in(jax.random.fold_in(stream_key, 6), dim), (blocks,), jnp.float32, low / len(shards), largest / len(shards))
        return jnp.repeat(jnp.exp(draws), dims[dim] // blocks).reshape((-1,) + (1,) * (len(dims) - dim - 1))

    level = one(*shards[0])
    for cut in shards[1:]:
        level = level * one(*cut)
    return level


def routed_block(own_key, own, number, rows, count, top, most, slope):
    sequence = jax.random.permutation(own_key, count)
    crowded, ordinary = shares(count, rows * top, most, slope, True), shares(count, rows * top, most, slope, False)
    places = jnp.arange(count)

    def named(lengths, rotation):
        used = int((lengths > 0).sum())
        fixed = max(1, used // 4)
        shifted = fixed + (places - fixed + rotation * (used - fixed)) % max(1, count - fixed)
        return jnp.zeros((count,), jnp.int32).at[sequence[jnp.where(places < fixed, places, shifted)]].set(jnp.asarray(lengths, jnp.int32))

    lengths = jnp.where(number % 4 == 0, named(crowded, number // 4), named(ordinary, number - number // 4 - 1))
    mixed = jax.random.permutation(jax.random.fold_in(own, 3), count)
    giver, taker = mixed[0:count // 2 * 2:2], mixed[1:count // 2 * 2:2]
    slack = jnp.minimum(lengths[giver] - 1, most - lengths[taker]) // 2
    slack = jnp.where((giver == sequence[0]) | (taker == sequence[0]) | (lengths[taker] == 0), 0, jnp.maximum(slack, 0))
    shifted = jax.random.randint(jax.random.fold_in(own, 4), (count // 2,), 0, 1 << 20) % (slack + 1)
    lengths = lengths.at[giver].add(-shifted).at[taker].add(shifted)
    items = jnp.searchsorted(jnp.cumsum(lengths), jnp.arange(rows * top), side="right").astype(jnp.int32)
    grid = items.reshape(top, rows).T
    grid = grid[jax.random.permutation(jax.random.fold_in(own, 1), rows)]
    rotation = jax.random.randint(jax.random.fold_in(own, 2), (rows, 1), 0, top)
    return jnp.take_along_axis(grid, (jnp.arange(top)[None, :] + rotation) % top, axis=1)


def shares(number_of, total, most, lean, full):
    loads = [(1 << 20) // math.isqrt(grade ** lean) + 1 for grade in range(1, number_of + 1)]
    largest = most if full else min(most, max(-(-total // number_of), total * loads[0] // sum(loads)))
    least = 1 if total - largest >= number_of - 1 else 0
    holding, surplus = [largest] + [least] * (number_of - 1), total - largest - least * (number_of - 1)
    while surplus > 0:
        free = [i for i in range(1, number_of) if holding[i] < largest] or [i for i in range(1, number_of) if holding[i] < most]
        whole, remaining = sum([loads[i] for i in free]), surplus
        for i in free:
            addition = min(most - holding[i], max(1, remaining * loads[i] // whole), surplus)
            holding[i] = holding[i] + addition
            surplus = surplus - addition
    return np.array(holding)


def gaussian(stream_key, shape, scale, most, pieces=(), kind=jnp.bfloat16):
    values = jax.random.normal(stream_key, shape, jnp.float32) * scale
    if len(pieces) > 0:
        values = steps_of(stream_key, shape, pieces, -0.22, 0.18) * values
    return jnp.clip(values, min=-most, max=most).astype(kind)


def setup_inputs(seed: int = 0) -> dict:
    splits = jax.random.split(jax.random.key(seed), 21)
    projected_queries = gaussian(splits[0], (TOKENS, HEADS * HD), 1.0, 6.0, ((0, 64), (1, 2)))
    projected_keys = gaussian(splits[1], (TOKENS, HEADS * HD), 1.0, 6.0, ((0, 64), (1, 2)))
    projected_values = gaussian(splits[2], (TOKENS, HEADS * HD), 1.0, 6.0, ((0, 64), (1, 2)))
    output_gate_values = gaussian(splits[3], (TOKENS, HEADS * HD), 1.0, 6.0, ((0, 64), (1, 2)))
    write_strength_logits = draw_write_strength_logits(jax.random.fold_in(splits[20], 71), 0)
    decay_input_logits = draw_decay_input_logits(jax.random.fold_in(splits[20], 71), 0)
    head_rate_logarithm = draw_head_rate_logarithm(jax.random.fold_in(splits[20], 71), 0)
    extra_log_decay = draw_extra_log_decay(jax.random.fold_in(splits[20], 71), 0)
    per_head_norm_gain = jnp.clip(1.0 + 0.18 * jax.random.normal(splits[8], (HD,), jnp.float32), 0.1, 1.9)
    output_matrix = gaussian(splits[9], (HEADS * HD, D), (HEADS * HD) ** -0.5, 0.1875)
    residual = gaussian(splits[10], (TOKENS, D), 1.0, 6.0, ((0, 128),))
    mixture_norm_gain = jnp.clip(1.0 + 0.18 * jax.random.normal(splits[11], (D,), jnp.float32), 0.1, 1.9)
    selected_expert_index_keys = jax.random.split(jax.random.fold_in(splits[12], 1), TOKENS // (TOK_DEV // N_TP))
    selected_expert_index_turns = jax.random.permutation(jax.random.fold_in(splits[12], 3), TOKENS // (TOK_DEV // N_TP))
    selected_expert_index = jax.vmap(lambda own, number: routed_block(jax.random.fold_in(splits[12], 2), own, number, TOK_DEV // N_TP, EXPERTS, TOP_K, CAP, 1))(selected_expert_index_keys, selected_expert_index_turns).reshape((TOKENS, TOP_K))
    routing_weight = jnp.clip(0.1 + 0.79999997 * jax.random.uniform(splits[13], (TOKENS, TOP_K), jnp.float32) ** steps_of(splits[13], (TOKENS, TOP_K), ((0, 128),), -0.2, 0.2), 0.1, 0.9)
    routed_gate_weight = gaussian(splits[14], (EXPERTS, D, EFF), D ** -0.5, 0.125, ((0, 128),))
    routed_up_weight = gaussian(splits[15], (EXPERTS, D, EFF), D ** -0.5, 0.125, ((0, 128),))
    routed_down_weight = gaussian(splits[16], (EXPERTS, EFF, D), EFF ** -0.5, 0.25, ((0, 128),))
    common_gate_weight = gaussian(splits[17], (D, SFF), D ** -0.5, 0.125)
    common_up_weight = gaussian(splits[18], (D, SFF), D ** -0.5, 0.125)
    common_down_weight = gaussian(splits[19], (SFF, D), SFF ** -0.5, 0.25)
    return dict(projected_queries=projected_queries, projected_keys=projected_keys, projected_values=projected_values, output_gate_values=output_gate_values, write_strength_logits=write_strength_logits, decay_input_logits=decay_input_logits, head_rate_logarithm=head_rate_logarithm, extra_log_decay=extra_log_decay, per_head_norm_gain=per_head_norm_gain, output_matrix=output_matrix, residual=residual, mixture_norm_gain=mixture_norm_gain, selected_expert_index=selected_expert_index, routing_weight=routing_weight, routed_gate_weight=routed_gate_weight, routed_up_weight=routed_up_weight, routed_down_weight=routed_down_weight, common_gate_weight=common_gate_weight, common_up_weight=common_up_weight, common_down_weight=common_down_weight)


EPS = 1e-06
HIGH = lax.Precision.HIGHEST

def unit_heads(raw, heads):
    active = jax.nn.silu(raw.astype(jnp.float32)).reshape(raw.shape[0], heads, -1)
    return active * lax.rsqrt(lax.optimization_barrier(jnp.sum(active * active, axis=-1, keepdims=True)) + EPS)

def prepare_inputs(projected_queries, projected_keys, projected_values, write_strength_logits, decay_input_logits, head_rate_logarithm, extra_log_decay):
    heads = head_rate_logarithm.shape[0]
    queries = unit_heads(projected_queries, heads)
    keys = unit_heads(projected_keys, heads)
    values = jax.nn.silu(projected_values.astype(jnp.float32)).reshape(projected_values.shape[0], heads, -1)
    beta = jax.nn.sigmoid(write_strength_logits.astype(jnp.float32))
    decay_logarithm = extra_log_decay - jnp.exp(head_rate_logarithm)[None, :] * jax.nn.softplus(decay_input_logits.astype(jnp.float32) - 6.0)
    return (queries, keys, values, beta, decay_logarithm)

def block_terms(queries, keys, values, beta, decay_logarithm):
    length, heads, width = queries.shape
    number = length // SPAN

    def split(array):
        return jnp.moveaxis(array.reshape(number, SPAN, heads, -1), 2, 0)
    q_blocks = split(queries)
    k_blocks = split(keys)
    v_blocks = split(values)
    b_blocks = split(beta[..., None])[..., 0]
    g_cumul = jnp.cumsum(split(decay_logarithm[..., None])[..., 0], axis=-1)
    place = jnp.arange(SPAN)
    causal = place[:, None] >= place[None, :]
    strict = place[:, None] > place[None, :]
    spread = jnp.where(causal, g_cumul[..., :, None] - g_cumul[..., None, :], 0.0)
    decay = jnp.where(causal, jnp.exp(spread), 0.0)
    k_beta = k_blocks * b_blocks[..., None]
    inner = jnp.einsum('hncd,hnsd->hncs', k_beta, k_blocks, precision=HIGH)
    lower = jnp.where(strict, inner * decay, 0.0) + jnp.eye(SPAN, dtype=jnp.float32)
    right = jnp.concatenate([v_blocks * b_blocks[..., None], k_beta * jnp.exp(g_cumul)[..., None]], axis=-1)
    solved = jax.scipy.linalg.solve_triangular(lower, right, lower=True, unit_diagonal=True)
    u_part = solved[..., :width]
    w_part = solved[..., width:]
    scores = jnp.einsum('hncd,hnsd->hncs', q_blocks, k_blocks, precision=HIGH) * decay
    q_decayed = q_blocks * jnp.exp(g_cumul)[..., None]
    log_last = g_cumul[..., -1]
    k_decayed = k_blocks * jnp.exp(log_last[..., None] - g_cumul)[..., None]
    return (q_decayed, scores, u_part, w_part, k_decayed, log_last)

def run_blocks(terms, start):

    def advance(state, items):
        q_one, s_one, u_one, w_one, k_one, log_one = items
        fresh = u_one - jnp.einsum('hcd,hde->hce', w_one, state, precision=HIGH)
        result = jnp.einsum('hcd,hde->hce', q_one, state, precision=HIGH)
        result = result + jnp.einsum('hcs,hse->hce', s_one, fresh, precision=HIGH)
        state = state * jnp.exp(log_one)[:, None, None] + jnp.einsum('hcd,hce->hde', k_one, fresh, precision=HIGH)
        return (state, result)
    items = tuple((jnp.moveaxis(array, 1, 0) for array in terms))
    _, results = lax.scan(advance, start, items)
    number, heads, span, width = results.shape
    return results.transpose(0, 2, 1, 3).reshape(number * span, heads, width)

def finish(head_mix, output_gate_values, per_head_norm_gain):
    length, heads, width = head_mix.shape
    scaled = head_mix * lax.rsqrt(lax.optimization_barrier(jnp.mean(head_mix * head_mix, axis=-1, keepdims=True)) + EPS)
    gated = scaled * per_head_norm_gain * jax.nn.silu(output_gate_values.astype(jnp.float32).reshape(length, heads, width))
    return gated.reshape(length, heads * width).astype(jnp.bfloat16)

def normalize(stream, gain):
    wide = stream.astype(jnp.float32)
    return (wide * lax.rsqrt(lax.optimization_barrier(jnp.mean(wide * wide, axis=-1, keepdims=True)) + EPS) * gain).astype(jnp.bfloat16)

def feed_forward(rows, w_gate, w_up, w_down):
    hidden = jax.nn.silu(jnp.dot(rows.astype(jnp.float32), w_gate.astype(jnp.float32), preferred_element_type=jnp.float32))
    hidden = (hidden * jnp.dot(rows.astype(jnp.float32), w_up.astype(jnp.float32), preferred_element_type=jnp.float32)).astype(jnp.bfloat16)
    return jnp.dot(hidden.astype(jnp.float32), w_down.astype(jnp.float32), preferred_element_type=jnp.float32)

def routed_sum(normed, selected_expert_index, routing_weight, routed_gate_weight, routed_up_weight, routed_down_weight):
    length = normed.shape[0]
    room = N_SP * N_TP * CAP
    flat_ids = selected_expert_index.reshape(-1)
    flat_rows = (jnp.arange(flat_ids.shape[0]) // TOP_K).astype(jnp.int32)
    flat_weight = routing_weight.reshape(-1)

    def one_expert(total, items):
        w_gate, w_up, w_down, expert = items
        chosen = flat_ids == expert
        slot = (jnp.cumsum(chosen.astype(jnp.int32)) - 1).astype(jnp.int32)
        target = jnp.where(chosen, slot, room).astype(jnp.int32)
        source = jnp.zeros((room,), jnp.int32).at[target].set(flat_rows, mode='drop')
        weight = jnp.zeros((room,), jnp.float32).at[target].set(flat_weight, mode='drop')
        result = feed_forward(normed[source], w_gate, w_up, w_down).astype(jnp.bfloat16)
        return (total.at[source].add(result.astype(jnp.float32) * weight[:, None]), None)
    experts_all = jnp.arange(EXPERTS).astype(jnp.int32)
    total, _ = lax.scan(one_expert, jnp.zeros((length, D), jnp.float32), (routed_gate_weight, routed_up_weight, routed_down_weight, experts_all))
    return total

def reference(projected_queries, projected_keys, projected_values, output_gate_values, write_strength_logits, decay_input_logits, head_rate_logarithm, extra_log_decay, per_head_norm_gain, output_matrix, residual, mixture_norm_gain, selected_expert_index, routing_weight, routed_gate_weight, routed_up_weight, routed_down_weight, common_gate_weight, common_up_weight, common_down_weight):
    prepared_inputs = prepare_inputs(projected_queries, projected_keys, projected_values, write_strength_logits, decay_input_logits, head_rate_logarithm, extra_log_decay)
    terms = block_terms(*prepared_inputs)
    start = jnp.zeros((HEADS, HD, HD), jnp.float32)
    heads_out = finish(run_blocks(terms, start), output_gate_values, per_head_norm_gain)
    attended = residual.astype(jnp.float32) + jnp.dot(heads_out.astype(jnp.float32), output_matrix.astype(jnp.float32), preferred_element_type=jnp.float32)
    attended = attended.astype(jnp.bfloat16)
    normed = normalize(attended, mixture_norm_gain)
    shared = feed_forward(normed, common_gate_weight, common_up_weight, common_down_weight)
    routed = routed_sum(normed, selected_expert_index, routing_weight, routed_gate_weight, routed_up_weight, routed_down_weight)
    return (attended.astype(jnp.float32) + shared + routed).astype(jnp.bfloat16)
```

```python
import functools

import jax
import jax.numpy as jnp
from jax import lax
from jax.experimental import pallas as pl
from jax.experimental.pallas import tpu as pltpu
from jax.sharding import Mesh
from jax.sharding import PartitionSpec as P

TOP_K = 4
SPAN = 64
CAP = 12
HD = 128
AXES = ("sp_0", "sp_1", "sp_2", "tp")
SP = AXES[:3]
EPS = 1e-06
F32, BF16 = jnp.float32, jnp.bfloat16
HIGH = lax.Precision.HIGHEST
MESH = pl.DeviceIdType.MESH
VMEM = pl.BlockSpec(memory_space=pltpu.VMEM)
OFFSETS = (1, 3, 2)
ORDERS = ((2, 1, 0), (1, 0, 2), (0, 2, 1))
STATE_TYPE = BF16


def params(**kw):
    return pltpu.CompilerParams(vmem_limit_bytes=62 * 2**20, **kw)


def mm(a, b, dims=((1,), (0,))):
    return lax.dot_general(a, b, (dims, ((), ())), preferred_element_type=F32)


def halves(x):
    high = x.astype(BF16)
    return high, (x - high.astype(F32)).astype(BF16)


def mm3(a, b, dims=((1,), (0,))):
    (ah, al), (bh, bl) = a, b
    return mm(ah, bh, dims) + mm(al, bh, dims) + mm(ah, bl, dims)


def silu(x):
    return x / (1.0 + jnp.exp(-x))


def iota(shape, dim):
    return lax.broadcasted_iota(jnp.int32, shape, dim)


def local_kernel(
    q_ref, k_ref, v_ref, beta_ref, decay_ref, decay_t_ref,
    map_ref, z_ref, h_ref,
    low_s, score_s, inv_s, right_s, qd_s, kdt_s, wu_s, qp_s, step_s, pre_s,
):
    heads, tokens = 4, q_ref.shape[0]
    blocks = tokens // SPAN
    i256, j256 = iota((256, 256), 0), iota((256, 256), 1)
    same = (i256 // SPAN) == (j256 // SPAN)
    tri = jnp.where(same & (j256 <= i256), 1.0, 0.0)
    tri_t = jnp.where(same & (i256 <= j256), 1.0, 0.0)
    ones = jnp.where(same, 1.0, 0.0)

    def high(a, b):
        return lax.dot_general(a, b, (((1,), (0,)), ((), ())), precision=HIGH, preferred_element_type=F32)

    dec = [decay_ref[256 * i : 256 * i + 256, :] for i in range(2)]
    dec_t = [decay_t_ref[:, 256 * i : 256 * i + 256] for i in range(2)]
    g_col = jnp.concatenate([high(tri, d) for d in dec], 0)
    total_col = jnp.concatenate([high(ones, d) for d in dec], 0)
    g_row = jnp.concatenate([high(d, tri_t) for d in dec_t], 1)
    total_row = jnp.concatenate([high(d, ones) for d in dec_t], 1)
    beta = beta_ref[...]

    row, lane = iota((SPAN, 128), 0), iota((SPAN, 128), 1)
    first = lane < SPAN
    place = lane % SPAN
    causal, strict = row >= place, row > place
    pair_masks = [jnp.where(first, 1.0, 0.0).astype(BF16), jnp.where(first, 0.0, 1.0).astype(BF16)]
    first_wide = iota((128, 128), 1) < SPAN
    eye = jnp.where(iota((128, 128), 0) == iota((128, 128), 1), 1.0, 0.0)

    for h in range(heads):
        cols = slice(h * HD, h * HD + HD)
        q = silu(q_ref[:, cols].astype(F32))
        q = q * lax.rsqrt(jnp.sum(q * q, axis=-1, keepdims=True) + EPS)
        k = silu(k_ref[:, cols].astype(F32))
        k = k * lax.rsqrt(jnp.sum(k * k, axis=-1, keepdims=True) + EPS)
        v = silu(v_ref[:, cols].astype(F32))
        b_h, g_h = beta[:, h : h + 1], g_col[:, h : h + 1]
        grown = jnp.exp(g_h)
        kb = k * b_h
        right_s[h, :, :HD] = kb * grown
        right_s[h, :, HD:] = v * b_h
        qd_s[h] = q * grown
        gr = g_row[h : h + 1, :]
        kdt_s[h] = k.T * jnp.exp(total_row[h : h + 1, :] - gr)
        ks, kbs, qs = halves(k), halves(kb), halves(q)
        for j in range(tokens // 128):
            rows = slice(128 * j, 128 * j + 128)
            left = tuple(jnp.concatenate([a[rows], b[rows]], 0) for a, b in zip(kbs, qs))
            both = mm3(left, tuple(a[rows] for a in ks), ((1,), (1,)))
            inner = jnp.where(first, both[0:64], both[64:128])
            score = jnp.where(first, both[128:192], both[192:256])
            gi = jnp.where(first, g_h[128 * j : 128 * j + 64], g_h[128 * j + 64 : 128 * j + 128])
            spread = jnp.where(causal, gi - gr[:, rows], 0.0)
            decay = jnp.where(causal, jnp.exp(spread), 0.0)
            low_s[h, :, rows] = jnp.where(strict, inner * decay, 0.0)
            score_s[h, :, rows] = score * decay

    r4, l4 = iota((SPAN, 256), 0), iota((SPAN, 256), 1)
    p4 = l4 % SPAN
    quad_masks = [jnp.where(l4 // SPAN == n, 1.0, 0.0).astype(BF16) for n in range(4)]
    eye4 = jnp.where(r4 == p4, 1.0, 0.0)

    def diag4(x):
        return jnp.concatenate([x * m for m in quad_masks], 0)

    def times(a, b):
        return mm3(a, tuple(diag4(x) for x in b))

    groups = [(h, slice(256 * i, 256 * i + 256)) for h in range(heads) for i in range(2)]
    for part in range(2):
        mine = groups[4 * part : 4 * part + 4]
        lows = [low_s[h, :, s] for h, s in mine]
        small = r4 // 8 == p4 // 8
        d1 = [jnp.where(small, x, 0.0) for x in lows]
        d1s = [halves(x) for x in d1]
        d2s = [halves(times(x, x)) for x in d1s]
        x1 = [eye4 - x for x in d1]
        x2 = [x + times(halves(x), d) for x, d in zip(x1, d2s)]
        d4s = [halves(times(d, d)) for d in d2s]
        inv = [x + times(halves(x), d) for x, d in zip(x2, d4s)]
        for size in (8, 16, 32):
            off = (r4 // (2 * size) == p4 // (2 * size)) & (r4 // size != p4 // size)
            invs = [halves(x) for x in inv]
            ex = [halves(times(halves(jnp.where(off, x, 0.0)), y)) for x, y in zip(lows, invs)]
            inv = [x - times(y, e) for x, y, e in zip(inv, invs, ex)]
        for (h, s), x in zip(mine, inv):
            inv_s[h, :, s] = x

    def diag2(x):
        return jnp.concatenate([x * m for m in pair_masks], 0)

    for h in range(heads):
        for j in range(tokens // 128):
            rows = slice(128 * j, 128 * j + 128)
            inv = tuple(diag2(x) for x in halves(inv_s[h, :, rows]))
            wu = mm3(inv, halves(right_s[h, rows, :]))
            wus = halves(wu)
            score = tuple(diag2(x) for x in halves(score_s[h, :, rows]))
            applied = mm3(score, wus)
            qp_s[h, rows, :] = qd_s[h, rows, :] - applied[:, :HD]
            h_ref[h, rows, :] = applied[:, HD:]
            kdt = kdt_s[h, :, rows]
            kdt = jnp.concatenate([jnp.where(first_wide, kdt, 0.0), jnp.where(first_wide, 0.0, kdt)], 0)
            change = mm3(halves(kdt), wus)
            for c in range(2):
                n = 2 * j + c
                factor = jnp.exp(total_col[n * SPAN : n * SPAN + 1, h : h + 1])
                step_s[h, n, :, :HD] = eye * factor - change[128 * c : 128 * c + 128, :HD]
                step_s[h, n, :, HD:] = change[128 * c : 128 * c + 128, HD:]

    for h in range(heads):
        pre_s[h, 1] = step_s[h, 0]
    for n in range(1, blocks):
        for h in range(heads):
            moved = mm3(halves(step_s[h, n, :, :HD]), halves(pre_s[h, n]))
            pre = jnp.concatenate([moved[:, :HD], moved[:, HD:] + step_s[h, n, :, HD:]], 1)
            if n + 1 < blocks:
                pre_s[h, n + 1] = pre
            else:
                map_ref[h] = pre.astype(map_ref.dtype)
    for h in range(heads):
        z_ref[h, 0:SPAN, :] = qp_s[h, 0:SPAN, :]
        for n in range(1, blocks):
            rows = slice(SPAN * n, SPAN * n + SPAN)
            moved = mm3(halves(qp_s[h, rows, :]), halves(pre_s[h, n]))
            z_ref[h, rows, :] = moved[:, :HD]
            h_ref[h, rows, :] = h_ref[h, rows, :] + moved[:, HD:]


def local_terms(q, k, v, beta, decay):
    tokens = q.shape[0]
    heads = 4
    return pl.pallas_call(
        local_kernel,
        out_shape=(
            jax.ShapeDtypeStruct((heads, HD, 2 * HD), STATE_TYPE),
            jax.ShapeDtypeStruct((heads, tokens, HD), F32),
            jax.ShapeDtypeStruct((heads, tokens, HD), F32),
        ),
        in_specs=[VMEM] * 6,
        out_specs=(VMEM,) * 3,
        scratch_shapes=[
            pltpu.VMEM((heads, SPAN, tokens), F32),
            pltpu.VMEM((heads, SPAN, tokens), F32),
            pltpu.VMEM((heads, SPAN, tokens), F32),
            pltpu.VMEM((heads, tokens, 2 * HD), F32),
            pltpu.VMEM((heads, tokens, HD), F32),
            pltpu.VMEM((heads, HD, tokens), F32),
            pltpu.VMEM((8, 128), F32),
            pltpu.VMEM((heads, tokens, HD), F32),
            pltpu.VMEM((heads, tokens // SPAN, HD, 2 * HD), F32),
            pltpu.VMEM((heads, tokens // SPAN, HD, 2 * HD), F32),
        ],
        compiler_params=params(),
        name="local_terms",
    )(q, k, v, beta, decay, decay.T)


def along(dim, off):
    at = [lax.axis_index(a) for a in AXES]
    at[dim] = lax.rem(at[dim] + off, 4)
    return tuple(at)


def partner():
    at = [lax.axis_index(a) for a in AXES]
    at[3] = 1 - at[3]
    return tuple(at)


def greet(dims, pair):
    barrier = pltpu.get_barrier_semaphore()
    count = 0
    for dim in dims:
        for off in OFFSETS:
            pl.semaphore_signal(barrier, inc=1, device_id=along(dim, off), device_id_type=MESH)
            count += 1
    if pair:
        pl.semaphore_signal(barrier, inc=1, device_id=partner(), device_id_type=MESH)
        count += 1
    pl.semaphore_wait(barrier, count)


def mixed_kernel(
    map_ref, z_ref, h_ref, gate_ref, gain_ref, out_w_ref, residual_ref, norm_ref,
    attended_ref, normed_ref,
    row_s, plane_s, all_s, row_total, plane_total, state_out, state_in, mix_s, mix_in, acc_s,
    send_sem, recv_sem,
):
    greet((0, 1, 2), True)
    z, y, x, c = (lax.axis_index(a) for a in AXES)

    def send(stage, dim, source, target):
        copies = []
        here = lax.axis_index(AXES[dim])
        for n, off in enumerate(OFFSETS):
            copies.append(
                pltpu.make_async_remote_copy(
                    src_ref=source(lax.rem(here + off, 4)),
                    dst_ref=target.at[here],
                    send_sem=send_sem.at[stage, n],
                    recv_sem=recv_sem.at[stage, n],
                    device_id=along(dim, off),
                    device_id_type=MESH,
                )
            )
        for copy in copies:
            copy.start()
        return copies

    def applied(step, carried):
        high, low = halves(carried)
        moved = mm(step[:, :HD], high) + mm(step[:, :HD], low)
        if carried.shape[1] == HD:
            return moved + step[:, HD:].astype(F32)
        return jnp.concatenate([moved[:, :HD], moved[:, HD:] + step[:, HD:].astype(F32)], 1)

    def total(steps):
        carried = steps[0].astype(F32)
        for i in range(1, 4):
            carried = applied(steps[i], carried)
        return carried.astype(STATE_TYPE)

    sent = []
    copies = send(0, 2, lambda t: map_ref.at[t], row_s)
    row_s[x] = map_ref[x]
    for copy in copies:
        copy.wait_recv()
    sent += copies
    row_total[...] = total(row_s)
    copies = send(1, 1, lambda t: row_total, plane_s)
    plane_s[y] = row_total[...]
    for copy in copies:
        copy.wait_recv()
    sent += copies
    plane_total[...] = total(plane_s)
    copies = send(2, 0, lambda t: plane_total, all_s)
    all_s[z] = plane_total[...]
    for copy in copies:
        copy.wait_recv()
    sent += copies
    state = jnp.where(z > 0, all_s[0, :, HD:].astype(F32), 0.0)
    for i in range(1, 3):
        state = jnp.where(i < z, applied(all_s[i], state), state)
    for i in range(3):
        state = jnp.where(i < y, applied(plane_s[i], state), state)
    state_out[0] = state.astype(STATE_TYPE)
    for i in range(3):
        state = applied(row_s[i], state)
        state_out[i + 1] = state.astype(STATE_TYPE)
    copies = send(3, 2, lambda t: state_out.at[t], state_in)
    state_in[x] = state_out[x]
    for copy in copies:
        copy.wait_recv()
    sent += copies

    gain = gain_ref[...]
    for h in range(4):
        high, low = halves(z_ref[h])
        state = state_in[h]
        mix = h_ref[h] + mm(high, state) + mm(low, state)
        mix = mix * lax.rsqrt(jnp.mean(mix * mix, axis=-1, keepdims=True) + EPS) * gain
        mix = mix * silu(gate_ref[:, h * HD : h * HD + HD].astype(F32))
        mix_s[:, h * HD : h * HD + HD] = mix.astype(BF16)
    half = mix_s.shape[0] // 2
    width = mix_s.shape[1]
    other = 1 - c
    swap = pltpu.make_async_remote_copy(
        src_ref=mix_s.at[pl.ds(pl.multiple_of(other * half, half), half)],
        dst_ref=mix_in,
        send_sem=send_sem.at[4, 0],
        recv_sem=recv_sem.at[4, 0],
        device_id=partner(),
        device_id_type=MESH,
    )
    swap.start()
    own = pl.ds(pl.multiple_of(c * half, half), half)
    own_w = pl.ds(pl.multiple_of(c * width, width), width)
    other_w = pl.ds(pl.multiple_of(other * width, width), width)
    model = out_w_ref.shape[1]
    for n in range(model // 512):
        cols = slice(512 * n, 512 * n + 512)
        acc_s[:, cols] = residual_ref[:, cols].astype(F32) + mm(mix_s[own, :], out_w_ref[own_w, cols])
    swap.wait()
    squares = jnp.zeros((half, 1), F32)
    for n in range(model // 512):
        cols = slice(512 * n, 512 * n + 512)
        piece = acc_s[:, cols] + mm(mix_in[...], out_w_ref[other_w, cols])
        piece = piece.astype(BF16)
        attended_ref[:, cols] = piece
        wide = piece.astype(F32)
        acc_s[:, cols] = wide
        squares = squares + jnp.sum(wide * wide, axis=-1, keepdims=True)
    scale = lax.rsqrt(squares / model + EPS)
    for n in range(model // 512):
        cols = slice(512 * n, 512 * n + 512)
        normed_ref[own, cols] = (acc_s[:, cols] * scale * norm_ref[:, cols]).astype(BF16)
    share = pltpu.make_async_remote_copy(
        src_ref=normed_ref.at[own],
        dst_ref=normed_ref.at[own],
        send_sem=send_sem.at[4, 1],
        recv_sem=recv_sem.at[4, 1],
        device_id=partner(),
        device_id_type=MESH,
    )
    share.start()
    share.wait()
    for copy in sent:
        copy.wait_send()


def mixed(maps, z, h, gate, gain, out_w, residual, norm_gain):
    half, model = residual.shape
    return pl.pallas_call(
        mixed_kernel,
        out_shape=(
            jax.ShapeDtypeStruct((half, model), BF16),
            jax.ShapeDtypeStruct((2 * half, model), BF16),
        ),
        in_specs=[VMEM] * 8,
        out_specs=(VMEM,) * 2,
        scratch_shapes=[
            pltpu.VMEM((4, HD, 2 * HD), STATE_TYPE),
            pltpu.VMEM((4, HD, 2 * HD), STATE_TYPE),
            pltpu.VMEM((4, HD, 2 * HD), STATE_TYPE),
            pltpu.VMEM((HD, 2 * HD), STATE_TYPE),
            pltpu.VMEM((HD, 2 * HD), STATE_TYPE),
            pltpu.VMEM((4, HD, HD), STATE_TYPE),
            pltpu.VMEM((4, HD, HD), STATE_TYPE),
            pltpu.VMEM((2 * half, 4 * HD), BF16),
            pltpu.VMEM((half, 4 * HD), BF16),
            pltpu.VMEM((half, model), F32),
            pltpu.SemaphoreType.DMA((5, 3)),
            pltpu.SemaphoreType.DMA((5, 3)),
        ],
        compiler_params=params(collective_id=0, has_side_effects=True),
        name="mixed",
    )(maps, z, h, gate, gain, out_w, residual, norm_gain)


def piece(ref, dim, i):
    if dim == 0:
        return ref.at[i]
    if dim == 1:
        return ref.at[:, i]
    return ref.at[:, :, i]


def exchange_kernel(src_ref, dst_ref, one_ref, two_ref, send_sem, recv_sem):
    greet((0, 1, 2), False)
    buffers = (src_ref, one_ref, two_ref, dst_ref)
    sent = []
    for stage in range(3):
        copies = []
        for n, off in enumerate(OFFSETS):
            for k in range(3):
                dim = ORDERS[k][stage]
                here = lax.axis_index(AXES[dim])
                copy = pltpu.make_async_remote_copy(
                    src_ref=piece(buffers[stage].at[k], dim, lax.rem(here + off, 4)),
                    dst_ref=piece(buffers[stage + 1].at[k], dim, here),
                    send_sem=send_sem.at[stage, k, n],
                    recv_sem=recv_sem.at[stage, k, n],
                    device_id=along(dim, off),
                    device_id_type=MESH,
                )
                copy.start()
                copies.append(copy)
        for k in range(3):
            dim = ORDERS[k][stage]
            here = lax.axis_index(AXES[dim])
            source = piece(buffers[stage].at[k], dim, here)
            target = piece(buffers[stage + 1].at[k], dim, here)

            def keep(i, _):
                target[i // 4, i % 4] = source[i // 4, i % 4]
                return 0

            lax.fori_loop(0, 16, keep, 0)
        for copy in copies:
            copy.wait_recv()
        sent += copies
    for copy in sent:
        copy.wait_send()


def exchange(rows):
    return pl.pallas_call(
        exchange_kernel,
        out_shape=jax.ShapeDtypeStruct(rows.shape, rows.dtype),
        in_specs=[VMEM],
        out_specs=VMEM,
        scratch_shapes=[pltpu.VMEM(rows.shape, rows.dtype)] * 2
        + [pltpu.SemaphoreType.DMA((3, 3, 3))] * 2,
        compiler_params=params(collective_id=1, has_side_effects=True),
        name="exchange",
    )(rows)


def dispatch_kernel(normed_ref, ids_ref, expert_ref, rows_ref, code_s):
    tokens = normed_ref.shape[0]
    half = tokens // 2
    chips = expert_ref.shape[0]
    chosen = jnp.zeros((chips, tokens), F32)
    for j in range(TOP_K):
        chosen = chosen + jnp.where(ids_ref[j : j + 1, :] == expert_ref[...], 1.0, 0.0)
    i, j = iota((tokens, tokens), 0), iota((tokens, tokens), 1)
    before = jnp.where((i // half == j // half) & (i < j), 1.0, 0.0).astype(BF16)
    slot = mm(chosen.astype(BF16), before)
    shift = jnp.where(iota((chips, tokens), 1) < half, 0.0, float(CAP))
    code_s[...] = jnp.where(chosen > 0.0, slot + shift, -1.0)
    for k in range(3):
        low = 0 if k < 2 else half
        high = half if k == 0 else tokens

        def one(zi, _):
            code = code_s[pl.ds(pl.multiple_of(zi * 16, 16), 16), low:high]
            wanted = (iota((16, 8, high - low), 1) + 8 * k).astype(F32)
            pick = jnp.where(code[:, None, :] == wanted, 1.0, 0.0).reshape(128, high - low).astype(BF16)
            rows = mm(pick, normed_ref[low:high, :]).astype(BF16)
            rows_ref[k, zi] = rows.reshape(4, 4, 8, rows.shape[-1])
            return 0

        lax.fori_loop(0, 4, one, 0)


def dispatch(normed, ids, experts):
    return pl.pallas_call(
        dispatch_kernel,
        out_shape=jax.ShapeDtypeStruct((3, 4, 4, 4, 8, normed.shape[1]), BF16),
        in_specs=[VMEM] * 3,
        out_specs=VMEM,
        scratch_shapes=[pltpu.VMEM((64, normed.shape[0]), F32)],
        compiler_params=params(),
        name="dispatch",
    )(normed, ids, experts)


def experts_kernel(rows_ref, gate_ref, up_ref, down_ref, out_ref):
    def one(k, _):
        rows = rows_ref[k].reshape(512, rows_ref.shape[-1])
        hidden = silu(mm(rows, gate_ref[...])) * mm(rows, up_ref[...])
        result = mm(hidden.astype(BF16), down_ref[...]).astype(BF16)
        out_ref[k] = result.reshape(out_ref.shape[1:])
        return 0

    lax.fori_loop(0, 3, one, 0)


def run_experts(rows, gate, up, down):
    return pl.pallas_call(
        experts_kernel,
        out_shape=jax.ShapeDtypeStruct(rows.shape, BF16),
        in_specs=[VMEM] * 4,
        out_specs=VMEM,
        compiler_params=params(),
        name="experts",
    )(rows, gate, up, down)


def combine_kernel(
    back_ref, ids_ref, expert_ref, weight_ref, normed_ref, attended_ref, gate_ref, up_ref, down_ref,
    out_ref, pick_s, away_s, here_s, send_sem, recv_sem,
):
    greet((), True)
    tokens, model = normed_ref.shape
    half = tokens // 2
    chips = expert_ref.shape[1]
    c = lax.axis_index("tp")
    chosen = jnp.zeros((tokens, chips), F32)
    weight = jnp.zeros((tokens, chips), F32)
    for j in range(TOP_K):
        hit = ids_ref[:, j : j + 1] == expert_ref[...]
        chosen = chosen + jnp.where(hit, 1.0, 0.0)
        weight = weight + jnp.where(hit, weight_ref[:, j : j + 1], 0.0)
    i, j = iota((tokens, tokens), 0), iota((tokens, tokens), 1)
    before = jnp.where((i // half == j // half) & (j < i), 1.0, 0.0).astype(BF16)
    slot = mm(before, chosen.astype(BF16))
    shift = jnp.where(iota((tokens, chips), 0) < half, 0.0, float(CAP))
    code = jnp.where(chosen > 0.0, slot + shift, -1.0).astype(BF16)
    spread = jnp.where(iota((chips, 8 * chips), 1) // 8 == iota((chips, 8 * chips), 0), 1.0, 0.0).astype(BF16)
    code = mm(code, spread)
    weight = mm(weight.astype(BF16), spread)
    place = (iota((tokens, 8 * chips), 1) % 8).astype(F32)
    for k in range(3):
        pick_s[k] = jnp.where(code == place + 8.0 * k, weight, 0.0).astype(BF16)

    def partial(core, n):
        rows = pl.ds(pl.multiple_of(core * half, half), half)
        cols = slice(512 * n, 512 * n + 512)
        total = jnp.zeros((half, 512), F32)
        for k in range(3):
            total = total + mm(pick_s[k, rows, :], back_ref[k, :, :, :, :, cols].reshape(8 * chips, 512))
        return total

    for n in range(model // 512):
        away_s[:, 512 * n : 512 * n + 512] = partial(1 - c, n)
    copy = pltpu.make_async_remote_copy(
        src_ref=away_s,
        dst_ref=here_s,
        send_sem=send_sem,
        recv_sem=recv_sem,
        device_id=partner(),
        device_id_type=MESH,
    )
    copy.start()
    own = pl.ds(pl.multiple_of(c * half, half), half)
    rows = normed_ref[own, :]
    hidden = (silu(mm(rows, gate_ref[...])) * mm(rows, up_ref[...])).astype(BF16)
    copy.wait()
    for n in range(model // 512):
        cols = slice(512 * n, 512 * n + 512)
        total = attended_ref[:, cols].astype(F32) + mm(hidden, down_ref[:, cols])
        out_ref[:, cols] = (total + (partial(c, n) + here_s[:, cols])).astype(BF16)


def combine(back, ids, experts, weight, normed, attended, gate, up, down):
    half, model = attended.shape
    return pl.pallas_call(
        combine_kernel,
        out_shape=jax.ShapeDtypeStruct((half, model), BF16),
        in_specs=[VMEM] * 9,
        out_specs=VMEM,
        scratch_shapes=[
            pltpu.VMEM((3, 2 * half, 512), BF16),
            pltpu.VMEM((half, model), F32),
            pltpu.VMEM((half, model), F32),
            pltpu.SemaphoreType.DMA,
            pltpu.SemaphoreType.DMA,
        ],
        compiler_params=params(collective_id=2, has_side_effects=True),
        name="combine",
    )(back, ids, experts, weight, normed, attended, gate, up, down)


def shards(
    projected_queries,
    projected_keys,
    projected_values,
    output_gate_values,
    write_strength_logits,
    decay_input_logits,
    head_rate_logarithm,
    extra_log_decay,
    per_head_norm_gain,
    output_matrix,
    residual,
    mixture_norm_gain,
    selected_expert_index,
    routing_weight,
    routed_gate_weight,
    routed_up_weight,
    routed_down_weight,
    common_gate_weight,
    common_up_weight,
    common_down_weight,
):
    beta = jax.nn.sigmoid(write_strength_logits.astype(F32))
    decay = extra_log_decay - jnp.exp(head_rate_logarithm)[None, :] * jax.nn.softplus(
        decay_input_logits.astype(F32) - 6.0
    )
    ids = lax.all_gather(selected_expert_index, "tp", tiled=True)
    weight = lax.all_gather(routing_weight, "tp", tiled=True)
    experts = 2 * jnp.arange(64, dtype=jnp.int32) + lax.axis_index("tp").astype(jnp.int32)
    maps, z, h = local_terms(projected_queries, projected_keys, projected_values, beta, decay)
    attended, normed = mixed(
        maps,
        z,
        h,
        output_gate_values,
        per_head_norm_gain[None, :],
        output_matrix,
        residual,
        mixture_norm_gain[None, :],
    )
    outgoing = dispatch(normed, ids.T, experts[:, None])
    arrived = exchange(outgoing)
    served = run_experts(arrived, routed_gate_weight[0], routed_up_weight[0], routed_down_weight[0])
    back = exchange(served)
    return combine(
        back,
        ids,
        experts[None, :],
        weight,
        normed,
        attended,
        common_gate_weight,
        common_up_weight,
        common_down_weight,
    )


def solution(mesh):
    finer = Mesh(mesh.devices.reshape(4, 4, 4, mesh.shape["tp"]), AXES)
    in_specs = (
        P(SP, "tp"),
        P(SP, "tp"),
        P(SP, "tp"),
        P(SP, "tp"),
        P(SP, "tp"),
        P(SP, "tp"),
        P("tp"),
        P(SP, "tp"),
        P(),
        P(),
        P(AXES, None),
        P(),
        P(AXES, None),
        P(AXES, None),
        P(AXES, None, None),
        P(AXES, None, None),
        P(AXES, None, None),
        P(),
        P(),
        P(),
    )
    return jax.shard_map(
        shards, mesh=finer, in_specs=in_specs, out_specs=P(AXES, None), check_vma=False
    )
```

```python
import functools

import jax
import jax.numpy as jnp
from jax import lax
from jax.experimental import pallas as pl
from jax.experimental.pallas import tpu as pltpu
from jax.sharding import Mesh
from jax.sharding import PartitionSpec as P

TOP_K = 4
SPAN = 64
CAP = 12
HD = 128
AXES = ("sp_0", "sp_1", "sp_2", "tp")
SP = AXES[:3]
EPS = 1e-06
F32, BF16 = jnp.float32, jnp.bfloat16
HIGH = lax.Precision.HIGHEST
MESH = pl.DeviceIdType.MESH
VMEM = pl.BlockSpec(memory_space=pltpu.VMEM)
OFFSETS = (1, 3, 2)
ORDERS = ((2, 1, 0), (1, 0, 2), (0, 2, 1))
STATE_TYPE = BF16


def params(**kw):
    return pltpu.CompilerParams(vmem_limit_bytes=62 * 2**20, **kw)


def mm(a, b, dims=((1,), (0,))):
    return lax.dot_general(a, b, (dims, ((), ())), preferred_element_type=F32)


def halves(x):
    high = x.astype(BF16)
    return high, (x - high.astype(F32)).astype(BF16)


def mm3(a, b, dims=((1,), (0,))):
    (ah, al), (bh, bl) = a, b
    return mm(ah, bh, dims) + mm(al, bh, dims) + mm(ah, bl, dims)


def silu(x):
    return x / (1.0 + jnp.exp(-x))


def iota(shape, dim):
    return lax.broadcasted_iota(jnp.int32, shape, dim)


def local_kernel(
    q_ref, k_ref, v_ref, beta_ref, decay_ref, decay_t_ref,
    map_ref, z_ref, h_ref,
    low_s, score_s, inv_s, right_s, qd_s, kdt_s, wu_s, qp_s, step_s, pre_s,
):
    heads, tokens = 4, q_ref.shape[0]
    blocks = tokens // SPAN
    i256, j256 = iota((256, 256), 0), iota((256, 256), 1)
    same = (i256 // SPAN) == (j256 // SPAN)
    tri = jnp.where(same & (j256 <= i256), 1.0, 0.0)
    tri_t = jnp.where(same & (i256 <= j256), 1.0, 0.0)
    ones = jnp.where(same, 1.0, 0.0)

    def high(a, b):
        return lax.dot_general(a, b, (((1,), (0,)), ((), ())), precision=HIGH, preferred_element_type=F32)

    dec = [decay_ref[256 * i : 256 * i + 256, :] for i in range(2)]
    dec_t = [decay_t_ref[:, 256 * i : 256 * i + 256] for i in range(2)]
    g_col = jnp.concatenate([high(tri, d) for d in dec], 0)
    total_col = jnp.concatenate([high(ones, d) for d in dec], 0)
    g_row = jnp.concatenate([high(d, tri_t) for d in dec_t], 1)
    total_row = jnp.concatenate([high(d, ones) for d in dec_t], 1)
    beta = beta_ref[...]

    row, lane = iota((SPAN, 128), 0), iota((SPAN, 128), 1)
    first = lane < SPAN
    place = lane % SPAN
    causal, strict = row >= place, row > place
    pair_masks = [jnp.where(first, 1.0, 0.0).astype(BF16), jnp.where(first, 0.0, 1.0).astype(BF16)]
    first_wide = iota((128, 128), 1) < SPAN
    eye = jnp.where(iota((128, 128), 0) == iota((128, 128), 1), 1.0, 0.0)

    for h in range(heads):
        cols = slice(h * HD, h * HD + HD)
        q = silu(q_ref[:, cols].astype(F32))
        q = q * lax.rsqrt(jnp.sum(q * q, axis=-1, keepdims=True) + EPS)
        k = silu(k_ref[:, cols].astype(F32))
        k = k * lax.rsqrt(jnp.sum(k * k, axis=-1, keepdims=True) + EPS)
        v = silu(v_ref[:, cols].astype(F32))
        b_h, g_h = beta[:, h : h + 1], g_col[:, h : h + 1]
        grown = jnp.exp(g_h)
        kb = k * b_h
        right_s[h, :, :HD] = kb * grown
        right_s[h, :, HD:] = v * b_h
        qd_s[h] = q * grown
        gr = g_row[h : h + 1, :]
        kdt_s[h] = k.T * jnp.exp(total_row[h : h + 1, :] - gr)
        ks, kbs, qs = halves(k), halves(kb), halves(q)
        for j in range(tokens // 128):
            rows = slice(128 * j, 128 * j + 128)
            left = tuple(jnp.concatenate([a[rows], b[rows]], 0) for a, b in zip(kbs, qs))
            both = mm3(left, tuple(a[rows] for a in ks), ((1,), (1,)))
            inner = jnp.where(first, both[0:64], both[64:128])
            score = jnp.where(first, both[128:192], both[192:256])
            gi = jnp.where(first, g_h[128 * j : 128 * j + 64], g_h[128 * j + 64 : 128 * j + 128])
            spread = jnp.where(causal, gi - gr[:, rows], 0.0)
            decay = jnp.where(causal, jnp.exp(spread), 0.0)
            low_s[h, :, rows] = jnp.where(strict, inner * decay, 0.0)
            score_s[h, :, rows] = score * decay

    r4, l4 = iota((SPAN, 256), 0), iota((SPAN, 256), 1)
    p4 = l4 % SPAN
    quad_masks = [jnp.where(l4 // SPAN == n, 1.0, 0.0).astype(BF16) for n in range(4)]
    eye4 = jnp.where(r4 == p4, 1.0, 0.0)

    def diag4(x):
        return jnp.concatenate([x * m for m in quad_masks], 0)

    def times(a, b):
        return mm3(a, tuple(diag4(x) for x in b))

    groups = [(h, slice(256 * i, 256 * i + 256)) for h in range(heads) for i in range(2)]
    for part in range(2):
        mine = groups[4 * part : 4 * part + 4]
        lows = [low_s[h, :, s] for h, s in mine]
        small = r4 // 8 == p4 // 8
        d1 = [jnp.where(small, x, 0.0) for x in lows]
        d1s = [halves(x) for x in d1]
        d2s = [halves(times(x, x)) for x in d1s]
        x1 = [eye4 - x for x in d1]
        x2 = [x + times(halves(x), d) for x, d in zip(x1, d2s)]
        d4s = [halves(times(d, d)) for d in d2s]
        inv = [x + times(halves(x), d) for x, d in zip(x2, d4s)]
        for size in (8, 16, 32):
            off = (r4 // (2 * size) == p4 // (2 * size)) & (r4 // size != p4 // size)
            invs = [halves(x) for x in inv]
            ex = [halves(times(halves(jnp.where(off, x, 0.0)), y)) for x, y in zip(lows, invs)]
            inv = [x - times(y, e) for x, y, e in zip(inv, invs, ex)]
        for (h, s), x in zip(mine, inv):
            inv_s[h, :, s] = x

    def diag2(x):
        return jnp.concatenate([x * m for m in pair_masks], 0)

    for h in range(heads):
        for j in range(tokens // 128):
            rows = slice(128 * j, 128 * j + 128)
            inv = tuple(diag2(x) for x in halves(inv_s[h, :, rows]))
            wu = mm3(inv, halves(right_s[h, rows, :]))
            wus = halves(wu)
            score = tuple(diag2(x) for x in halves(score_s[h, :, rows]))
            applied = mm3(score, wus)
            qp_s[h, rows, :] = qd_s[h, rows, :] - applied[:, :HD]
            h_ref[h, rows, :] = applied[:, HD:]
            kdt = kdt_s[h, :, rows]
            kdt = jnp.concatenate([jnp.where(first_wide, kdt, 0.0), jnp.where(first_wide, 0.0, kdt)], 0)
            change = mm3(halves(kdt), wus)
            for c in range(2):
                n = 2 * j + c
                factor = jnp.exp(total_col[n * SPAN : n * SPAN + 1, h : h + 1])
                step_s[h, n, :, :HD] = eye * factor - change[128 * c : 128 * c + 128, :HD]
                step_s[h, n, :, HD:] = change[128 * c : 128 * c + 128, HD:]

    for h in range(heads):
        pre_s[h, 1] = step_s[h, 0]
    for n in range(1, blocks):
        for h in range(heads):
            moved = mm3(halves(step_s[h, n, :, :HD]), halves(pre_s[h, n]))
            pre = jnp.concatenate([moved[:, :HD], moved[:, HD:] + step_s[h, n, :, HD:]], 1)
            if n + 1 < blocks:
                pre_s[h, n + 1] = pre
            else:
                map_ref[h] = pre.astype(map_ref.dtype)
    for h in range(heads):
        z_ref[h, 0:SPAN, :] = qp_s[h, 0:SPAN, :]
        for n in range(1, blocks):
            rows = slice(SPAN * n, SPAN * n + SPAN)
            moved = mm3(halves(qp_s[h, rows, :]), halves(pre_s[h, n]))
            z_ref[h, rows, :] = moved[:, :HD]
            h_ref[h, rows, :] = h_ref[h, rows, :] + moved[:, HD:]


def local_terms(q, k, v, beta, decay):
    tokens = q.shape[0]
    heads = 4
    return pl.pallas_call(
        local_kernel,
        out_shape=(
            jax.ShapeDtypeStruct((heads, HD, 2 * HD), STATE_TYPE),
            jax.ShapeDtypeStruct((heads, tokens, HD), F32),
            jax.ShapeDtypeStruct((heads, tokens, HD), F32),
        ),
        in_specs=[VMEM] * 6,
        out_specs=(VMEM,) * 3,
        scratch_shapes=[
            pltpu.VMEM((heads, SPAN, tokens), F32),
            pltpu.VMEM((heads, SPAN, tokens), F32),
            pltpu.VMEM((heads, SPAN, tokens), F32),
            pltpu.VMEM((heads, tokens, 2 * HD), F32),
            pltpu.VMEM((heads, tokens, HD), F32),
            pltpu.VMEM((heads, HD, tokens), F32),
            pltpu.VMEM((8, 128), F32),
            pltpu.VMEM((heads, tokens, HD), F32),
            pltpu.VMEM((heads, tokens // SPAN, HD, 2 * HD), F32),
            pltpu.VMEM((heads, tokens // SPAN, HD, 2 * HD), F32),
        ],
        compiler_params=params(),
        name="local_terms",
    )(q, k, v, beta, decay, decay.T)


def along(dim, off):
    at = [lax.axis_index(a) for a in AXES]
    at[dim] = lax.rem(at[dim] + off, 4)
    return tuple(at)


def partner():
    at = [lax.axis_index(a) for a in AXES]
    at[3] = 1 - at[3]
    return tuple(at)


def greet(dims, pair):
    barrier = pltpu.get_barrier_semaphore()
    count = 0
    for dim in dims:
        for off in OFFSETS:
            pl.semaphore_signal(barrier, inc=1, device_id=along(dim, off), device_id_type=MESH)
            count += 1
    if pair:
        pl.semaphore_signal(barrier, inc=1, device_id=partner(), device_id_type=MESH)
        count += 1
    pl.semaphore_wait(barrier, count)


def mixed_kernel(
    map_ref, z_ref, h_ref, gate_ref, gain_ref, out_w_ref, residual_ref, norm_ref, meta_ref,
    attended_ref, normed_ref, both_meta_ref,
    row_s, plane_s, all_s, row_total, plane_total, state_out, state_in, mix_s, mix_in, acc_s,
    send_sem, recv_sem,
):
    greet((0, 1, 2), True)
    z, y, x, c = (lax.axis_index(a) for a in AXES)

    def send(stage, dim, source, target):
        copies = []
        here = lax.axis_index(AXES[dim])
        for n, off in enumerate(OFFSETS):
            copies.append(
                pltpu.make_async_remote_copy(
                    src_ref=source(lax.rem(here + off, 4)),
                    dst_ref=target.at[here],
                    send_sem=send_sem.at[stage, n],
                    recv_sem=recv_sem.at[stage, n],
                    device_id=along(dim, off),
                    device_id_type=MESH,
                )
            )
        for copy in copies:
            copy.start()
        return copies

    def applied(step, carried):
        high, low = halves(carried)
        moved = mm(step[:, :HD], high) + mm(step[:, :HD], low)
        if carried.shape[1] == HD:
            return moved + step[:, HD:].astype(F32)
        return jnp.concatenate([moved[:, :HD], moved[:, HD:] + step[:, HD:].astype(F32)], 1)

    def total(steps):
        carried = steps[0].astype(F32)
        for i in range(1, 4):
            carried = applied(steps[i], carried)
        return carried.astype(STATE_TYPE)

    sent = []
    copies = send(0, 2, lambda t: map_ref.at[t], row_s)
    tell = pltpu.make_async_remote_copy(
        src_ref=meta_ref,
        dst_ref=both_meta_ref.at[c],
        send_sem=send_sem.at[4, 2],
        recv_sem=recv_sem.at[4, 2],
        device_id=partner(),
        device_id_type=MESH,
    )
    tell.start()
    both_meta_ref[c] = meta_ref[...]
    row_s[x] = map_ref[x]
    for copy in copies:
        copy.wait_recv()
    sent += copies
    row_total[...] = total(row_s)
    copies = send(1, 1, lambda t: row_total, plane_s)
    plane_s[y] = row_total[...]
    for copy in copies:
        copy.wait_recv()
    sent += copies
    plane_total[...] = total(plane_s)
    copies = send(2, 0, lambda t: plane_total, all_s)
    all_s[z] = plane_total[...]
    for copy in copies:
        copy.wait_recv()
    sent += copies
    state = jnp.where(z > 0, all_s[0, :, HD:].astype(F32), 0.0)
    for i in range(1, 3):
        state = jnp.where(i < z, applied(all_s[i], state), state)
    for i in range(3):
        state = jnp.where(i < y, applied(plane_s[i], state), state)
    state_out[0] = state.astype(STATE_TYPE)
    for i in range(3):
        state = applied(row_s[i], state)
        state_out[i + 1] = state.astype(STATE_TYPE)
    copies = send(3, 2, lambda t: state_out.at[t], state_in)
    state_in[x] = state_out[x]
    for copy in copies:
        copy.wait_recv()
    sent += copies

    gain = gain_ref[...]
    for h in range(4):
        high, low = halves(z_ref[h])
        state = state_in[h]
        mix = h_ref[h] + mm(high, state) + mm(low, state)
        mix = mix * lax.rsqrt(jnp.mean(mix * mix, axis=-1, keepdims=True) + EPS) * gain
        mix = mix * silu(gate_ref[:, h * HD : h * HD + HD].astype(F32))
        mix_s[:, h * HD : h * HD + HD] = mix.astype(BF16)
    half = mix_s.shape[0] // 2
    width = mix_s.shape[1]
    other = 1 - c
    swap = pltpu.make_async_remote_copy(
        src_ref=mix_s.at[pl.ds(pl.multiple_of(other * half, half), half)],
        dst_ref=mix_in,
        send_sem=send_sem.at[4, 0],
        recv_sem=recv_sem.at[4, 0],
        device_id=partner(),
        device_id_type=MESH,
    )
    swap.start()
    own = pl.ds(pl.multiple_of(c * half, half), half)
    own_w = pl.ds(pl.multiple_of(c * width, width), width)
    other_w = pl.ds(pl.multiple_of(other * width, width), width)
    model = out_w_ref.shape[1]
    for n in range(model // 512):
        cols = slice(512 * n, 512 * n + 512)
        acc_s[:, cols] = residual_ref[:, cols].astype(F32) + mm(mix_s[own, :], out_w_ref[own_w, cols])
    swap.wait()
    squares = jnp.zeros((half, 1), F32)
    for n in range(model // 512):
        cols = slice(512 * n, 512 * n + 512)
        piece = acc_s[:, cols] + mm(mix_in[...], out_w_ref[other_w, cols])
        piece = piece.astype(BF16)
        attended_ref[:, cols] = piece
        wide = piece.astype(F32)
        acc_s[:, cols] = wide
        squares = squares + jnp.sum(wide * wide, axis=-1, keepdims=True)
    scale = lax.rsqrt(squares / model + EPS)
    for n in range(model // 512):
        cols = slice(512 * n, 512 * n + 512)
        normed_ref[own, cols] = (acc_s[:, cols] * scale * norm_ref[:, cols]).astype(BF16)
    share = pltpu.make_async_remote_copy(
        src_ref=normed_ref.at[own],
        dst_ref=normed_ref.at[own],
        send_sem=send_sem.at[4, 1],
        recv_sem=recv_sem.at[4, 1],
        device_id=partner(),
        device_id_type=MESH,
    )
    share.start()
    tell.wait()
    share.wait()
    for copy in sent:
        copy.wait_send()


def mixed(maps, z, h, gate, gain, out_w, residual, norm_gain, meta):
    half, model = residual.shape
    return pl.pallas_call(
        mixed_kernel,
        out_shape=(
            jax.ShapeDtypeStruct((half, model), BF16),
            jax.ShapeDtypeStruct((2 * half, model), BF16),
            jax.ShapeDtypeStruct((2,) + meta.shape, F32),
        ),
        in_specs=[VMEM] * 9,
        out_specs=(VMEM,) * 3,
        scratch_shapes=[
            pltpu.VMEM((4, HD, 2 * HD), STATE_TYPE),
            pltpu.VMEM((4, HD, 2 * HD), STATE_TYPE),
            pltpu.VMEM((4, HD, 2 * HD), STATE_TYPE),
            pltpu.VMEM((HD, 2 * HD), STATE_TYPE),
            pltpu.VMEM((HD, 2 * HD), STATE_TYPE),
            pltpu.VMEM((4, HD, HD), STATE_TYPE),
            pltpu.VMEM((4, HD, HD), STATE_TYPE),
            pltpu.VMEM((2 * half, 4 * HD), BF16),
            pltpu.VMEM((half, 4 * HD), BF16),
            pltpu.VMEM((half, model), F32),
            pltpu.SemaphoreType.DMA((5, 3)),
            pltpu.SemaphoreType.DMA((5, 3)),
        ],
        compiler_params=params(collective_id=0, has_side_effects=True),
        name="mixed",
    )(maps, z, h, gate, gain, out_w, residual, norm_gain, meta)


def at(ref, fixed):
    return ref.at[tuple(fixed.get(d, slice(None)) for d in range(3))]


def experts_kernel(
    normed_ref, attended_ref, meta_ref, gate_hbm, up_hbm, down_hbm, common_gate_hbm, common_up_hbm, common_down_hbm,
    out_ref,
    buf0, buf1, buf2, buf3, buf4, gate_w, up_w, down_w, common_gate_w, common_up_w, common_down_w,
    code_s, pick_s, acc_s, away_s, here_s,
    send1, recv1, send2, recv2, send3, recv3, free_sem, swap_send, swap_recv, load_sem,
):
    tokens, model = normed_ref.shape
    half = tokens // 2
    chips = 64
    c = lax.axis_index("tp")
    loads = [
        pltpu.make_async_copy(a, b, load_sem.at[i])
        for i, (a, b) in enumerate(
            (
                (common_gate_hbm, common_gate_w),
                (common_up_hbm, common_up_w),
                (common_down_hbm, common_down_w),
                (gate_hbm, gate_w),
                (up_hbm, up_w),
                (down_hbm, down_w),
            )
        )
    ]
    for load in loads:
        load.start()

    coord = [lax.axis_index(a) for a in SP]
    away = [[lax.rem(coord[d] + off, 4) for off in OFFSETS] for d in range(3)]
    back = [[lax.rem(coord[d] + 4 - off, 4) for off in OFFSETS] for d in range(3)]
    forward = (buf0, buf1, buf2, buf3)
    backward = (buf3, buf4, buf1, buf0)

    def dims(way, k):
        return ORDERS[k] if way == 0 else ORDERS[k][::-1]

    def remote(src, dst, send, recv, dim, n):
        return pltpu.make_async_remote_copy(
            src_ref=src,
            dst_ref=dst,
            send_sem=send,
            recv_sem=recv,
            device_id=along(dim, OFFSETS[n]),
            device_id_type=MESH,
        )

    def keep(source, target):
        for i in range(4):
            target[i] = source[i]

    def first(way, k, n):
        bufs = forward if way == 0 else backward
        d1 = dims(way, k)[0]
        return remote(
            at(bufs[0].at[k], {d1: away[d1][n]}),
            at(bufs[1].at[k], {d1: coord[d1]}),
            send1.at[way, k, n],
            recv1.at[way, k, n],
            d1,
            n,
        )

    def second(way, k, m, n):
        bufs = forward if way == 0 else backward
        d1, d2, _ = dims(way, k)
        source = bufs[0] if m == 0 else bufs[1]
        place = coord[d1] if m == 0 else back[d1][m - 1]
        return remote(
            at(source.at[k], {d1: place, d2: away[d2][n]}),
            at(bufs[2].at[k], {d1: place, d2: coord[d2]}),
            send2.at[way, k, m, n],
            recv2.at[way, k, m, n],
            d2,
            n,
        )

    def third(way, k, m, n):
        bufs = forward if way == 0 else backward
        _, d2, d3 = dims(way, k)
        place = coord[d2] if m == 0 else back[d2][m - 1]
        return remote(
            at(bufs[2].at[k], {d2: place, d3: away[d3][n]}),
            at(bufs[3].at[k], {d2: place, d3: coord[d3]}),
            send3.at[way, k, m, n],
            recv3.at[way, k, m, n],
            d3,
            n,
        )

    def start_second(way, k, m):
        bufs = forward if way == 0 else backward
        d1, d2, _ = dims(way, k)
        for n in range(3):
            second(way, k, m, n).start()
        source = bufs[0] if m == 0 else bufs[1]
        place = coord[d1] if m == 0 else back[d1][m - 1]
        keep(at(source.at[k], {d1: place, d2: coord[d2]}), at(bufs[2].at[k], {d1: place, d2: coord[d2]}))

    def start_third(way, k, m):
        bufs = forward if way == 0 else backward
        _, d2, d3 = dims(way, k)
        for n in range(3):
            third(way, k, m, n).start()
        place = coord[d2] if m == 0 else back[d2][m - 1]
        keep(at(bufs[2].at[k], {d2: place, d3: coord[d3]}), at(bufs[3].at[k], {d2: place, d3: coord[d3]}))

    expert = (2 * iota((chips, 1), 0) + c).astype(F32)
    chosen = jnp.zeros((chips, tokens), F32)
    for j in range(TOP_K):
        ids = jnp.concatenate([meta_ref[0, j : j + 1, :], meta_ref[1, j : j + 1, :]], 1)
        chosen = chosen + jnp.where(ids == expert, 1.0, 0.0)
    i, j = iota((tokens, tokens), 0), iota((tokens, tokens), 1)
    same = i // half == j // half
    before = jnp.where(same & (i < j), 1.0, 0.0).astype(BF16)
    slot = mm(chosen.astype(BF16), before)
    shift = jnp.where(iota((chips, tokens), 1) < half, 0.0, float(CAP))
    code_s[...] = jnp.where(chosen > 0.0, slot + shift, -1.0)
    greet((0, 1, 2), True)
    for k in range(3):
        low = 0 if k < 2 else half
        high = half if k == 0 else tokens

        def one(zi, _):
            code = code_s[pl.ds(pl.multiple_of(zi * 16, 16), 16), low:high]
            wanted = (iota((16, 8, high - low), 1) + 8 * k).astype(F32)
            pick = jnp.where(code[:, None, :] == wanted, 1.0, 0.0).reshape(128, high - low).astype(BF16)
            rows = mm(pick, normed_ref[low:high, :]).astype(BF16)
            buf0[k, zi] = rows.reshape(4, 4, 8, model)
            return 0

        lax.fori_loop(0, 4, one, 0)
        for n in range(3):
            first(0, k, n).start()
    for k in range(3):
        start_second(0, k, 0)

    for load in loads[:3]:
        load.wait()
    own = pl.ds(pl.multiple_of(c * half, half), half)
    hidden = silu(mm(normed_ref[own, :], common_gate_w[...])) * mm(normed_ref[own, :], common_up_w[...])
    hidden = hidden.astype(BF16)
    for n in range(model // 512):
        cols = slice(512 * n, 512 * n + 512)
        acc_s[:, cols] = attended_ref[:, cols].astype(F32) + mm(hidden, common_down_w[:, cols])

    for n in range(3):
        for k in range(3):
            first(0, k, n).wait_recv()
            start_second(0, k, n + 1)
    for k in range(3):
        start_third(0, k, 0)

    meta = jnp.concatenate([meta_ref[0], meta_ref[1]], 1).T
    expert = (2 * iota((1, chips), 1) + c).astype(F32)
    chosen = jnp.zeros((tokens, chips), F32)
    weight = jnp.zeros((tokens, chips), F32)
    for q in range(TOP_K):
        hit = meta[:, q : q + 1] == expert
        chosen = chosen + jnp.where(hit, 1.0, 0.0)
        weight = weight + jnp.where(hit, meta[:, TOP_K + q : TOP_K + q + 1], 0.0)
    before = jnp.where(same & (j < i), 1.0, 0.0).astype(BF16)
    slot = mm(before, chosen.astype(BF16))
    shift = jnp.where(iota((tokens, chips), 0) < half, 0.0, float(CAP))
    code = jnp.where(chosen > 0.0, slot + shift, -1.0).astype(BF16)
    spread = jnp.where(iota((chips, 8 * chips), 1) // 8 == iota((chips, 8 * chips), 0), 1.0, 0.0).astype(BF16)
    code = mm(code, spread)
    weight = mm(weight.astype(BF16), spread)
    place = (iota((tokens, 8 * chips), 1) % 8).astype(F32)
    for k in range(3):
        pick_s[k] = jnp.where(code == place + 8.0 * k, weight, 0.0).astype(BF16)

    for n in range(3):
        for k in range(3):
            for m in range(4):
                second(0, k, m, n).wait_recv()
            start_third(0, k, n + 1)
    for k in range(3):
        for n in range(3):
            first(0, k, n).wait_send()
        for m in range(4):
            for n in range(3):
                second(0, k, m, n).wait_send()
        d1, d2, _ = ORDERS[k]
        for off in OFFSETS:
            pl.semaphore_signal(free_sem.at[0, k], inc=1, device_id=along(d2, off), device_id_type=MESH)
            pl.semaphore_signal(free_sem.at[1, k], inc=1, device_id=along(d1, off), device_id_type=MESH)
    for load in loads[3:]:
        load.wait()

    def serve(places):
        views = [at(buf3.at[k], {ORDERS[k][2]: places[k]}) for k in range(3)]
        rows = jnp.concatenate([v[...].reshape(128, model) for v in views], 0)
        hidden = (silu(mm(rows, gate_w[...])) * mm(rows, up_w[...])).astype(BF16)
        for n in range(model // 512):
            cols = slice(512 * n, 512 * n + 512)
            result = mm(hidden, down_w[:, cols]).astype(BF16)
            for k in range(3):
                views[k][:, :, :, cols] = result[128 * k : 128 * k + 128].reshape(4, 4, 8, 512)

    last = [ORDERS[k][2] for k in range(3)]
    serve([coord[d] for d in last])
    for k in range(3):
        pl.semaphore_wait(free_sem.at[0, k], 3)
        start_second(1, k, 0)
    for n in range(3):
        for k in range(3):
            for m in range(4):
                third(0, k, m, n).wait_recv()
        serve([back[d][n] for d in last])
        turned = OFFSETS.index(4 - OFFSETS[n])
        for k in range(3):
            first(1, k, turned).start()
    for n in range(3):
        for k in range(3):
            first(1, k, n).wait_recv()
            start_second(1, k, n + 1)
    for k in range(3):
        pl.semaphore_wait(free_sem.at[1, k], 3)
        start_third(1, k, 0)
    for n in range(3):
        for k in range(3):
            for m in range(4):
                second(1, k, m, n).wait_recv()
            start_third(1, k, n + 1)
    for n in range(3):
        for k in range(3):
            for m in range(4):
                third(1, k, m, n).wait_recv()

    def partial(core, cols):
        rows = pl.ds(pl.multiple_of(core * half, half), half)
        total = mm(pick_s[1, rows, :], buf0[1, :, :, :, :, cols].reshape(8 * chips, 512))
        return total + mm(pick_s[2 * core, rows, :], buf0[2 * core, :, :, :, :, cols].reshape(8 * chips, 512))

    swaps = []
    for n in range(model // 512):
        away_s[n] = partial(1 - c, slice(512 * n, 512 * n + 512))
        swap = pltpu.make_async_remote_copy(
            src_ref=away_s.at[n],
            dst_ref=here_s.at[n],
            send_sem=swap_send.at[n],
            recv_sem=swap_recv.at[n],
            device_id=partner(),
            device_id_type=MESH,
        )
        swap.start()
        swaps.append(swap)
    for n in range(model // 512):
        cols = slice(512 * n, 512 * n + 512)
        acc_s[:, cols] = acc_s[:, cols] + partial(c, cols)
    for n in range(model // 512):
        cols = slice(512 * n, 512 * n + 512)
        swaps[n].wait()
        out_ref[:, cols] = (acc_s[:, cols] + here_s[n]).astype(BF16)

    for k in range(3):
        for m in range(4):
            for n in range(3):
                third(0, k, m, n).wait_send()
                second(1, k, m, n).wait_send()
                third(1, k, m, n).wait_send()
        for n in range(3):
            first(1, k, n).wait_send()


def run_experts(normed, attended, meta, gate, up, down, common_gate, common_up, common_down):
    half, model = attended.shape
    buffer = pltpu.VMEM((3, 4, 4, 4, 8, model), BF16)
    hbm = pl.BlockSpec(memory_space=pl.ANY)
    return pl.pallas_call(
        experts_kernel,
        out_shape=jax.ShapeDtypeStruct((half, model), BF16),
        in_specs=[VMEM] * 3 + [hbm] * 6,
        out_specs=VMEM,
        scratch_shapes=[buffer] * 5
        + [pltpu.VMEM(w.shape, BF16) for w in (gate, up, down, common_gate, common_up, common_down)]
        + [
            pltpu.VMEM((64, 2 * half), F32),
            pltpu.VMEM((3, 2 * half, 512), BF16),
            pltpu.VMEM((half, model), F32),
            pltpu.VMEM((model // 512, half, 512), F32),
            pltpu.VMEM((model // 512, half, 512), F32),
        ]
        + [pltpu.SemaphoreType.DMA((2, 3, 3))] * 2
        + [pltpu.SemaphoreType.DMA((2, 3, 4, 3))] * 4
        + [
            pltpu.SemaphoreType.REGULAR((2, 3)),
            pltpu.SemaphoreType.DMA((model // 512,)),
            pltpu.SemaphoreType.DMA((model // 512,)),
            pltpu.SemaphoreType.DMA((6,)),
        ],
        compiler_params=params(collective_id=1, has_side_effects=True),
        name="experts",
    )(normed, attended, meta, gate, up, down, common_gate, common_up, common_down)


def shards(
    projected_queries,
    projected_keys,
    projected_values,
    output_gate_values,
    write_strength_logits,
    decay_input_logits,
    head_rate_logarithm,
    extra_log_decay,
    per_head_norm_gain,
    output_matrix,
    residual,
    mixture_norm_gain,
    selected_expert_index,
    routing_weight,
    routed_gate_weight,
    routed_up_weight,
    routed_down_weight,
    common_gate_weight,
    common_up_weight,
    common_down_weight,
):
    beta = jax.nn.sigmoid(write_strength_logits.astype(F32))
    decay = extra_log_decay - jnp.exp(head_rate_logarithm)[None, :] * jax.nn.softplus(
        decay_input_logits.astype(F32) - 6.0
    )
    meta = jnp.concatenate([selected_expert_index.T.astype(F32), routing_weight.T], 0)
    maps, z, h = local_terms(projected_queries, projected_keys, projected_values, beta, decay)
    attended, normed, meta = mixed(
        maps,
        z,
        h,
        output_gate_values,
        per_head_norm_gain[None, :],
        output_matrix,
        residual,
        mixture_norm_gain[None, :],
        meta,
    )
    return run_experts(
        normed,
        attended,
        meta,
        routed_gate_weight[0],
        routed_up_weight[0],
        routed_down_weight[0],
        common_gate_weight,
        common_up_weight,
        common_down_weight,
    )


def solution(mesh):
    finer = Mesh(mesh.devices.reshape(4, 4, 4, mesh.shape["tp"]), AXES)
    in_specs = (
        P(SP, "tp"),
        P(SP, "tp"),
        P(SP, "tp"),
        P(SP, "tp"),
        P(SP, "tp"),
        P(SP, "tp"),
        P("tp"),
        P(SP, "tp"),
        P(),
        P(),
        P(AXES, None),
        P(),
        P(AXES, None),
        P(AXES, None),
        P(AXES, None, None),
        P(AXES, None, None),
        P(AXES, None, None),
        P(),
        P(),
        P(),
    )
    return jax.shard_map(
        shards, mesh=finer, in_specs=in_specs, out_specs=P(AXES, None), check_vma=False
    )
```

```python
import functools

import jax
import jax.numpy as jnp
from jax import lax
from jax.experimental import pallas as pl
from jax.experimental.pallas import tpu as pltpu
from jax.sharding import Mesh
from jax.sharding import PartitionSpec as P

TOP_K = 4
SPAN = 64
CAP = 12
HD = 128
AXES = ("sp_0", "sp_1", "sp_2", "tp")
SP = AXES[:3]
EPS = 1e-06
F32, BF16 = jnp.float32, jnp.bfloat16
HIGH = lax.Precision.HIGHEST
MESH = pl.DeviceIdType.MESH
VMEM = pl.BlockSpec(memory_space=pltpu.VMEM)
OFFSETS = (1, 3, 2)
ORDERS = ((2, 1, 0), (1, 0, 2), (0, 2, 1))
STATE_TYPE = BF16


def params(**kw):
    return pltpu.CompilerParams(vmem_limit_bytes=62 * 2**20, **kw)


def mm(a, b, dims=((1,), (0,))):
    return lax.dot_general(a, b, (dims, ((), ())), preferred_element_type=F32)


def halves(x):
    high = x.astype(BF16)
    return high, (x - high.astype(F32)).astype(BF16)


def mm3(a, b, dims=((1,), (0,))):
    high, low = a
    both = mm2(a, b[0], dims)
    return both + mm(high, b[1], dims)


def mm2(a, b, dims=((1,), (0,))):
    rows = a[0].shape[0]
    both = mm(jnp.concatenate(a, 0), b, dims)
    return both[:rows] + both[rows:]


def silu(x):
    return x / (1.0 + jnp.exp(-x))


def iota(shape, dim):
    return lax.broadcasted_iota(jnp.int32, shape, dim)


def along(dim, off):
    at = [lax.axis_index(a) for a in AXES]
    at[dim] = lax.rem(at[dim] + off, 4)
    return tuple(at)


def partner():
    at = [lax.axis_index(a) for a in AXES]
    at[3] = 1 - at[3]
    return tuple(at)


def greet(dims, pair):
    pl.semaphore_wait(pltpu.get_barrier_semaphore(), arrive(dims, pair))


def arrive(dims, pair):
    barrier = pltpu.get_barrier_semaphore()
    count = 0
    for dim in dims:
        for off in OFFSETS:
            pl.semaphore_signal(barrier, inc=1, device_id=along(dim, off), device_id_type=MESH)
            count += 1
    if pair:
        pl.semaphore_signal(barrier, inc=1, device_id=partner(), device_id_type=MESH)
        count += 1
    return count


def attention_kernel(
    q_ref, k_ref, v_ref, strength_ref, input_ref, extra_ref, rate_ref, gate_hbm, gain_ref, out_w_hbm, residual_hbm,
    norm_ref, ids_ref, weight_ref,
    attended_ref, normed_ref, both_meta_ref,
    beta_s, g_s, row_s, low_s, score_s, inv_s, right_s, qd_s, kdt_s, qp_s, step_s, pre_s, z_s, h_s, map_s, meta_s,
    gate_s, out_w_s, residual_s, lit_s, rows_in, plane_in, all_in, row_total, plane_total, state_out, state_in,
    mix_s, mix_in, acc_s, send_sem, recv_sem, load_sem,
):
    heads, tokens = 4, q_ref.shape[0]
    blocks = tokens // SPAN
    loads = [
        pltpu.make_async_copy(src, dst, load_sem.at[i])
        for i, (src, dst) in enumerate(((gate_hbm, gate_s), (residual_hbm, residual_s), (out_w_hbm, out_w_s)))
    ]
    for load in loads:
        load.start()
    greeted = arrive((0, 1, 2), True)
    z, y, x, c = (lax.axis_index(a) for a in AXES)
    meta_s[0:TOP_K, :] = ids_ref[...].astype(F32)
    meta_s[TOP_K : 2 * TOP_K, :] = weight_ref[...]

    i256, j256 = iota((256, 256), 0), iota((256, 256), 1)
    same = (i256 // SPAN) == (j256 // SPAN)
    tri_t = jnp.where(same & (i256 <= j256), 1.0, 0.0)
    ones = jnp.where(same, 1.0, 0.0)

    def high(a, b):
        return lax.dot_general(a, b, (((1,), (0,)), ((), ())), precision=HIGH, preferred_element_type=F32)

    rate = jnp.where(iota((heads, heads), 0) == iota((heads, heads), 1), jnp.exp(rate_ref[...]), 0.0)
    rate = jnp.sum(rate, axis=1, keepdims=True)
    grown = input_ref[...].astype(F32) - 6.0
    tail = jnp.exp(-jnp.abs(grown))
    up = 1.0 + tail
    log_up = jnp.where(up == 1.0, tail, jnp.log(up) * tail / jnp.where(up == 1.0, 1.0, up - 1.0))
    decay = extra_ref[...] - rate * (jnp.maximum(grown, 0.0) + log_up)
    beta = 1.0 / (1.0 + jnp.exp(-strength_ref[...].astype(F32)))
    g_row = jnp.concatenate([high(decay[:, 256 * i : 256 * i + 256], tri_t) for i in range(2)], 1)
    total_row = jnp.concatenate([high(decay[:, 256 * i : 256 * i + 256], ones) for i in range(2)], 1)
    row_s[0:heads, :] = g_row
    row_s[heads : 2 * heads, :] = total_row
    cols = jnp.concatenate([beta, g_row], 0).T
    for h in range(heads):
        beta_s[h] = jnp.broadcast_to(cols[:, h : h + 1], (tokens, HD))
        g_s[h] = jnp.broadcast_to(cols[:, heads + h : heads + h + 1], (tokens, HD))

    row, lane = iota((SPAN, 128), 0), iota((SPAN, 128), 1)
    first = lane < SPAN
    place = lane % SPAN
    causal, strict = row >= place, row > place
    pair_masks = [jnp.where(first, 1.0, 0.0).astype(BF16), jnp.where(first, 0.0, 1.0).astype(BF16)]
    first_wide = iota((128, 128), 1) < SPAN
    eye = jnp.where(iota((128, 128), 0) == iota((128, 128), 1), 1.0, 0.0)

    def prepare(h, _):
        lanes = pl.ds(pl.multiple_of(h * HD, HD), HD)
        q = silu(q_ref[:, lanes].astype(F32))
        q = q * lax.rsqrt(jnp.sum(q * q, axis=-1, keepdims=True) + EPS)
        k = silu(k_ref[:, lanes].astype(F32))
        k = k * lax.rsqrt(jnp.sum(k * k, axis=-1, keepdims=True) + EPS)
        v = silu(v_ref[:, lanes].astype(F32))
        b_h, g_h = beta_s[h], g_s[h]
        grown = jnp.exp(g_h)
        kb = k * b_h
        right_s[h, :, :HD] = (kb * grown).astype(BF16)
        right_s[h, :, HD:] = (v * b_h).astype(BF16)
        qd_s[h] = q * grown
        gr = row_s[pl.ds(h, 1), :]
        kdt_s[h] = k.T * jnp.exp(row_s[pl.ds(h + heads, 1), :] - gr)
        ks, kbs, qs = halves(k), halves(kb), halves(q)
        for j in range(tokens // 128):
            rows = slice(128 * j, 128 * j + 128)
            left = tuple(jnp.concatenate([a[rows], b[rows]], 0) for a, b in zip(kbs, qs))
            both = mm3(left, tuple(a[rows] for a in ks), ((1,), (1,)))
            inner = jnp.where(first, both[0:64], both[64:128])
            score = jnp.where(first, both[128:192], both[192:256])
            gi = jnp.where(first, g_h[128 * j : 128 * j + 64], g_h[128 * j + 64 : 128 * j + 128])
            spread = jnp.where(causal, gi - gr[:, rows], 0.0)
            decay = jnp.where(causal, jnp.exp(spread), 0.0)
            low_s[h, :, rows] = jnp.where(strict, inner * decay, 0.0)
            score_s[h, :, rows] = score * decay
        return 0

    lax.fori_loop(0, heads, prepare, 0)

    r4, l4 = iota((SPAN, 256), 0), iota((SPAN, 256), 1)
    p4 = l4 % SPAN
    quad_masks = [jnp.where(l4 // SPAN == n, 1.0, 0.0).astype(BF16) for n in range(4)]
    eye4 = jnp.where(r4 == p4, 1.0, 0.0)

    def diag4(x):
        return jnp.concatenate([x * m for m in quad_masks], 0)

    def times(a, b):
        return mm3(a, tuple(diag4(x) for x in b))

    def times2(a, b):
        return mm2(a, diag4(b.astype(BF16)))

    def invert(part, _):
        mine = [(2 * part + i // 2, slice(256 * (i % 2), 256 * (i % 2) + 256)) for i in range(4)]
        lows = [low_s[h, :, s] for h, s in mine]
        small = r4 // 8 == p4 // 8
        d1 = [jnp.where(small, x, 0.0) for x in lows]
        d1s = [halves(x) for x in d1]
        d2s = [halves(times(x, x)) for x in d1s]
        x1 = [eye4 - x for x in d1]
        x2 = [x + times(halves(x), d) for x, d in zip(x1, d2s)]
        d4s = [halves(times(d, d)) for d in d2s]
        inv = [x + times(halves(x), d) for x, d in zip(x2, d4s)]
        for size in (8, 16, 32):
            off = (r4 // (2 * size) == p4 // (2 * size)) & (r4 // size != p4 // size)
            ex = [times2(halves(jnp.where(off, x, 0.0)), y) for x, y in zip(lows, inv)]
            inv = [x - times2(halves(x), e) for x, e in zip(inv, ex)]
        for (h, s), x in zip(mine, inv):
            inv_s[h, :, s] = x
        return 0

    lax.fori_loop(0, 2, invert, 0)

    def diag2(x):
        return jnp.concatenate([x * m for m in pair_masks], 0)

    def apply(h, _):
        for j in range(tokens // 128):
            rows = slice(128 * j, 128 * j + 128)
            inv = tuple(diag2(x) for x in halves(inv_s[h, :, rows]))
            wu = mm2(inv, right_s[h, rows, :]).astype(BF16)
            score = [diag2(x) for x in halves(score_s[h, :, rows])]
            kdt = kdt_s[h, :, rows]
            kdt = halves(jnp.concatenate([jnp.where(first_wide, kdt, 0.0), jnp.where(first_wide, 0.0, kdt)], 0))
            left = tuple(jnp.concatenate([a, b], 0) for a, b in zip(score, kdt))
            both = mm2(left, wu)
            qp_s[h, rows, :] = qd_s[h, rows, :] - both[:128, :HD]
            h_s[h, rows, :] = both[:128, HD:]
            change = both[128:]
            for i in range(2):
                n = 2 * j + i
                factor = jnp.exp(g_s[h, n * SPAN + SPAN - 1 : n * SPAN + SPAN, :])
                step_s[h, n, :, :HD] = eye * factor - change[128 * i : 128 * i + 128, :HD]
                step_s[h, n, :, HD:] = change[128 * i : 128 * i + 128, HD:]
        return 0

    lax.fori_loop(0, heads, apply, 0)

    for h in range(heads):
        pre_s[1, h] = step_s[h, 0]

    def grow(n, _):
        for h in range(heads):
            moved = mm3(halves(step_s[h, n, :, :HD]), halves(pre_s[n, h]))
            pre_s[n + 1, h, :, :HD] = moved[:, :HD]
            pre_s[n + 1, h, :, HD:] = moved[:, HD:] + step_s[h, n, :, HD:]
        return 0

    lax.fori_loop(1, blocks, grow, 0)
    for h in range(heads):
        map_s[h] = pre_s[blocks, h].astype(STATE_TYPE)

    def send(stage, dim, source, target):
        copies = []
        here = lax.axis_index(AXES[dim])
        for n, off in enumerate(OFFSETS):
            copies.append(
                pltpu.make_async_remote_copy(
                    src_ref=source(lax.rem(here + off, 4)),
                    dst_ref=target.at[here],
                    send_sem=send_sem.at[stage, n],
                    recv_sem=recv_sem.at[stage, n],
                    device_id=along(dim, off),
                    device_id_type=MESH,
                )
            )
        for copy in copies:
            copy.start()
        return copies

    def moved_by(step, carried):
        high, low = halves(carried)
        moved = mm(step[:, :HD], jnp.concatenate([high, low], 1))
        width = carried.shape[1]
        moved = moved[:, :width] + moved[:, width:]
        if width == HD:
            return moved + step[:, HD:].astype(F32)
        return jnp.concatenate([moved[:, :HD], moved[:, HD:] + step[:, HD:].astype(F32)], 1)

    def total(steps):
        carried = steps[0].astype(F32)
        for i in range(1, 4):
            carried = moved_by(steps[i], carried)
        return carried.astype(STATE_TYPE)

    def outputs(h):
        z_s[h, 0:SPAN, :] = qp_s[h, 0:SPAN, :]
        for n in range(1, blocks):
            rows = slice(SPAN * n, SPAN * n + SPAN)
            moved = mm2(halves(qp_s[h, rows, :]), pre_s[n, h].astype(BF16))
            z_s[h, rows, :] = moved[:, :HD]
            h_s[h, rows, :] = h_s[h, rows, :] + moved[:, HD:]

    def light(h):
        lanes = slice(h * HD, h * HD + HD)
        lit_s[:, lanes] = silu(gate_s[:, lanes].astype(F32)) * gain_ref[...]

    sent = []
    pl.semaphore_wait(pltpu.get_barrier_semaphore(), greeted)
    copies = send(0, 2, lambda t: map_s.at[t], rows_in)
    tell = pltpu.make_async_remote_copy(
        src_ref=meta_s,
        dst_ref=both_meta_ref.at[c],
        send_sem=send_sem.at[4, 2],
        recv_sem=recv_sem.at[4, 2],
        device_id=partner(),
        device_id_type=MESH,
    )
    tell.start()
    both_meta_ref[c] = meta_s[...]
    rows_in[x] = map_s[x]
    for h in range(heads):
        outputs(h)
    for copy in copies:
        copy.wait_recv()
    sent += copies
    row_total[...] = total(rows_in)
    copies = send(1, 1, lambda t: row_total, plane_in)
    plane_in[y] = row_total[...]
    loads[0].wait()
    for h in range(heads):
        light(h)
    for copy in copies:
        copy.wait_recv()
    sent += copies
    plane_total[...] = total(plane_in)
    copies = send(2, 0, lambda t: plane_total, all_in)
    all_in[z] = plane_total[...]
    for copy in copies:
        copy.wait_recv()
    sent += copies
    state = jnp.where(z > 0, all_in[0, :, HD:].astype(F32), 0.0)
    for i in range(1, 3):
        state = jnp.where(i < z, moved_by(all_in[i], state), state)
    for i in range(3):
        state = jnp.where(i < y, moved_by(plane_in[i], state), state)
    state_out[0] = state.astype(STATE_TYPE)
    for i in range(3):
        state = moved_by(rows_in[i], state)
        state_out[i + 1] = state.astype(STATE_TYPE)
    copies = send(3, 2, lambda t: state_out.at[t], state_in)
    state_in[x] = state_out[x]
    for copy in copies:
        copy.wait_recv()
    sent += copies

    for h in range(heads):
        lanes = slice(h * HD, h * HD + HD)
        mix = h_s[h] + mm2(halves(z_s[h]), state_in[h])
        mix = mix * lax.rsqrt(jnp.mean(mix * mix, axis=-1, keepdims=True) + EPS) * lit_s[:, lanes]
        mix_s[:, lanes] = mix.astype(BF16)
    half = tokens // 2
    width = mix_s.shape[1]
    other = 1 - c
    swap = pltpu.make_async_remote_copy(
        src_ref=mix_s.at[pl.ds(pl.multiple_of(other * half, half), half)],
        dst_ref=mix_in,
        send_sem=send_sem.at[4, 0],
        recv_sem=recv_sem.at[4, 0],
        device_id=partner(),
        device_id_type=MESH,
    )
    swap.start()
    for load in loads[1:]:
        load.wait()
    own = pl.ds(pl.multiple_of(c * half, half), half)
    own_w = pl.ds(pl.multiple_of(c * width, width), width)
    other_w = pl.ds(pl.multiple_of(other * width, width), width)
    model = out_w_s.shape[1]
    for n in range(model // 512):
        cols = slice(512 * n, 512 * n + 512)
        acc_s[:, cols] = residual_s[:, cols].astype(F32) + mm(mix_s[own, :], out_w_s[own_w, cols])
    swap.wait()
    squares = jnp.zeros((half, 1), F32)
    for n in range(model // 512):
        cols = slice(512 * n, 512 * n + 512)
        piece = acc_s[:, cols] + mm(mix_in[...], out_w_s[other_w, cols])
        piece = piece.astype(BF16)
        attended_ref[:, cols] = piece
        wide = piece.astype(F32)
        acc_s[:, cols] = wide
        squares = squares + jnp.sum(wide * wide, axis=-1, keepdims=True)
    scale = lax.rsqrt(squares / model + EPS)
    for n in range(model // 512):
        cols = slice(512 * n, 512 * n + 512)
        normed_ref[own, cols] = (acc_s[:, cols] * scale * norm_ref[:, cols]).astype(BF16)
    share = pltpu.make_async_remote_copy(
        src_ref=normed_ref.at[own],
        dst_ref=normed_ref.at[own],
        send_sem=send_sem.at[4, 1],
        recv_sem=recv_sem.at[4, 1],
        device_id=partner(),
        device_id_type=MESH,
    )
    share.start()
    tell.wait()
    share.wait()
    for copy in sent:
        copy.wait_send()


def attention(q, k, v, strength, inputs, extra, rate, gate, gain, out_w, residual, norm_gain, ids, weight):
    half, model = residual.shape
    tokens, heads, blocks = 2 * half, 4, 2 * half // SPAN
    hbm = pl.BlockSpec(memory_space=pl.ANY)
    per_head = pltpu.VMEM((heads, tokens, HD), F32)
    side = pltpu.VMEM((heads, SPAN, tokens), F32)
    maps = pltpu.VMEM((4, HD, 2 * HD), STATE_TYPE)
    return pl.pallas_call(
        attention_kernel,
        out_shape=(
            jax.ShapeDtypeStruct((half, model), BF16),
            jax.ShapeDtypeStruct((tokens, model), BF16),
            jax.ShapeDtypeStruct((2, 2 * TOP_K, half), F32),
        ),
        in_specs=[VMEM] * 7 + [hbm, VMEM, hbm, hbm] + [VMEM] * 3,
        out_specs=(VMEM,) * 3,
        scratch_shapes=[
            per_head,
            per_head,
            pltpu.VMEM((8, tokens), F32),
            side,
            side,
            side,
            pltpu.VMEM((heads, tokens, 2 * HD), BF16),
            per_head,
            pltpu.VMEM((heads, HD, tokens), F32),
            per_head,
            pltpu.VMEM((heads, blocks, HD, 2 * HD), F32),
            pltpu.VMEM((blocks + 1, heads, HD, 2 * HD), F32),
            per_head,
            per_head,
            maps,
            pltpu.VMEM((2 * TOP_K, half), F32),
            pltpu.VMEM((tokens, heads * HD), BF16),
            pltpu.VMEM((2 * heads * HD, model), BF16),
            pltpu.VMEM((half, model), BF16),
            pltpu.VMEM((tokens, heads * HD), F32),
            maps,
            maps,
            maps,
            pltpu.VMEM((HD, 2 * HD), STATE_TYPE),
            pltpu.VMEM((HD, 2 * HD), STATE_TYPE),
            pltpu.VMEM((4, HD, HD), STATE_TYPE),
            pltpu.VMEM((4, HD, HD), STATE_TYPE),
            pltpu.VMEM((tokens, heads * HD), BF16),
            pltpu.VMEM((half, heads * HD), BF16),
            pltpu.VMEM((half, model), F32),
            pltpu.SemaphoreType.DMA((5, 3)),
            pltpu.SemaphoreType.DMA((5, 3)),
            pltpu.SemaphoreType.DMA((3,)),
        ],
        compiler_params=params(collective_id=0, has_side_effects=True),
        name="attention",
    )(q, k, v, strength, inputs, extra, rate, gate, gain, out_w, residual, norm_gain, ids, weight)


def at(ref, fixed):
    return ref.at[tuple(fixed.get(d, slice(None)) for d in range(3))]


def experts_kernel(
    normed_ref, attended_ref, meta_ref, gate_hbm, up_hbm, down_hbm, common_gate_hbm, common_up_hbm, common_down_hbm,
    out_ref,
    buf0, buf1, buf2, buf3, buf4, gate_w, up_w, down_w, common_gate_w, common_up_w, common_down_w,
    code_s, pick_s, acc_s, away_s, here_s,
    send1, recv1, send2, recv2, send3, recv3, free_sem, swap_send, swap_recv, load_sem,
):
    tokens, model = normed_ref.shape
    half = tokens // 2
    chips = 64
    c = lax.axis_index("tp")
    loads = [
        pltpu.make_async_copy(a, b, load_sem.at[i])
        for i, (a, b) in enumerate(
            (
                (common_gate_hbm, common_gate_w),
                (common_up_hbm, common_up_w),
                (common_down_hbm, common_down_w),
                (gate_hbm, gate_w),
                (up_hbm, up_w),
                (down_hbm, down_w),
            )
        )
    ]
    for load in loads:
        load.start()

    coord = [lax.axis_index(a) for a in SP]
    away = [[lax.rem(coord[d] + off, 4) for off in OFFSETS] for d in range(3)]
    back = [[lax.rem(coord[d] + 4 - off, 4) for off in OFFSETS] for d in range(3)]
    forward = (buf0, buf1, buf2, buf3)
    backward = (buf3, buf4, buf1, buf0)

    def dims(way, k):
        return ORDERS[k] if way == 0 else ORDERS[k][::-1]

    def remote(src, dst, send, recv, dim, n):
        return pltpu.make_async_remote_copy(
            src_ref=src,
            dst_ref=dst,
            send_sem=send,
            recv_sem=recv,
            device_id=along(dim, OFFSETS[n]),
            device_id_type=MESH,
        )

    def keep(source, target):
        for i in range(4):
            target[i] = source[i]

    def first(way, k, n):
        bufs = forward if way == 0 else backward
        d1 = dims(way, k)[0]
        return remote(
            at(bufs[0].at[k], {d1: away[d1][n]}),
            at(bufs[1].at[k], {d1: coord[d1]}),
            send1.at[way, k, n],
            recv1.at[way, k, n],
            d1,
            n,
        )

    def second(way, k, m, n):
        bufs = forward if way == 0 else backward
        d1, d2, _ = dims(way, k)
        source = bufs[0] if m == 0 else bufs[1]
        place = coord[d1] if m == 0 else back[d1][m - 1]
        return remote(
            at(source.at[k], {d1: place, d2: away[d2][n]}),
            at(bufs[2].at[k], {d1: place, d2: coord[d2]}),
            send2.at[way, k, m, n],
            recv2.at[way, k, m, n],
            d2,
            n,
        )

    def third(way, k, m, n):
        bufs = forward if way == 0 else backward
        _, d2, d3 = dims(way, k)
        place = coord[d2] if m == 0 else back[d2][m - 1]
        return remote(
            at(bufs[2].at[k], {d2: place, d3: away[d3][n]}),
            at(bufs[3].at[k], {d2: place, d3: coord[d3]}),
            send3.at[way, k, m, n],
            recv3.at[way, k, m, n],
            d3,
            n,
        )

    def start_second(way, k, m):
        bufs = forward if way == 0 else backward
        d1, d2, _ = dims(way, k)
        for n in range(3):
            second(way, k, m, n).start()
        source = bufs[0] if m == 0 else bufs[1]
        place = coord[d1] if m == 0 else back[d1][m - 1]
        keep(at(source.at[k], {d1: place, d2: coord[d2]}), at(bufs[2].at[k], {d1: place, d2: coord[d2]}))

    def start_third(way, k, m):
        bufs = forward if way == 0 else backward
        _, d2, d3 = dims(way, k)
        for n in range(3):
            third(way, k, m, n).start()
        place = coord[d2] if m == 0 else back[d2][m - 1]
        keep(at(bufs[2].at[k], {d2: place, d3: coord[d3]}), at(bufs[3].at[k], {d2: place, d3: coord[d3]}))

    expert = (2 * iota((chips, 1), 0) + c).astype(F32)
    chosen = jnp.zeros((chips, tokens), F32)
    for j in range(TOP_K):
        ids = jnp.concatenate([meta_ref[0, j : j + 1, :], meta_ref[1, j : j + 1, :]], 1)
        chosen = chosen + jnp.where(ids == expert, 1.0, 0.0)
    i, j = iota((tokens, tokens), 0), iota((tokens, tokens), 1)
    same = i // half == j // half
    before = jnp.where(same & (i < j), 1.0, 0.0).astype(BF16)
    slot = mm(chosen.astype(BF16), before)
    shift = jnp.where(iota((chips, tokens), 1) < half, 0.0, float(CAP))
    code_s[...] = jnp.where(chosen > 0.0, slot + shift, -1.0)
    greet((0, 1, 2), True)
    for k in range(3):
        low = 0 if k < 2 else half
        high = half if k == 0 else tokens

        def one(zi, _):
            code = code_s[pl.ds(pl.multiple_of(zi * 16, 16), 16), low:high]
            wanted = (iota((16, 8, high - low), 1) + 8 * k).astype(F32)
            pick = jnp.where(code[:, None, :] == wanted, 1.0, 0.0).reshape(128, high - low).astype(BF16)
            rows = mm(pick, normed_ref[low:high, :]).astype(BF16)
            buf0[k, zi] = rows.reshape(4, 4, 8, model)
            return 0

        lax.fori_loop(0, 4, one, 0)
        for n in range(3):
            first(0, k, n).start()
    for k in range(3):
        start_second(0, k, 0)

    for load in loads[:3]:
        load.wait()
    own = pl.ds(pl.multiple_of(c * half, half), half)
    hidden = silu(mm(normed_ref[own, :], common_gate_w[...])) * mm(normed_ref[own, :], common_up_w[...])
    hidden = hidden.astype(BF16)
    for n in range(model // 512):
        cols = slice(512 * n, 512 * n + 512)
        acc_s[:, cols] = attended_ref[:, cols].astype(F32) + mm(hidden, common_down_w[:, cols])

    for n in range(3):
        for k in range(3):
            first(0, k, n).wait_recv()
            start_second(0, k, n + 1)
    for k in range(3):
        start_third(0, k, 0)

    meta = jnp.concatenate([meta_ref[0], meta_ref[1]], 1).T
    expert = (2 * iota((1, chips), 1) + c).astype(F32)
    chosen = jnp.zeros((tokens, chips), F32)
    weight = jnp.zeros((tokens, chips), F32)
    for q in range(TOP_K):
        hit = meta[:, q : q + 1] == expert
        chosen = chosen + jnp.where(hit, 1.0, 0.0)
        weight = weight + jnp.where(hit, meta[:, TOP_K + q : TOP_K + q + 1], 0.0)
    before = jnp.where(same & (j < i), 1.0, 0.0).astype(BF16)
    slot = mm(before, chosen.astype(BF16))
    shift = jnp.where(iota((tokens, chips), 0) < half, 0.0, float(CAP))
    code = jnp.where(chosen > 0.0, slot + shift, -1.0).astype(BF16)
    spread = jnp.where(iota((chips, 8 * chips), 1) // 8 == iota((chips, 8 * chips), 0), 1.0, 0.0).astype(BF16)
    code = mm(code, spread)
    weight = mm(weight.astype(BF16), spread)
    place = (iota((tokens, 8 * chips), 1) % 8).astype(F32)
    for k in range(3):
        pick_s[k] = jnp.where(code == place + 8.0 * k, weight, 0.0).astype(BF16)

    for n in range(3):
        for k in range(3):
            for m in range(4):
                second(0, k, m, n).wait_recv()
            start_third(0, k, n + 1)
    for k in range(3):
        for n in range(3):
            first(0, k, n).wait_send()
        for m in range(4):
            for n in range(3):
                second(0, k, m, n).wait_send()
        d1, d2, _ = ORDERS[k]
        for off in OFFSETS:
            pl.semaphore_signal(free_sem.at[0, k], inc=1, device_id=along(d2, off), device_id_type=MESH)
            pl.semaphore_signal(free_sem.at[1, k], inc=1, device_id=along(d1, off), device_id_type=MESH)
    for load in loads[3:]:
        load.wait()

    def serve(places):
        views = [at(buf3.at[k], {ORDERS[k][2]: places[k]}) for k in range(3)]
        rows = jnp.concatenate([v[...].reshape(128, model) for v in views], 0)
        hidden = (silu(mm(rows, gate_w[...])) * mm(rows, up_w[...])).astype(BF16)
        for n in range(model // 512):
            cols = slice(512 * n, 512 * n + 512)
            result = mm(hidden, down_w[:, cols]).astype(BF16)
            for k in range(3):
                views[k][:, :, :, cols] = result[128 * k : 128 * k + 128].reshape(4, 4, 8, 512)

    last = [ORDERS[k][2] for k in range(3)]
    serve([coord[d] for d in last])
    for k in range(3):
        pl.semaphore_wait(free_sem.at[0, k], 3)
        start_second(1, k, 0)
    for n in range(3):
        for k in range(3):
            for m in range(4):
                third(0, k, m, n).wait_recv()
        serve([back[d][n] for d in last])
        turned = OFFSETS.index(4 - OFFSETS[n])
        for k in range(3):
            first(1, k, turned).start()
    for n in range(3):
        for k in range(3):
            first(1, k, n).wait_recv()
            start_second(1, k, n + 1)
    for k in range(3):
        pl.semaphore_wait(free_sem.at[1, k], 3)
        start_third(1, k, 0)
    for n in range(3):
        for k in range(3):
            for m in range(4):
                second(1, k, m, n).wait_recv()
            start_third(1, k, n + 1)
    for n in range(3):
        for k in range(3):
            for m in range(4):
                third(1, k, m, n).wait_recv()

    def partial(core, cols):
        rows = pl.ds(pl.multiple_of(core * half, half), half)
        total = mm(pick_s[1, rows, :], buf0[1, :, :, :, :, cols].reshape(8 * chips, 512))
        return total + mm(pick_s[2 * core, rows, :], buf0[2 * core, :, :, :, :, cols].reshape(8 * chips, 512))

    swaps = []
    for n in range(model // 512):
        away_s[n] = partial(1 - c, slice(512 * n, 512 * n + 512))
        swap = pltpu.make_async_remote_copy(
            src_ref=away_s.at[n],
            dst_ref=here_s.at[n],
            send_sem=swap_send.at[n],
            recv_sem=swap_recv.at[n],
            device_id=partner(),
            device_id_type=MESH,
        )
        swap.start()
        swaps.append(swap)
    for n in range(model // 512):
        cols = slice(512 * n, 512 * n + 512)
        acc_s[:, cols] = acc_s[:, cols] + partial(c, cols)
    for n in range(model // 512):
        cols = slice(512 * n, 512 * n + 512)
        swaps[n].wait()
        out_ref[:, cols] = (acc_s[:, cols] + here_s[n]).astype(BF16)

    for k in range(3):
        for m in range(4):
            for n in range(3):
                third(0, k, m, n).wait_send()
                second(1, k, m, n).wait_send()
                third(1, k, m, n).wait_send()
        for n in range(3):
            first(1, k, n).wait_send()


def run_experts(normed, attended, meta, gate, up, down, common_gate, common_up, common_down):
    half, model = attended.shape
    buffer = pltpu.VMEM((3, 4, 4, 4, 8, model), BF16)
    hbm = pl.BlockSpec(memory_space=pl.ANY)
    return pl.pallas_call(
        experts_kernel,
        out_shape=jax.ShapeDtypeStruct((half, model), BF16),
        in_specs=[VMEM] * 3 + [hbm] * 6,
        out_specs=VMEM,
        scratch_shapes=[buffer] * 5
        + [pltpu.VMEM(w.shape, BF16) for w in (gate, up, down, common_gate, common_up, common_down)]
        + [
            pltpu.VMEM((64, 2 * half), F32),
            pltpu.VMEM((3, 2 * half, 512), BF16),
            pltpu.VMEM((half, model), F32),
            pltpu.VMEM((model // 512, half, 512), F32),
            pltpu.VMEM((model // 512, half, 512), F32),
        ]
        + [pltpu.SemaphoreType.DMA((2, 3, 3))] * 2
        + [pltpu.SemaphoreType.DMA((2, 3, 4, 3))] * 4
        + [
            pltpu.SemaphoreType.REGULAR((2, 3)),
            pltpu.SemaphoreType.DMA((model // 512,)),
            pltpu.SemaphoreType.DMA((model // 512,)),
            pltpu.SemaphoreType.DMA((6,)),
        ],
        compiler_params=params(collective_id=1, has_side_effects=True),
        name="experts",
    )(normed, attended, meta, gate, up, down, common_gate, common_up, common_down)


def shards(
    projected_queries,
    projected_keys,
    projected_values,
    output_gate_values,
    write_strength_logits,
    decay_input_logits,
    head_rate_logarithm,
    extra_log_decay,
    per_head_norm_gain,
    output_matrix,
    residual,
    mixture_norm_gain,
    selected_expert_index,
    routing_weight,
    routed_gate_weight,
    routed_up_weight,
    routed_down_weight,
    common_gate_weight,
    common_up_weight,
    common_down_weight,
):
    attended, normed, meta = attention(
        projected_queries,
        projected_keys,
        projected_values,
        write_strength_logits.T,
        decay_input_logits.T,
        extra_log_decay.T,
        head_rate_logarithm[None, :],
        output_gate_values,
        per_head_norm_gain[None, :],
        output_matrix,
        residual,
        mixture_norm_gain[None, :],
        selected_expert_index.T,
        routing_weight.T,
    )
    return run_experts(
        normed,
        attended,
        meta,
        routed_gate_weight[0],
        routed_up_weight[0],
        routed_down_weight[0],
        common_gate_weight,
        common_up_weight,
        common_down_weight,
    )


def solution(mesh):
    finer = Mesh(mesh.devices.reshape(4, 4, 4, mesh.shape["tp"]), AXES)
    in_specs = (
        P(SP, "tp"),
        P(SP, "tp"),
        P(SP, "tp"),
        P(SP, "tp"),
        P(SP, "tp"),
        P(SP, "tp"),
        P("tp"),
        P(SP, "tp"),
        P(),
        P(),
        P(AXES, None),
        P(),
        P(AXES, None),
        P(AXES, None),
        P(AXES, None, None),
        P(AXES, None, None),
        P(AXES, None, None),
        P(),
        P(),
        P(),
    )
    return jax.shard_map(
        shards, mesh=finer, in_specs=in_specs, out_specs=P(AXES, None), check_vma=False
    )
```

```python
import functools

import jax
import jax.numpy as jnp
from jax import lax
from jax.experimental import pallas as pl
from jax.experimental.pallas import tpu as pltpu
from jax.sharding import Mesh
from jax.sharding import PartitionSpec as P

TOP_K = 4
SPAN = 64
CAP = 12
HD = 128
AXES = ("sp_0", "sp_1", "sp_2", "tp")
SP = AXES[:3]
EPS = 1e-06
F32, BF16 = jnp.float32, jnp.bfloat16
HIGH = lax.Precision.HIGHEST
MESH = pl.DeviceIdType.MESH
VMEM = pl.BlockSpec(memory_space=pltpu.VMEM)
OFFSETS = (1, 3, 2)
ORDERS = ((2, 1, 0), (1, 0, 2), (0, 2, 1))
STATE_TYPE = BF16


def params(**kw):
    return pltpu.CompilerParams(vmem_limit_bytes=62 * 2**20, **kw)


def mm(a, b, dims=((1,), (0,))):
    return lax.dot_general(a, b, (dims, ((), ())), preferred_element_type=F32)


def halves(x):
    high = x.astype(BF16)
    return high, (x - high.astype(F32)).astype(BF16)


def mm3(a, b, dims=((1,), (0,))):
    high, low = a
    both = mm2(a, b[0], dims)
    return both + mm(high, b[1], dims)


def mm2(a, b, dims=((1,), (0,))):
    rows = a[0].shape[0]
    if a[0].shape[1] == HD:
        return mm(jnp.concatenate(a, 1), jnp.concatenate([b, b], dims[1][0]), dims)
    both = mm(jnp.concatenate(a, 0), b, dims)
    return both[:rows] + both[rows:]


def silu(x):
    return (0.5 * x) * (1.0 + jnp.tanh(0.5 * x))


def iota(shape, dim):
    return lax.broadcasted_iota(jnp.int32, shape, dim)


def along(dim, off):
    at = [lax.axis_index(a) for a in AXES]
    at[dim] = lax.rem(at[dim] + off, 4)
    return tuple(at)


def partner():
    at = [lax.axis_index(a) for a in AXES]
    at[3] = 1 - at[3]
    return tuple(at)


def greet(dims, pair):
    pl.semaphore_wait(pltpu.get_barrier_semaphore(), arrive(dims, pair))


def arrive(dims, pair):
    barrier = pltpu.get_barrier_semaphore()
    count = 0
    for dim in dims:
        for off in OFFSETS:
            pl.semaphore_signal(barrier, inc=1, device_id=along(dim, off), device_id_type=MESH)
            count += 1
    if pair:
        pl.semaphore_signal(barrier, inc=1, device_id=partner(), device_id_type=MESH)
        count += 1
    return count


def attention_kernel(
    q_ref, k_ref, v_ref, strength_ref, input_ref, extra_ref, rate_ref, gate_hbm, gain_ref, out_w_hbm, residual_hbm,
    norm_ref, ids_ref, weight_ref,
    attended_ref, normed_ref, both_meta_ref, code_ref,
    beta_s, g_s, row_s, low_s, score_s, inv_s, right_s, qd_s, kdt_s, qp_s, step_s, pair_s, pre_s, span_s, z_s, h_s, map_s, meta_s,
    gate_s, out_w_s, residual_s, lit_s, rows_in, plane_in, all_in, row_total, plane_total, state_out, state_in,
    mix_s, mix_in, acc_s, send_sem, recv_sem, share_send, share_recv, load_sem,
):
    heads, tokens = 4, q_ref.shape[0]
    blocks = tokens // SPAN
    loads = [
        pltpu.make_async_copy(src, dst, load_sem.at[i])
        for i, (src, dst) in enumerate(((gate_hbm, gate_s), (residual_hbm, residual_s), (out_w_hbm, out_w_s)))
    ]
    for load in loads:
        load.start()
    greeted = arrive((0, 1, 2), True)
    z, y, x, c = (lax.axis_index(a) for a in AXES)
    meta_s[0:TOP_K, :] = ids_ref[...].astype(F32)
    meta_s[TOP_K : 2 * TOP_K, :] = weight_ref[...]

    i256, j256 = iota((256, 256), 0), iota((256, 256), 1)
    same = (i256 // SPAN) == (j256 // SPAN)
    tri_t = jnp.where(same & (i256 <= j256), 1.0, 0.0)
    ones = jnp.where(same, 1.0, 0.0)

    def high(a, b):
        return lax.dot_general(a, b, (((1,), (0,)), ((), ())), precision=HIGH, preferred_element_type=F32)

    rate = jnp.where(iota((heads, heads), 0) == iota((heads, heads), 1), jnp.exp(rate_ref[...]), 0.0)
    rate = jnp.sum(rate, axis=1, keepdims=True)
    grown = input_ref[...].astype(F32) - 6.0
    tail = jnp.exp(-jnp.abs(grown))
    up = 1.0 + tail
    log_up = jnp.where(up == 1.0, tail, jnp.log(up) * tail / jnp.where(up == 1.0, 1.0, up - 1.0))
    decay = extra_ref[...] - rate * (jnp.maximum(grown, 0.0) + log_up)
    beta = 1.0 / (1.0 + jnp.exp(-strength_ref[...].astype(F32)))
    g_row = jnp.concatenate([high(decay[:, 256 * i : 256 * i + 256], tri_t) for i in range(2)], 1)
    total_row = jnp.concatenate([high(decay[:, 256 * i : 256 * i + 256], ones) for i in range(2)], 1)
    row_s[0:heads, :] = g_row
    row_s[heads : 2 * heads, :] = total_row
    cols = jnp.concatenate([beta, g_row], 0).T
    for h in range(heads):
        beta_s[h] = jnp.broadcast_to(cols[:, h : h + 1], (tokens, HD))
        g_s[h] = jnp.broadcast_to(cols[:, heads + h : heads + h + 1], (tokens, HD))

    row, lane = iota((SPAN, 128), 0), iota((SPAN, 128), 1)
    first = lane < SPAN
    place = lane % SPAN
    causal, strict = row >= place, row > place
    pair_masks = [jnp.where(first, 1.0, 0.0).astype(BF16), jnp.where(first, 0.0, 1.0).astype(BF16)]
    first_wide = iota((128, 128), 1) < SPAN
    eye = jnp.where(iota((128, 128), 0) == iota((128, 128), 1), 1.0, 0.0)

    def prepare(h, _):
        lanes = pl.ds(pl.multiple_of(h * HD, HD), HD)
        q = silu(q_ref[:, lanes].astype(F32))
        q = q * lax.rsqrt(jnp.sum(q * q, axis=-1, keepdims=True) + EPS)
        k = silu(k_ref[:, lanes].astype(F32))
        k = k * lax.rsqrt(jnp.sum(k * k, axis=-1, keepdims=True) + EPS)
        v = silu(v_ref[:, lanes].astype(F32))
        b_h, g_h = beta_s[h], g_s[h]
        grown = jnp.exp(g_h)
        kb = k * b_h
        right_s[h, :, :HD] = (kb * grown).astype(BF16)
        right_s[h, :, HD:] = (v * b_h).astype(BF16)
        qd_s[h] = q * grown
        gr = row_s[pl.ds(h, 1), :]
        kdt_s[h] = k.T * jnp.exp(row_s[pl.ds(h + heads, 1), :] - gr)
        ks, kbs, qs = halves(k), halves(kb), halves(q)
        for j in range(tokens // 128):
            rows = slice(128 * j, 128 * j + 128)
            left = tuple(jnp.concatenate([a[rows], b[rows]], 0) for a, b in zip(kbs, qs))
            both = mm3(left, tuple(a[rows] for a in ks), ((1,), (1,)))
            inner = jnp.where(first, both[0:64], both[64:128])
            score = jnp.where(first, both[128:192], both[192:256])
            gi = jnp.where(first, g_h[128 * j : 128 * j + 64], g_h[128 * j + 64 : 128 * j + 128])
            spread = jnp.where(causal, gi - gr[:, rows], 0.0)
            decay = jnp.where(causal, jnp.exp(spread), 0.0)
            low_s[h, :, rows] = jnp.where(strict, inner * decay, 0.0)
            score_s[h, :, rows] = score * decay
        return 0

    lax.fori_loop(0, heads, prepare, 0)

    r4, l4 = iota((SPAN, 256), 0), iota((SPAN, 256), 1)
    p4 = l4 % SPAN
    quad_masks = [jnp.where(l4 // SPAN == n, 1.0, 0.0).astype(BF16) for n in range(4)]
    eye4 = jnp.where(r4 == p4, 1.0, 0.0)

    def diag4(x):
        return jnp.concatenate([x * m for m in quad_masks], 0)

    def times(a, b):
        return mm3(a, tuple(diag4(x) for x in b))

    def times2(a, b):
        return mm2(a, diag4(b.astype(BF16)))

    def invert():
        mine = [(i // 2, slice(256 * (i % 2), 256 * (i % 2) + 256)) for i in range(8)]
        lows = [low_s[h, :, s] for h, s in mine]
        small = r4 // 8 == p4 // 8
        d1 = [jnp.where(small, x, 0.0) for x in lows]
        d1s = [halves(x) for x in d1]
        d2s = [halves(times(x, x)) for x in d1s]
        x1 = [eye4 - x for x in d1]
        x2 = [x + times(halves(x), d) for x, d in zip(x1, d2s)]
        d4s = [halves(times(d, d)) for d in d2s]
        inv = [x + times(halves(x), d) for x, d in zip(x2, d4s)]
        for size in (8, 16, 32):
            off = (r4 // (2 * size) == p4 // (2 * size)) & (r4 // size != p4 // size)
            ex = [times2(halves(jnp.where(off, x, 0.0)), y) for x, y in zip(lows, inv)]
            inv = [x - times2(halves(x), e) for x, e in zip(inv, ex)]
        for (h, s), x in zip(mine, inv):
            inv_s[h, :, s] = x

    invert()

    def diag2(x):
        return jnp.concatenate([x * m for m in pair_masks], 0)

    def apply(h, _):
        for j in range(tokens // 128):
            rows = slice(128 * j, 128 * j + 128)
            inv = tuple(diag2(x) for x in halves(inv_s[h, :, rows]))
            wu = mm2(inv, right_s[h, rows, :]).astype(BF16)
            score = [diag2(x) for x in halves(score_s[h, :, rows])]
            kdt = kdt_s[h, :, rows]
            kdt = halves(jnp.concatenate([jnp.where(first_wide, kdt, 0.0), jnp.where(first_wide, 0.0, kdt)], 0))
            left = tuple(jnp.concatenate([a, b], 0) for a, b in zip(score, kdt))
            both = mm2(left, wu)
            qp_s[h, rows, :] = qd_s[h, rows, :] - both[:128, :HD]
            h_s[h, rows, :] = both[:128, HD:]
            change = both[128:]
            for i in range(2):
                n = 2 * j + i
                factor = jnp.exp(g_s[h, n * SPAN + SPAN - 1 : n * SPAN + SPAN, :])
                step_s[h, n, :, :HD] = eye * factor - change[128 * i : 128 * i + 128, :HD]
                step_s[h, n, :, HD:] = change[128 * i : 128 * i + 128, HD:]
        return 0

    lax.fori_loop(0, heads, apply, 0)

    def compose(later, earlier):
        moved = mm3(halves(later[:, :HD]), halves(earlier))
        return jnp.concatenate([moved[:, :HD], moved[:, HD:] + later[:, HD:]], 1)

    def pairs(i, _):
        for h in range(heads):
            pair_s[i, h] = compose(step_s[h, 2 * i + 1], step_s[h, 2 * i])
        return 0

    lax.fori_loop(0, 4, pairs, 0)
    for h in range(heads):
        pre_s[4, h] = compose(pair_s[1, h], pair_s[0, h])
        pair_s[4, h] = compose(pair_s[3, h], pair_s[2, h])
    for h in range(heads):
        map_s[h] = compose(pair_s[4, h], pre_s[4, h]).astype(STATE_TYPE)

    def send(stage, dim, source, target):
        copies = []
        here = lax.axis_index(AXES[dim])
        for n, off in enumerate(OFFSETS):
            copies.append(
                pltpu.make_async_remote_copy(
                    src_ref=source(lax.rem(here + off, 4)),
                    dst_ref=target.at[here],
                    send_sem=send_sem.at[stage, n],
                    recv_sem=recv_sem.at[stage, n],
                    device_id=along(dim, off),
                    device_id_type=MESH,
                )
            )
        for n in (2, 0, 1):
            copies[n].start()
        return copies

    def moved_by(step, carried):
        high, low = halves(carried)
        moved = mm(step[:, :HD], jnp.concatenate([high, low], 1))
        width = carried.shape[1]
        moved = moved[:, :width] + moved[:, width:]
        if width == HD:
            return moved + step[:, HD:].astype(F32)
        return jnp.concatenate([moved[:, :HD], moved[:, HD:] + step[:, HD:].astype(F32)], 1)

    def outputs(h):
        pre_s[1, h] = step_s[h, 0]
        pre_s[2, h] = pair_s[0, h]
        pre_s[3, h] = compose(step_s[h, 2], pair_s[0, h])
        pre_s[5, h] = compose(step_s[h, 4], pre_s[4, h])
        pre_s[6, h] = compose(pair_s[2, h], pre_s[4, h])
        pre_s[7, h] = compose(step_s[h, 6], pre_s[6, h])
        z_s[h, 0:SPAN, :] = qp_s[h, 0:SPAN, :]
        for n in range(1, blocks):
            rows = slice(SPAN * n, SPAN * n + SPAN)
            moved = mm2(halves(qp_s[h, rows, :]), pre_s[n, h].astype(BF16))
            z_s[h, rows, :] = moved[:, :HD]
            h_s[h, rows, :] = h_s[h, rows, :] + moved[:, HD:]

    def light(h):
        lanes = slice(h * HD, h * HD + HD)
        lit_s[:, lanes] = silu(gate_s[:, lanes].astype(F32)) * gain_ref[...]

    sent = []
    pl.semaphore_wait(pltpu.get_barrier_semaphore(), greeted)
    copies = send(0, 2, lambda t: map_s.at[t], rows_in)
    tell = pltpu.make_async_remote_copy(
        src_ref=meta_s,
        dst_ref=both_meta_ref.at[c],
        send_sem=send_sem.at[4, 2],
        recv_sem=recv_sem.at[4, 2],
        device_id=partner(),
        device_id_type=MESH,
    )
    tell.start()
    both_meta_ref[c] = meta_s[...]
    rows_in[x] = map_s[x]
    for h in range(heads):
        outputs(h)
    for copy in copies:
        copy.wait_recv()
    sent += copies
    low_pair = moved_by(rows_in[1], rows_in[0].astype(F32))
    high_pair = moved_by(rows_in[3], rows_in[2].astype(F32))
    span_s[2] = low_pair
    row_total[...] = compose(high_pair, low_pair).astype(STATE_TYPE)
    copies = send(1, 1, lambda t: row_total, plane_in)
    plane_in[y] = row_total[...]
    span_s[1] = rows_in[0].astype(F32)
    span_s[3] = moved_by(rows_in[2], span_s[2])
    loads[0].wait()
    for h in range(heads):
        light(h)
    for copy in copies:
        copy.wait_recv()
    sent += copies
    low_pair = moved_by(plane_in[1], plane_in[0].astype(F32))
    high_pair = moved_by(plane_in[3], plane_in[2].astype(F32))
    plane_total[...] = compose(high_pair, low_pair).astype(STATE_TYPE)
    copies = send(2, 0, lambda t: plane_total, all_in)
    all_in[z] = plane_total[...]
    entry = jnp.where(y == 1, plane_in[0].astype(F32), jnp.concatenate([eye, jnp.zeros((HD, HD), F32)], 1))
    entry = jnp.where(y == 2, low_pair, entry)
    entry = jnp.where(y == 3, moved_by(plane_in[2], low_pair), entry)
    span_s[0] = entry
    for i in range(1, 4):
        span_s[i] = compose(span_s[i], entry)

    tell.wait()
    chips = code_ref.shape[0]
    expert = (2 * iota((chips, 1), 0) + c).astype(F32)
    chosen = jnp.zeros((chips, tokens), F32)
    for j in range(TOP_K):
        ids = jnp.concatenate([both_meta_ref[0, j : j + 1, :], both_meta_ref[1, j : j + 1, :]], 1)
        chosen = chosen + jnp.where(ids == expert, 1.0, 0.0)
    i512, j512 = iota((tokens, tokens), 0), iota((tokens, tokens), 1)
    half = tokens // 2
    before = jnp.where((i512 // half == j512 // half) & (i512 < j512), 1.0, 0.0).astype(BF16)
    slot = mm(chosen.astype(BF16), before)
    shift = jnp.where(iota((chips, tokens), 1) < half, 0.0, float(CAP))
    code_ref[...] = jnp.where(chosen > 0.0, slot + shift, -1.0)

    for copy in copies:
        copy.wait_recv()
    sent += copies
    state = jnp.where(z > 0, all_in[0, :, HD:].astype(F32), 0.0)
    for i in range(1, 3):
        state = jnp.where(i < z, moved_by(all_in[i], state), state)
    state = halves(state)
    for i in range(4):
        entering = mm3(halves(span_s[i, :, :HD]), state) + span_s[i, :, HD:]
        state_out[i] = entering.astype(STATE_TYPE)
    copies = send(3, 2, lambda t: state_out.at[t], state_in)
    state_in[x] = state_out[x]
    for copy in copies:
        copy.wait_recv()
    sent += copies

    for h in range(heads):
        lanes = slice(h * HD, h * HD + HD)
        mix = h_s[h] + mm2(halves(z_s[h]), state_in[h])
        mix = mix * lax.rsqrt(jnp.mean(mix * mix, axis=-1, keepdims=True) + EPS) * lit_s[:, lanes]
        mix_s[:, lanes] = mix.astype(BF16)
    width = mix_s.shape[1]
    other = 1 - c
    swap = pltpu.make_async_remote_copy(
        src_ref=mix_s.at[pl.ds(pl.multiple_of(other * half, half), half)],
        dst_ref=mix_in,
        send_sem=send_sem.at[4, 0],
        recv_sem=recv_sem.at[4, 0],
        device_id=partner(),
        device_id_type=MESH,
    )
    swap.start()
    for load in loads[1:]:
        load.wait()
    own = pl.ds(pl.multiple_of(c * half, half), half)
    own_w = pl.ds(pl.multiple_of(c * width, width), width)
    other_w = pl.ds(pl.multiple_of(other * width, width), width)
    model = out_w_s.shape[1]
    for n in range(model // 512):
        cols = slice(512 * n, 512 * n + 512)
        acc_s[:, cols] = residual_s[:, cols].astype(F32) + mm(mix_s[own, :], out_w_s[own_w, cols])
    swap.wait()
    squares = jnp.zeros((half, 1), F32)
    for n in range(model // 512):
        cols = slice(512 * n, 512 * n + 512)
        piece = acc_s[:, cols] + mm(mix_in[...], out_w_s[other_w, cols])
        piece = piece.astype(BF16)
        attended_ref[:, cols] = piece
        wide = piece.astype(F32)
        acc_s[:, cols] = wide
        squares = squares + jnp.sum(wide * wide, axis=-1, keepdims=True)
    scale = lax.rsqrt(squares / model + EPS)
    shares = []
    for n in range(model // 512):
        cols = slice(512 * n, 512 * n + 512)
        normed_ref[own, cols] = (acc_s[:, cols] * scale * norm_ref[:, cols]).astype(BF16)
        share = pltpu.make_async_remote_copy(
            src_ref=normed_ref.at[own, cols],
            dst_ref=normed_ref.at[own, cols],
            send_sem=share_send.at[n],
            recv_sem=share_recv.at[n],
            device_id=partner(),
            device_id_type=MESH,
        )
        share.start()
        shares.append(share)
    for share in shares:
        share.wait()
    for copy in sent:
        copy.wait_send()


def attention(q, k, v, strength, inputs, extra, rate, gate, gain, out_w, residual, norm_gain, ids, weight):
    half, model = residual.shape
    tokens, heads, blocks = 2 * half, 4, 2 * half // SPAN
    hbm = pl.BlockSpec(memory_space=pl.ANY)
    per_head = pltpu.VMEM((heads, tokens, HD), F32)
    side = pltpu.VMEM((heads, SPAN, tokens), F32)
    maps = pltpu.VMEM((4, HD, 2 * HD), STATE_TYPE)
    return pl.pallas_call(
        attention_kernel,
        out_shape=(
            jax.ShapeDtypeStruct((half, model), BF16),
            jax.ShapeDtypeStruct((tokens, model), BF16),
            jax.ShapeDtypeStruct((2, 2 * TOP_K, half), F32),
            jax.ShapeDtypeStruct((64, tokens), F32),
        ),
        in_specs=[VMEM] * 7 + [hbm, VMEM, hbm, hbm] + [VMEM] * 3,
        out_specs=(VMEM,) * 4,
        scratch_shapes=[
            per_head,
            per_head,
            pltpu.VMEM((8, tokens), F32),
            side,
            side,
            side,
            pltpu.VMEM((heads, tokens, 2 * HD), BF16),
            per_head,
            pltpu.VMEM((heads, HD, tokens), F32),
            per_head,
            pltpu.VMEM((heads, blocks, HD, 2 * HD), F32),
            pltpu.VMEM((5, heads, HD, 2 * HD), F32),
            pltpu.VMEM((blocks, heads, HD, 2 * HD), F32),
            pltpu.VMEM((4, HD, 2 * HD), F32),
            per_head,
            per_head,
            maps,
            pltpu.VMEM((2 * TOP_K, half), F32),
            pltpu.VMEM((tokens, heads * HD), BF16),
            pltpu.VMEM((2 * heads * HD, model), BF16),
            pltpu.VMEM((half, model), BF16),
            pltpu.VMEM((tokens, heads * HD), F32),
            maps,
            maps,
            maps,
            pltpu.VMEM((HD, 2 * HD), STATE_TYPE),
            pltpu.VMEM((HD, 2 * HD), STATE_TYPE),
            pltpu.VMEM((4, HD, HD), STATE_TYPE),
            pltpu.VMEM((4, HD, HD), STATE_TYPE),
            pltpu.VMEM((tokens, heads * HD), BF16),
            pltpu.VMEM((half, heads * HD), BF16),
            pltpu.VMEM((half, model), F32),
            pltpu.SemaphoreType.DMA((5, 3)),
            pltpu.SemaphoreType.DMA((5, 3)),
            pltpu.SemaphoreType.DMA((4,)),
            pltpu.SemaphoreType.DMA((4,)),
            pltpu.SemaphoreType.DMA((3,)),
        ],
        compiler_params=params(collective_id=0, has_side_effects=True),
        name="attention",
    )(q, k, v, strength, inputs, extra, rate, gate, gain, out_w, residual, norm_gain, ids, weight)


def at(ref, fixed):
    return ref.at[tuple(fixed.get(d, slice(None)) for d in range(3))]


def experts_kernel(
    normed_ref, attended_hbm, meta_ref, code_ref, gate_hbm, up_hbm, down_hbm, common_gate_hbm, common_up_hbm, common_down_hbm,
    out_ref,
    buf0, buf1, buf2, buf3, buf4, gate_w, up_w, down_w, common_gate_w, common_up_w, common_down_w,
    attended_s, pick_s, acc_s, away_s, here_s,
    send1, recv1, send2, recv2, send3, recv3, free_sem, swap_send, swap_recv, load_sem,
):
    tokens, model = normed_ref.shape
    half = tokens // 2
    chips = 64
    c = lax.axis_index("tp")
    loads = [
        pltpu.make_async_copy(a, b, load_sem.at[i])
        for i, (a, b) in enumerate(
            (
                (attended_hbm, attended_s),
                (common_gate_hbm, common_gate_w),
                (common_up_hbm, common_up_w),
                (common_down_hbm, common_down_w),
                (gate_hbm, gate_w),
                (up_hbm, up_w),
                (down_hbm, down_w),
            )
        )
    ]
    for load in loads:
        load.start()

    coord = [lax.axis_index(a) for a in SP]
    away = [[lax.rem(coord[d] + off, 4) for off in OFFSETS] for d in range(3)]
    back = [[lax.rem(coord[d] + 4 - off, 4) for off in OFFSETS] for d in range(3)]
    forward = (buf0, buf1, buf2, buf3)
    backward = (buf3, buf4, buf1, buf0)

    def dims(way, k):
        return ORDERS[k] if way == 0 else ORDERS[k][::-1]

    def remote(src, dst, send, recv, dim, n):
        return pltpu.make_async_remote_copy(
            src_ref=src,
            dst_ref=dst,
            send_sem=send,
            recv_sem=recv,
            device_id=along(dim, OFFSETS[n]),
            device_id_type=MESH,
        )

    def keep(source, target):
        for i in range(4):
            target[i] = source[i]

    def first(way, k, n):
        bufs = forward if way == 0 else backward
        d1 = dims(way, k)[0]
        return remote(
            at(bufs[0].at[k], {d1: away[d1][n]}),
            at(bufs[1].at[k], {d1: coord[d1]}),
            send1.at[way, k, n],
            recv1.at[way, k, n],
            d1,
            n,
        )

    def second(way, k, m, n):
        bufs = forward if way == 0 else backward
        d1, d2, _ = dims(way, k)
        source = bufs[0] if m == 0 else bufs[1]
        place = coord[d1] if m == 0 else back[d1][m - 1]
        return remote(
            at(source.at[k], {d1: place, d2: away[d2][n]}),
            at(bufs[2].at[k], {d1: place, d2: coord[d2]}),
            send2.at[way, k, m, n],
            recv2.at[way, k, m, n],
            d2,
            n,
        )

    def third(way, k, m, n):
        bufs = forward if way == 0 else backward
        _, d2, d3 = dims(way, k)
        place = coord[d2] if m == 0 else back[d2][m - 1]
        return remote(
            at(bufs[2].at[k], {d2: place, d3: away[d3][n]}),
            at(bufs[3].at[k], {d2: place, d3: coord[d3]}),
            send3.at[way, k, m, n],
            recv3.at[way, k, m, n],
            d3,
            n,
        )

    def start_second(way, k, m):
        bufs = forward if way == 0 else backward
        d1, d2, _ = dims(way, k)
        for n in range(3):
            second(way, k, m, n).start()
        source = bufs[0] if m == 0 else bufs[1]
        place = coord[d1] if m == 0 else back[d1][m - 1]
        keep(at(source.at[k], {d1: place, d2: coord[d2]}), at(bufs[2].at[k], {d1: place, d2: coord[d2]}))

    def start_third(way, k, m):
        bufs = forward if way == 0 else backward
        _, d2, d3 = dims(way, k)
        for n in range(3):
            third(way, k, m, n).start()
        place = coord[d2] if m == 0 else back[d2][m - 1]
        keep(at(bufs[2].at[k], {d2: place, d3: coord[d3]}), at(bufs[3].at[k], {d2: place, d3: coord[d3]}))

    greet((0, 1, 2), True)
    for k in (0, 2, 1):
        low = 0 if k < 2 else half
        high = half if k == 0 else tokens
        wanted = (iota((chips, 8, high - low), 1) + 8 * k).astype(F32)
        pick = jnp.where(code_ref[:, low:high][:, None, :] == wanted, 1.0, 0.0)
        pick = pick.reshape(8 * chips, high - low).astype(BF16)
        for n in range(model // 512):
            cols = slice(512 * n, 512 * n + 512)
            rows = mm(pick, normed_ref[low:high, cols]).astype(BF16)
            buf0[k, :, :, :, :, cols] = rows.reshape(4, 4, 4, 8, 512)
        for n in range(3):
            first(0, k, n).start()
    for k in range(3):
        start_second(0, k, 0)

    for load in loads[:4]:
        load.wait()
    own = pl.ds(pl.multiple_of(c * half, half), half)
    hidden = silu(mm(normed_ref[own, :], common_gate_w[...])) * mm(normed_ref[own, :], common_up_w[...])
    hidden = hidden.astype(BF16)
    for n in range(model // 512):
        cols = slice(512 * n, 512 * n + 512)
        acc_s[:, cols] = attended_s[:, cols].astype(F32) + mm(hidden, common_down_w[:, cols])

    for n in range(3):
        for k in range(3):
            first(0, k, n).wait_recv()
            start_second(0, k, n + 1)
    for k in range(3):
        start_third(0, k, 0)

    meta = jnp.concatenate([meta_ref[0], meta_ref[1]], 1).T
    expert = (2 * iota((1, chips), 1) + c).astype(F32)
    chosen = jnp.zeros((tokens, chips), F32)
    weight = jnp.zeros((tokens, chips), F32)
    for q in range(TOP_K):
        hit = meta[:, q : q + 1] == expert
        chosen = chosen + jnp.where(hit, 1.0, 0.0)
        weight = weight + jnp.where(hit, meta[:, TOP_K + q : TOP_K + q + 1], 0.0)
    i, j = iota((tokens, tokens), 0), iota((tokens, tokens), 1)
    before = jnp.where((i // half == j // half) & (j < i), 1.0, 0.0).astype(BF16)
    slot = mm(before, chosen.astype(BF16))
    shift = jnp.where(iota((tokens, chips), 0) < half, 0.0, float(CAP))
    code = jnp.where(chosen > 0.0, slot + shift, -1.0).astype(BF16)
    spread = jnp.where(iota((chips, 8 * chips), 1) // 8 == iota((chips, 8 * chips), 0), 1.0, 0.0).astype(BF16)
    code = mm(code, spread)
    weight = mm(weight.astype(BF16), spread)
    place = (iota((tokens, 8 * chips), 1) % 8).astype(F32)
    for k in range(3):
        pick_s[k] = jnp.where(code == place + 8.0 * k, weight, 0.0).astype(BF16)

    for n in range(3):
        for k in range(3):
            for m in range(4):
                second(0, k, m, n).wait_recv()
            start_third(0, k, n + 1)
    for k in range(3):
        for n in range(3):
            first(0, k, n).wait_send()
        for m in range(4):
            for n in range(3):
                second(0, k, m, n).wait_send()
        d1, d2, _ = ORDERS[k]
        for off in OFFSETS:
            pl.semaphore_signal(free_sem.at[0, k], inc=1, device_id=along(d2, off), device_id_type=MESH)
            pl.semaphore_signal(free_sem.at[1, k], inc=1, device_id=along(d1, off), device_id_type=MESH)
    for load in loads[4:]:
        load.wait()

    def serve(places):
        views = [at(buf3.at[k], {ORDERS[k][2]: places[k]}) for k in range(3)]
        rows = jnp.concatenate([v[...].reshape(128, model) for v in views], 0)
        hidden = (silu(mm(rows, gate_w[...])) * mm(rows, up_w[...])).astype(BF16)
        for n in range(model // 512):
            cols = slice(512 * n, 512 * n + 512)
            result = mm(hidden, down_w[:, cols]).astype(BF16)
            for k in range(3):
                views[k][:, :, :, cols] = result[128 * k : 128 * k + 128].reshape(4, 4, 8, 512)

    last = [ORDERS[k][2] for k in range(3)]
    serve([coord[d] for d in last])
    for k in range(3):
        pl.semaphore_wait(free_sem.at[0, k], 3)
        start_second(1, k, 0)
    for n in range(3):
        for k in range(3):
            for m in range(4):
                third(0, k, m, n).wait_recv()
        serve([back[d][n] for d in last])
        turned = OFFSETS.index(4 - OFFSETS[n])
        for k in range(3):
            first(1, k, turned).start()
    for n in range(3):
        for k in range(3):
            first(1, k, n).wait_recv()
            start_second(1, k, n + 1)
    for k in range(3):
        pl.semaphore_wait(free_sem.at[1, k], 3)
        start_third(1, k, 0)
    for n in range(3):
        for k in range(3):
            for m in range(4):
                second(1, k, m, n).wait_recv()
            start_third(1, k, n + 1)
    for n in range(3):
        for k in range(3):
            for m in range(4):
                third(1, k, m, n).wait_recv()

    def partial(core, cols):
        rows = pl.ds(pl.multiple_of(core * half, half), half)
        total = mm(pick_s[1, rows, :], buf0[1, :, :, :, :, cols].reshape(8 * chips, 512))
        return total + mm(pick_s[2 * core, rows, :], buf0[2 * core, :, :, :, :, cols].reshape(8 * chips, 512))

    swaps = []
    for n in range(model // 512):
        away_s[n] = partial(1 - c, slice(512 * n, 512 * n + 512))
        swap = pltpu.make_async_remote_copy(
            src_ref=away_s.at[n],
            dst_ref=here_s.at[n],
            send_sem=swap_send.at[n],
            recv_sem=swap_recv.at[n],
            device_id=partner(),
            device_id_type=MESH,
        )
        swap.start()
        swaps.append(swap)
    for n in range(model // 512):
        cols = slice(512 * n, 512 * n + 512)
        acc_s[:, cols] = acc_s[:, cols] + partial(c, cols)
    for n in range(model // 512):
        cols = slice(512 * n, 512 * n + 512)
        swaps[n].wait()
        out_ref[:, cols] = (acc_s[:, cols] + here_s[n]).astype(BF16)

    for k in range(3):
        for m in range(4):
            for n in range(3):
                third(0, k, m, n).wait_send()
                second(1, k, m, n).wait_send()
                third(1, k, m, n).wait_send()
        for n in range(3):
            first(1, k, n).wait_send()


def run_experts(normed, attended, meta, code, gate, up, down, common_gate, common_up, common_down):
    half, model = attended.shape
    buffer = pltpu.VMEM((3, 4, 4, 4, 8, model), BF16)
    hbm = pl.BlockSpec(memory_space=pl.ANY)
    return pl.pallas_call(
        experts_kernel,
        out_shape=jax.ShapeDtypeStruct((half, model), BF16),
        in_specs=[VMEM, hbm, VMEM, VMEM] + [hbm] * 6,
        out_specs=VMEM,
        scratch_shapes=[buffer] * 5
        + [pltpu.VMEM(w.shape, BF16) for w in (gate, up, down, common_gate, common_up, common_down)]
        + [
            pltpu.VMEM((half, model), BF16),
            pltpu.VMEM((3, 2 * half, 512), BF16),
            pltpu.VMEM((half, model), F32),
            pltpu.VMEM((model // 512, half, 512), F32),
            pltpu.VMEM((model // 512, half, 512), F32),
        ]
        + [pltpu.SemaphoreType.DMA((2, 3, 3))] * 2
        + [pltpu.SemaphoreType.DMA((2, 3, 4, 3))] * 4
        + [
            pltpu.SemaphoreType.REGULAR((2, 3)),
            pltpu.SemaphoreType.DMA((model // 512,)),
            pltpu.SemaphoreType.DMA((model // 512,)),
            pltpu.SemaphoreType.DMA((7,)),
        ],
        compiler_params=params(collective_id=1, has_side_effects=True),
        name="experts",
    )(normed, attended, meta, code, gate, up, down, common_gate, common_up, common_down)


def shards(
    projected_queries,
    projected_keys,
    projected_values,
    output_gate_values,
    write_strength_logits,
    decay_input_logits,
    head_rate_logarithm,
    extra_log_decay,
    per_head_norm_gain,
    output_matrix,
    residual,
    mixture_norm_gain,
    selected_expert_index,
    routing_weight,
    routed_gate_weight,
    routed_up_weight,
    routed_down_weight,
    common_gate_weight,
    common_up_weight,
    common_down_weight,
):
    attended, normed, meta, code = attention(
        projected_queries,
        projected_keys,
        projected_values,
        write_strength_logits.T,
        decay_input_logits.T,
        extra_log_decay.T,
        head_rate_logarithm[None, :],
        output_gate_values,
        per_head_norm_gain[None, :],
        output_matrix,
        residual,
        mixture_norm_gain[None, :],
        selected_expert_index.T,
        routing_weight.T,
    )
    return run_experts(
        normed,
        attended,
        meta,
        code,
        routed_gate_weight[0],
        routed_up_weight[0],
        routed_down_weight[0],
        common_gate_weight,
        common_up_weight,
        common_down_weight,
    )


def solution(mesh):
    finer = Mesh(mesh.devices.reshape(4, 4, 4, mesh.shape["tp"]), AXES)
    in_specs = (
        P(SP, "tp"),
        P(SP, "tp"),
        P(SP, "tp"),
        P(SP, "tp"),
        P(SP, "tp"),
        P(SP, "tp"),
        P("tp"),
        P(SP, "tp"),
        P(),
        P(),
        P(AXES, None),
        P(),
        P(AXES, None),
        P(AXES, None),
        P(AXES, None, None),
        P(AXES, None, None),
        P(AXES, None, None),
        P(),
        P(),
        P(),
    )
    return jax.shard_map(
        shards, mesh=finer, in_specs=in_specs, out_specs=P(AXES, None), check_vma=False
    )
```

```python
import functools

import jax
import jax.numpy as jnp
from jax import lax
from jax.experimental import pallas as pl
from jax.experimental.pallas import tpu as pltpu
from jax.sharding import Mesh
from jax.sharding import PartitionSpec as P

TOP_K = 4
SPAN = 64
CAP = 12
HD = 128
AXES = ("sp_0", "sp_1", "sp_2", "tp")
SP = AXES[:3]
EPS = 1e-06
F32, BF16 = jnp.float32, jnp.bfloat16
HIGH = lax.Precision.HIGHEST
MESH = pl.DeviceIdType.MESH
VMEM = pl.BlockSpec(memory_space=pltpu.VMEM)
OFFSETS = (1, 3, 2)
ORDERS = ((2, 1, 0), (1, 0, 2), (0, 2, 1))
STATE_TYPE = BF16


def params(**kw):
    return pltpu.CompilerParams(vmem_limit_bytes=62 * 2**20, **kw)


def mm(a, b, dims=((1,), (0,))):
    return lax.dot_general(a, b, (dims, ((), ())), preferred_element_type=F32)


def halves(x):
    high = x.astype(BF16)
    return high, (x - high.astype(F32)).astype(BF16)


def mm3(a, b, dims=((1,), (0,))):
    high, low = a
    both = mm2(a, b[0], dims)
    return both + mm(high, b[1], dims)


def mm2(a, b, dims=((1,), (0,))):
    rows = a[0].shape[0]
    if a[0].shape[1] == HD:
        return mm(jnp.concatenate(a, 1), jnp.concatenate([b, b], dims[1][0]), dims)
    both = mm(jnp.concatenate(a, 0), b, dims)
    return both[:rows] + both[rows:]


def silu(x):
    return (0.5 * x) * (1.0 + jnp.tanh(0.5 * x))


def iota(shape, dim):
    return lax.broadcasted_iota(jnp.int32, shape, dim)


def along(dim, off):
    at = [lax.axis_index(a) for a in AXES]
    at[dim] = lax.rem(at[dim] + off, 4)
    return tuple(at)


def partner():
    at = [lax.axis_index(a) for a in AXES]
    at[3] = 1 - at[3]
    return tuple(at)


def arrive(dims, pair):
    barrier = pltpu.get_barrier_semaphore()
    count = 0
    for dim in dims:
        for off in OFFSETS:
            pl.semaphore_signal(barrier, inc=1, device_id=along(dim, off), device_id_type=MESH)
            count += 1
    if pair:
        pl.semaphore_signal(barrier, inc=1, device_id=partner(), device_id_type=MESH)
        count += 1
    return count


def attention_kernel(
    q_ref, k_ref, v_ref, strength_ref, input_ref, extra_ref, rate_ref, gate_hbm, gain_ref, out_w_hbm, residual_hbm,
    norm_ref, ids_ref, weight_ref,
    attended_ref, normed_ref, both_meta_ref, code_ref,
    beta_s, g_s, row_s, low_s, decay_s, inv_s, right_s, kk_s, wu_s, kdt_s, qp_s, step_s, pair_s, pre_s, span_s, z_s, h_s, map_s, meta_s,
    gate_s, out_w_s, residual_s, lit_s, rows_in, plane_in, all_in, row_total, plane_total, state_out, state_in,
    mix_s, mix_in, acc_s, send_sem, recv_sem, share_send, share_recv, load_sem,
):
    heads, tokens = 4, q_ref.shape[0]
    blocks = tokens // SPAN
    loads = [
        pltpu.make_async_copy(src, dst, load_sem.at[i])
        for i, (src, dst) in enumerate(((gate_hbm, gate_s), (residual_hbm, residual_s), (out_w_hbm, out_w_s)))
    ]
    for load in loads:
        load.start()
    greeted = arrive((0, 1, 2), True)
    z, y, x, c = (lax.axis_index(a) for a in AXES)
    meta_s[0:TOP_K, :] = ids_ref[...].astype(F32)
    meta_s[TOP_K : 2 * TOP_K, :] = weight_ref[...]

    i256, j256 = iota((256, 256), 0), iota((256, 256), 1)
    same = (i256 // SPAN) == (j256 // SPAN)
    tri_t = jnp.where(same & (i256 <= j256), 1.0, 0.0)
    ones = jnp.where(same, 1.0, 0.0)

    def high(a, b):
        return lax.dot_general(a, b, (((1,), (0,)), ((), ())), precision=HIGH, preferred_element_type=F32)

    rate = jnp.where(iota((heads, heads), 0) == iota((heads, heads), 1), jnp.exp(rate_ref[...]), 0.0)
    rate = jnp.sum(rate, axis=1, keepdims=True)
    grown = input_ref[...].astype(F32) - 6.0
    tail = jnp.exp(-jnp.abs(grown))
    up = 1.0 + tail
    log_up = jnp.where(up == 1.0, tail, jnp.log(up) * tail / jnp.where(up == 1.0, 1.0, up - 1.0))
    decay = extra_ref[...] - rate * (jnp.maximum(grown, 0.0) + log_up)
    beta = 1.0 / (1.0 + jnp.exp(-strength_ref[...].astype(F32)))
    g_row = jnp.concatenate([high(decay[:, 256 * i : 256 * i + 256], tri_t) for i in range(2)], 1)
    total_row = jnp.concatenate([high(decay[:, 256 * i : 256 * i + 256], ones) for i in range(2)], 1)
    row_s[0:heads, :] = g_row
    row_s[heads : 2 * heads, :] = total_row
    cols = jnp.concatenate([beta, g_row], 0).T
    for h in range(heads):
        beta_s[h] = jnp.broadcast_to(cols[:, h : h + 1], (tokens, HD))
        g_s[h] = jnp.broadcast_to(cols[:, heads + h : heads + h + 1], (tokens, HD))

    row, lane = iota((SPAN, 128), 0), iota((SPAN, 128), 1)
    first = lane < SPAN
    place = lane % SPAN
    causal, strict = row >= place, row > place
    pair_masks = [jnp.where(first, 1.0, 0.0).astype(BF16), jnp.where(first, 0.0, 1.0).astype(BF16)]
    first_wide = iota((128, 128), 1) < SPAN
    eye = jnp.where(iota((128, 128), 0) == iota((128, 128), 1), 1.0, 0.0)

    def prepare(h, _):
        lanes = pl.ds(pl.multiple_of(h * HD, HD), HD)
        k = silu(k_ref[:, lanes].astype(F32))
        k = k * lax.rsqrt(jnp.sum(k * k, axis=-1, keepdims=True) + EPS)
        v = silu(v_ref[:, lanes].astype(F32))
        b_h, g_h = beta_s[h], g_s[h]
        grown = jnp.exp(g_h)
        kb = k * b_h
        right_s[h, :, :HD] = (kb * grown).astype(BF16)
        right_s[h, :, HD:] = (v * b_h).astype(BF16)
        gr = row_s[pl.ds(h, 1), :]
        kdt_s[h] = k.T * jnp.exp(row_s[pl.ds(h + heads, 1), :] - gr)
        ks, kbs = halves(k), halves(kb)
        kk_s[h, :, :HD] = ks[0]
        kk_s[h, :, HD:] = ks[1]
        for j in range(tokens // 128):
            rows = slice(128 * j, 128 * j + 128)
            both = mm3(tuple(a[rows] for a in kbs), tuple(a[rows] for a in ks), ((1,), (1,)))
            inner = jnp.where(first, both[0:64], both[64:128])
            gi = jnp.where(first, g_h[128 * j : 128 * j + 64], g_h[128 * j + 64 : 128 * j + 128])
            spread = jnp.where(causal, gi - gr[:, rows], 0.0)
            decay = jnp.where(causal, jnp.exp(spread), 0.0)
            low_s[h, :, rows] = jnp.where(strict, inner * decay, 0.0)
            decay_s[h, :, rows] = decay
        return 0

    lax.fori_loop(0, heads, prepare, 0)

    r4, l4 = iota((SPAN, 256), 0), iota((SPAN, 256), 1)
    p4 = l4 % SPAN
    quad_masks = [jnp.where(l4 // SPAN == n, 1.0, 0.0).astype(BF16) for n in range(4)]
    eye4 = jnp.where(r4 == p4, 1.0, 0.0)

    def diag4(x):
        return jnp.concatenate([x * m for m in quad_masks], 0)

    def times(a, b):
        return mm3(a, tuple(diag4(x) for x in b))

    def times2(a, b):
        return mm2(a, diag4(b.astype(BF16)))

    def invert():
        mine = [(i // 2, slice(256 * (i % 2), 256 * (i % 2) + 256)) for i in range(8)]
        lows = [low_s[h, :, s] for h, s in mine]
        small = r4 // 8 == p4 // 8
        d1 = [jnp.where(small, x, 0.0) for x in lows]
        d1s = [halves(x) for x in d1]
        d2s = [halves(times(x, x)) for x in d1s]
        x1 = [eye4 - x for x in d1]
        x2 = [x + times(halves(x), d) for x, d in zip(x1, d2s)]
        d4s = [halves(times(d, d)) for d in d2s]
        inv = [x + times(halves(x), d) for x, d in zip(x2, d4s)]
        for size in (8, 16, 32):
            off = (r4 // (2 * size) == p4 // (2 * size)) & (r4 // size != p4 // size)
            ex = [times2(halves(jnp.where(off, x, 0.0)), y) for x, y in zip(lows, inv)]
            inv = [x - times2(halves(x), e) for x, e in zip(inv, ex)]
        for (h, s), x in zip(mine, inv):
            inv_s[h, :, s] = x

    invert()

    def diag2(x):
        return jnp.concatenate([x * m for m in pair_masks], 0)

    def apply(h, _):
        for j in range(tokens // 128):
            rows = slice(128 * j, 128 * j + 128)
            inv = tuple(diag2(x) for x in halves(inv_s[h, :, rows]))
            wu = mm2(inv, right_s[h, rows, :]).astype(BF16)
            wu_s[h, rows, :] = wu
            kdt = kdt_s[h, :, rows]
            kdt = halves(jnp.concatenate([jnp.where(first_wide, kdt, 0.0), jnp.where(first_wide, 0.0, kdt)], 0))
            change = mm2(kdt, wu)
            for i in range(2):
                n = 2 * j + i
                factor = jnp.exp(g_s[h, n * SPAN + SPAN - 1 : n * SPAN + SPAN, :])
                step_s[h, n, :, :HD] = eye * factor - change[128 * i : 128 * i + 128, :HD]
                step_s[h, n, :, HD:] = change[128 * i : 128 * i + 128, HD:]
        return 0

    lax.fori_loop(0, heads, apply, 0)

    def compose(later, earlier):
        moved = mm3(halves(later[:, :HD]), halves(earlier))
        return jnp.concatenate([moved[:, :HD], moved[:, HD:] + later[:, HD:]], 1)

    def pairs(i, _):
        for h in range(heads):
            pair_s[i, h] = compose(step_s[h, 2 * i + 1], step_s[h, 2 * i])
        return 0

    lax.fori_loop(0, 4, pairs, 0)
    for h in range(heads):
        pre_s[4, h] = compose(pair_s[1, h], pair_s[0, h])
        pair_s[4, h] = compose(pair_s[3, h], pair_s[2, h])
    for h in range(heads):
        map_s[h] = compose(pair_s[4, h], pre_s[4, h]).astype(STATE_TYPE)

    def send(stage, dim, source, target):
        copies = []
        here = lax.axis_index(AXES[dim])
        for n, off in enumerate(OFFSETS):
            copies.append(
                pltpu.make_async_remote_copy(
                    src_ref=source(lax.rem(here + off, 4)),
                    dst_ref=target.at[here],
                    send_sem=send_sem.at[stage, n],
                    recv_sem=recv_sem.at[stage, n],
                    device_id=along(dim, off),
                    device_id_type=MESH,
                )
            )
        for n in (2, 0, 1):
            copies[n].start()
        return copies

    def moved_by(step, carried):
        high, low = halves(carried)
        moved = mm(step[:, :HD], jnp.concatenate([high, low], 1))
        width = carried.shape[1]
        moved = moved[:, :width] + moved[:, width:]
        if width == HD:
            return moved + step[:, HD:].astype(F32)
        return jnp.concatenate([moved[:, :HD], moved[:, HD:] + step[:, HD:].astype(F32)], 1)

    def scores(h, _):
        lanes = pl.ds(pl.multiple_of(h * HD, HD), HD)
        q = silu(q_ref[:, lanes].astype(F32))
        q = q * lax.rsqrt(jnp.sum(q * q, axis=-1, keepdims=True) + EPS)
        qd = q * jnp.exp(g_s[h])
        qs = halves(q)
        for j in range(tokens // 128):
            rows = slice(128 * j, 128 * j + 128)
            ks = (kk_s[h, rows, :HD], kk_s[h, rows, HD:])
            both = mm3(tuple(a[rows] for a in qs), ks, ((1,), (1,)))
            score = jnp.where(first, both[0:64], both[64:128]) * decay_s[h, :, rows]
            both = mm2(tuple(diag2(x) for x in halves(score)), wu_s[h, rows, :])
            qp_s[h, rows, :] = qd[rows] - both[:, :HD]
            h_s[h, rows, :] = both[:, HD:]
        return 0

    def outputs(h):
        pre_s[1, h] = step_s[h, 0]
        pre_s[2, h] = pair_s[0, h]
        pre_s[3, h] = compose(step_s[h, 2], pair_s[0, h])
        pre_s[5, h] = compose(step_s[h, 4], pre_s[4, h])
        pre_s[6, h] = compose(pair_s[2, h], pre_s[4, h])
        pre_s[7, h] = compose(step_s[h, 6], pre_s[6, h])
        z_s[h, 0:SPAN, :] = qp_s[h, 0:SPAN, :]
        for n in range(1, blocks):
            rows = slice(SPAN * n, SPAN * n + SPAN)
            moved = mm2(halves(qp_s[h, rows, :]), pre_s[n, h].astype(BF16))
            z_s[h, rows, :] = moved[:, :HD]
            h_s[h, rows, :] = h_s[h, rows, :] + moved[:, HD:]

    def light(h):
        lanes = slice(h * HD, h * HD + HD)
        lit_s[:, lanes] = silu(gate_s[:, lanes].astype(F32)) * gain_ref[...]

    sent = []
    pl.semaphore_wait(pltpu.get_barrier_semaphore(), greeted)
    copies = send(0, 2, lambda t: map_s.at[t], rows_in)
    tell = pltpu.make_async_remote_copy(
        src_ref=meta_s,
        dst_ref=both_meta_ref.at[c],
        send_sem=send_sem.at[4, 2],
        recv_sem=recv_sem.at[4, 2],
        device_id=partner(),
        device_id_type=MESH,
    )
    tell.start()
    both_meta_ref[c] = meta_s[...]
    rows_in[x] = map_s[x]
    lax.fori_loop(0, heads, scores, 0)
    for copy in copies:
        copy.wait_recv()
    sent += copies
    low_pair = moved_by(rows_in[1], rows_in[0].astype(F32))
    high_pair = moved_by(rows_in[3], rows_in[2].astype(F32))
    span_s[2] = low_pair
    row_total[...] = compose(high_pair, low_pair).astype(STATE_TYPE)
    copies = send(1, 1, lambda t: row_total, plane_in)
    plane_in[y] = row_total[...]
    span_s[1] = rows_in[0].astype(F32)
    span_s[3] = moved_by(rows_in[2], span_s[2])
    loads[0].wait()
    for h in range(heads):
        light(h)
        outputs(h)
    for copy in copies:
        copy.wait_recv()
    sent += copies
    low_pair = moved_by(plane_in[1], plane_in[0].astype(F32))
    high_pair = moved_by(plane_in[3], plane_in[2].astype(F32))
    plane_total[...] = compose(high_pair, low_pair).astype(STATE_TYPE)
    copies = send(2, 0, lambda t: plane_total, all_in)
    all_in[z] = plane_total[...]
    entry = jnp.where(y == 1, plane_in[0].astype(F32), jnp.concatenate([eye, jnp.zeros((HD, HD), F32)], 1))
    entry = jnp.where(y == 2, low_pair, entry)
    entry = jnp.where(y == 3, moved_by(plane_in[2], low_pair), entry)
    span_s[0] = entry
    for i in range(1, 4):
        span_s[i] = compose(span_s[i], entry)

    tell.wait()
    chips = code_ref.shape[0]
    expert = (2 * iota((chips, 1), 0) + c).astype(F32)
    chosen = jnp.zeros((chips, tokens), F32)
    for j in range(TOP_K):
        ids = jnp.concatenate([both_meta_ref[0, j : j + 1, :], both_meta_ref[1, j : j + 1, :]], 1)
        chosen = chosen + jnp.where(ids == expert, 1.0, 0.0)
    i512, j512 = iota((tokens, tokens), 0), iota((tokens, tokens), 1)
    half = tokens // 2
    before = jnp.where((i512 // half == j512 // half) & (i512 < j512), 1.0, 0.0).astype(BF16)
    slot = mm(chosen.astype(BF16), before)
    shift = jnp.where(iota((chips, tokens), 1) < half, 0.0, float(CAP))
    code_ref[...] = jnp.where(chosen > 0.0, slot + shift, -1.0)

    for copy in copies:
        copy.wait_recv()
    sent += copies
    state = jnp.where(z > 0, all_in[0, :, HD:].astype(F32), 0.0)
    for i in range(1, 3):
        state = jnp.where(i < z, moved_by(all_in[i], state), state)
    state = halves(state)
    for i in range(4):
        entering = mm3(halves(span_s[i, :, :HD]), state) + span_s[i, :, HD:]
        state_out[i] = entering.astype(STATE_TYPE)
    copies = send(3, 2, lambda t: state_out.at[t], state_in)
    state_in[x] = state_out[x]
    for copy in copies:
        copy.wait_recv()
    sent += copies

    for h in range(heads):
        lanes = slice(h * HD, h * HD + HD)
        mix = h_s[h] + mm2(halves(z_s[h]), state_in[h])
        mix = mix * lax.rsqrt(jnp.mean(mix * mix, axis=-1, keepdims=True) + EPS) * lit_s[:, lanes]
        mix_s[:, lanes] = mix.astype(BF16)
    width = mix_s.shape[1]
    other = 1 - c
    swap = pltpu.make_async_remote_copy(
        src_ref=mix_s.at[pl.ds(pl.multiple_of(other * half, half), half)],
        dst_ref=mix_in,
        send_sem=send_sem.at[4, 0],
        recv_sem=recv_sem.at[4, 0],
        device_id=partner(),
        device_id_type=MESH,
    )
    swap.start()
    for load in loads[1:]:
        load.wait()
    own = pl.ds(pl.multiple_of(c * half, half), half)
    own_w = pl.ds(pl.multiple_of(c * width, width), width)
    other_w = pl.ds(pl.multiple_of(other * width, width), width)
    model = out_w_s.shape[1]
    for n in range(model // 512):
        cols = slice(512 * n, 512 * n + 512)
        acc_s[:, cols] = residual_s[:, cols].astype(F32) + mm(mix_s[own, :], out_w_s[own_w, cols])
    swap.wait()
    squares = jnp.zeros((half, 1), F32)
    for n in range(model // 512):
        cols = slice(512 * n, 512 * n + 512)
        piece = acc_s[:, cols] + mm(mix_in[...], out_w_s[other_w, cols])
        piece = piece.astype(BF16)
        attended_ref[:, cols] = piece
        wide = piece.astype(F32)
        acc_s[:, cols] = wide
        squares = squares + jnp.sum(wide * wide, axis=-1, keepdims=True)
    scale = lax.rsqrt(squares / model + EPS)
    shares = []
    for n in range(model // 512):
        cols = slice(512 * n, 512 * n + 512)
        normed_ref[own, cols] = (acc_s[:, cols] * scale * norm_ref[:, cols]).astype(BF16)
        share = pltpu.make_async_remote_copy(
            src_ref=normed_ref.at[own, cols],
            dst_ref=normed_ref.at[own, cols],
            send_sem=share_send.at[n],
            recv_sem=share_recv.at[n],
            device_id=partner(),
            device_id_type=MESH,
        )
        share.start()
        shares.append(share)
    for share in shares:
        share.wait()
    for copy in sent:
        copy.wait_send()


def attention(q, k, v, strength, inputs, extra, rate, gate, gain, out_w, residual, norm_gain, ids, weight):
    half, model = residual.shape
    tokens, heads, blocks = 2 * half, 4, 2 * half // SPAN
    hbm = pl.BlockSpec(memory_space=pl.ANY)
    per_head = pltpu.VMEM((heads, tokens, HD), F32)
    side = pltpu.VMEM((heads, SPAN, tokens), F32)
    maps = pltpu.VMEM((4, HD, 2 * HD), STATE_TYPE)
    return pl.pallas_call(
        attention_kernel,
        out_shape=(
            jax.ShapeDtypeStruct((half, model), BF16),
            jax.ShapeDtypeStruct((tokens, model), BF16),
            jax.ShapeDtypeStruct((2, 2 * TOP_K, half), F32),
            jax.ShapeDtypeStruct((64, tokens), F32),
        ),
        in_specs=[VMEM] * 7 + [hbm, VMEM, hbm, hbm] + [VMEM] * 3,
        out_specs=(VMEM,) * 4,
        scratch_shapes=[
            per_head,
            per_head,
            pltpu.VMEM((8, tokens), F32),
            side,
            side,
            side,
            pltpu.VMEM((heads, tokens, 2 * HD), BF16),
            pltpu.VMEM((heads, tokens, 2 * HD), BF16),
            pltpu.VMEM((heads, tokens, 2 * HD), BF16),
            pltpu.VMEM((heads, HD, tokens), F32),
            per_head,
            pltpu.VMEM((heads, blocks, HD, 2 * HD), F32),
            pltpu.VMEM((5, heads, HD, 2 * HD), F32),
            pltpu.VMEM((blocks, heads, HD, 2 * HD), F32),
            pltpu.VMEM((4, HD, 2 * HD), F32),
            per_head,
            per_head,
            maps,
            pltpu.VMEM((2 * TOP_K, half), F32),
            pltpu.VMEM((tokens, heads * HD), BF16),
            pltpu.VMEM((2 * heads * HD, model), BF16),
            pltpu.VMEM((half, model), BF16),
            pltpu.VMEM((tokens, heads * HD), F32),
            maps,
            maps,
            maps,
            pltpu.VMEM((HD, 2 * HD), STATE_TYPE),
            pltpu.VMEM((HD, 2 * HD), STATE_TYPE),
            pltpu.VMEM((4, HD, HD), STATE_TYPE),
            pltpu.VMEM((4, HD, HD), STATE_TYPE),
            pltpu.VMEM((tokens, heads * HD), BF16),
            pltpu.VMEM((half, heads * HD), BF16),
            pltpu.VMEM((half, model), F32),
            pltpu.SemaphoreType.DMA((5, 3)),
            pltpu.SemaphoreType.DMA((5, 3)),
            pltpu.SemaphoreType.DMA((4,)),
            pltpu.SemaphoreType.DMA((4,)),
            pltpu.SemaphoreType.DMA((3,)),
        ],
        compiler_params=params(collective_id=0, has_side_effects=True),
        name="attention",
    )(q, k, v, strength, inputs, extra, rate, gate, gain, out_w, residual, norm_gain, ids, weight)


def at(ref, fixed):
    return ref.at[tuple(fixed.get(d, slice(None)) for d in range(3))]


def experts_kernel(
    normed_ref, attended_hbm, meta_ref, code_ref, gate_hbm, up_hbm, down_hbm, common_gate_hbm, common_up_hbm, common_down_hbm,
    out_ref,
    buf0, buf1, buf2, buf3, buf4, gate_w, up_w, down_w, common_gate_w, common_up_w, common_down_w,
    attended_s, pick_s, acc_s, away_s, here_s,
    send1, recv1, send2, recv2, send3, recv3, free_sem, swap_send, swap_recv, load_sem,
):
    tokens, model = normed_ref.shape
    half = tokens // 2
    chips = 64
    c = lax.axis_index("tp")
    loads = [
        pltpu.make_async_copy(a, b, load_sem.at[i])
        for i, (a, b) in enumerate(
            (
                (attended_hbm, attended_s),
                (common_gate_hbm, common_gate_w),
                (common_up_hbm, common_up_w),
                (common_down_hbm, common_down_w),
                (gate_hbm, gate_w),
                (up_hbm, up_w),
                (down_hbm, down_w),
            )
        )
    ]
    for load in loads:
        load.start()

    greeted = arrive((0, 1, 2), True)
    coord = [lax.axis_index(a) for a in SP]
    away = [[lax.rem(coord[d] + off, 4) for off in OFFSETS] for d in range(3)]
    back = [[lax.rem(coord[d] + 4 - off, 4) for off in OFFSETS] for d in range(3)]
    forward = (buf0, buf1, buf2, buf3)
    backward = (buf3, buf4, buf1, buf0)

    def dims(way, k):
        return ORDERS[k] if way == 0 else ORDERS[k][::-1]

    def remote(src, dst, send, recv, dim, n):
        return pltpu.make_async_remote_copy(
            src_ref=src,
            dst_ref=dst,
            send_sem=send,
            recv_sem=recv,
            device_id=along(dim, OFFSETS[n]),
            device_id_type=MESH,
        )

    def keep(source, target):
        for i in range(4):
            target[i] = source[i]

    def first(way, k, n):
        bufs = forward if way == 0 else backward
        d1 = dims(way, k)[0]
        return remote(
            at(bufs[0].at[k], {d1: away[d1][n]}),
            at(bufs[1].at[k], {d1: coord[d1]}),
            send1.at[way, k, n],
            recv1.at[way, k, n],
            d1,
            n,
        )

    def second(way, k, m, n):
        bufs = forward if way == 0 else backward
        d1, d2, _ = dims(way, k)
        source = bufs[0] if m == 0 else bufs[1]
        place = coord[d1] if m == 0 else back[d1][m - 1]
        return remote(
            at(source.at[k], {d1: place, d2: away[d2][n]}),
            at(bufs[2].at[k], {d1: place, d2: coord[d2]}),
            send2.at[way, k, m, n],
            recv2.at[way, k, m, n],
            d2,
            n,
        )

    def third(way, k, m, n):
        bufs = forward if way == 0 else backward
        _, d2, d3 = dims(way, k)
        place = coord[d2] if m == 0 else back[d2][m - 1]
        return remote(
            at(bufs[2].at[k], {d2: place, d3: away[d3][n]}),
            at(bufs[3].at[k], {d2: place, d3: coord[d3]}),
            send3.at[way, k, m, n],
            recv3.at[way, k, m, n],
            d3,
            n,
        )

    def start_second(way, k, m):
        bufs = forward if way == 0 else backward
        d1, d2, _ = dims(way, k)
        for n in range(3):
            second(way, k, m, n).start()
        source = bufs[0] if m == 0 else bufs[1]
        place = coord[d1] if m == 0 else back[d1][m - 1]
        keep(at(source.at[k], {d1: place, d2: coord[d2]}), at(bufs[2].at[k], {d1: place, d2: coord[d2]}))

    def start_third(way, k, m):
        bufs = forward if way == 0 else backward
        _, d2, d3 = dims(way, k)
        for n in range(3):
            third(way, k, m, n).start()
        place = coord[d2] if m == 0 else back[d2][m - 1]
        keep(at(bufs[2].at[k], {d2: place, d3: coord[d3]}), at(bufs[3].at[k], {d2: place, d3: coord[d3]}))

    for k in (0, 2, 1):
        low = 0 if k < 2 else half
        high = half if k == 0 else tokens
        wanted = (iota((chips, 8, high - low), 1) + 8 * k).astype(F32)
        pick = jnp.where(code_ref[:, low:high][:, None, :] == wanted, 1.0, 0.0)
        pick = pick.reshape(8 * chips, high - low).astype(BF16)
        for n in range(model // 512):
            cols = slice(512 * n, 512 * n + 512)
            rows = mm(pick, normed_ref[low:high, cols]).astype(BF16)
            buf0[k, :, :, :, :, cols] = rows.reshape(4, 4, 4, 8, 512)
        if k == 0:
            pl.semaphore_wait(pltpu.get_barrier_semaphore(), greeted)
        for n in range(3):
            first(0, k, n).start()
    for k in range(3):
        start_second(0, k, 0)

    for load in loads[:4]:
        load.wait()
    own = pl.ds(pl.multiple_of(c * half, half), half)
    hidden = silu(mm(normed_ref[own, :], common_gate_w[...])) * mm(normed_ref[own, :], common_up_w[...])
    hidden = hidden.astype(BF16)
    for n in range(model // 512):
        cols = slice(512 * n, 512 * n + 512)
        acc_s[:, cols] = attended_s[:, cols].astype(F32) + mm(hidden, common_down_w[:, cols])

    for n in range(3):
        for k in range(3):
            first(0, k, n).wait_recv()
            start_second(0, k, n + 1)
    for k in range(3):
        start_third(0, k, 0)

    meta = jnp.concatenate([meta_ref[0], meta_ref[1]], 1).T
    expert = (2 * iota((1, chips), 1) + c).astype(F32)
    chosen = jnp.zeros((tokens, chips), F32)
    weight = jnp.zeros((tokens, chips), F32)
    for q in range(TOP_K):
        hit = meta[:, q : q + 1] == expert
        chosen = chosen + jnp.where(hit, 1.0, 0.0)
        weight = weight + jnp.where(hit, meta[:, TOP_K + q : TOP_K + q + 1], 0.0)
    i, j = iota((tokens, tokens), 0), iota((tokens, tokens), 1)
    before = jnp.where((i // half == j // half) & (j < i), 1.0, 0.0).astype(BF16)
    slot = mm(before, chosen.astype(BF16))
    shift = jnp.where(iota((tokens, chips), 0) < half, 0.0, float(CAP))
    code = jnp.where(chosen > 0.0, slot + shift, -1.0).astype(BF16)
    spread = jnp.where(iota((chips, 8 * chips), 1) // 8 == iota((chips, 8 * chips), 0), 1.0, 0.0).astype(BF16)
    code = mm(code, spread)
    weight = mm(weight.astype(BF16), spread)
    place = (iota((tokens, 8 * chips), 1) % 8).astype(F32)
    for k in range(3):
        pick_s[k] = jnp.where(code == place + 8.0 * k, weight, 0.0).astype(BF16)

    for n in range(3):
        for k in range(3):
            for m in range(4):
                second(0, k, m, n).wait_recv()
            start_third(0, k, n + 1)
    for k in range(3):
        for n in range(3):
            first(0, k, n).wait_send()
        for m in range(4):
            for n in range(3):
                second(0, k, m, n).wait_send()
        d1, d2, _ = ORDERS[k]
        for off in OFFSETS:
            pl.semaphore_signal(free_sem.at[0, k], inc=1, device_id=along(d2, off), device_id_type=MESH)
            pl.semaphore_signal(free_sem.at[1, k], inc=1, device_id=along(d1, off), device_id_type=MESH)
    for load in loads[4:]:
        load.wait()

    def serve(places):
        views = [at(buf3.at[k], {ORDERS[k][2]: places[k]}) for k in range(3)]
        rows = jnp.concatenate([v[...].reshape(128, model) for v in views], 0)
        hidden = (silu(mm(rows, gate_w[...])) * mm(rows, up_w[...])).astype(BF16)
        for n in range(model // 512):
            cols = slice(512 * n, 512 * n + 512)
            result = mm(hidden, down_w[:, cols]).astype(BF16)
            for k in range(3):
                views[k][:, :, :, cols] = result[128 * k : 128 * k + 128].reshape(4, 4, 8, 512)

    last = [ORDERS[k][2] for k in range(3)]
    serve([coord[d] for d in last])
    for k in range(3):
        pl.semaphore_wait(free_sem.at[0, k], 3)
        start_second(1, k, 0)
    for n in range(3):
        for k in range(3):
            for m in range(4):
                third(0, k, m, n).wait_recv()
        serve([back[d][n] for d in last])
        turned = OFFSETS.index(4 - OFFSETS[n])
        for k in range(3):
            first(1, k, turned).start()
    for n in range(3):
        for k in range(3):
            first(1, k, n).wait_recv()
            start_second(1, k, n + 1)
    for k in range(3):
        pl.semaphore_wait(free_sem.at[1, k], 3)
        start_third(1, k, 0)
    for n in range(3):
        for k in range(3):
            for m in range(4):
                second(1, k, m, n).wait_recv()
            start_third(1, k, n + 1)
    for n in range(3):
        for k in range(3):
            for m in range(4):
                third(1, k, m, n).wait_recv()

    def partial(core, cols):
        rows = pl.ds(pl.multiple_of(core * half, half), half)
        total = mm(pick_s[1, rows, :], buf0[1, :, :, :, :, cols].reshape(8 * chips, 512))
        return total + mm(pick_s[2 * core, rows, :], buf0[2 * core, :, :, :, :, cols].reshape(8 * chips, 512))

    swaps = []
    for n in range(model // 512):
        away_s[n] = partial(1 - c, slice(512 * n, 512 * n + 512))
        swap = pltpu.make_async_remote_copy(
            src_ref=away_s.at[n],
            dst_ref=here_s.at[n],
            send_sem=swap_send.at[n],
            recv_sem=swap_recv.at[n],
            device_id=partner(),
            device_id_type=MESH,
        )
        swap.start()
        swaps.append(swap)
    for n in range(model // 512):
        cols = slice(512 * n, 512 * n + 512)
        acc_s[:, cols] = acc_s[:, cols] + partial(c, cols)
    for n in range(model // 512):
        cols = slice(512 * n, 512 * n + 512)
        swaps[n].wait()
        out_ref[:, cols] = (acc_s[:, cols] + here_s[n]).astype(BF16)

    for k in range(3):
        for m in range(4):
            for n in range(3):
                third(0, k, m, n).wait_send()
                second(1, k, m, n).wait_send()
                third(1, k, m, n).wait_send()
        for n in range(3):
            first(1, k, n).wait_send()


def run_experts(normed, attended, meta, code, gate, up, down, common_gate, common_up, common_down):
    half, model = attended.shape
    buffer = pltpu.VMEM((3, 4, 4, 4, 8, model), BF16)
    hbm = pl.BlockSpec(memory_space=pl.ANY)
    return pl.pallas_call(
        experts_kernel,
        out_shape=jax.ShapeDtypeStruct((half, model), BF16),
        in_specs=[VMEM, hbm, VMEM, VMEM] + [hbm] * 6,
        out_specs=VMEM,
        scratch_shapes=[buffer] * 5
        + [pltpu.VMEM(w.shape, BF16) for w in (gate, up, down, common_gate, common_up, common_down)]
        + [
            pltpu.VMEM((half, model), BF16),
            pltpu.VMEM((3, 2 * half, 512), BF16),
            pltpu.VMEM((half, model), F32),
            pltpu.VMEM((model // 512, half, 512), F32),
            pltpu.VMEM((model // 512, half, 512), F32),
        ]
        + [pltpu.SemaphoreType.DMA((2, 3, 3))] * 2
        + [pltpu.SemaphoreType.DMA((2, 3, 4, 3))] * 4
        + [
            pltpu.SemaphoreType.REGULAR((2, 3)),
            pltpu.SemaphoreType.DMA((model // 512,)),
            pltpu.SemaphoreType.DMA((model // 512,)),
            pltpu.SemaphoreType.DMA((7,)),
        ],
        compiler_params=params(collective_id=1, has_side_effects=True),
        name="experts",
    )(normed, attended, meta, code, gate, up, down, common_gate, common_up, common_down)


def shards(
    projected_queries,
    projected_keys,
    projected_values,
    output_gate_values,
    write_strength_logits,
    decay_input_logits,
    head_rate_logarithm,
    extra_log_decay,
    per_head_norm_gain,
    output_matrix,
    residual,
    mixture_norm_gain,
    selected_expert_index,
    routing_weight,
    routed_gate_weight,
    routed_up_weight,
    routed_down_weight,
    common_gate_weight,
    common_up_weight,
    common_down_weight,
):
    attended, normed, meta, code = attention(
        projected_queries,
        projected_keys,
        projected_values,
        write_strength_logits.T,
        decay_input_logits.T,
        extra_log_decay.T,
        head_rate_logarithm[None, :],
        output_gate_values,
        per_head_norm_gain[None, :],
        output_matrix,
        residual,
        mixture_norm_gain[None, :],
        selected_expert_index.T,
        routing_weight.T,
    )
    return run_experts(
        normed,
        attended,
        meta,
        code,
        routed_gate_weight[0],
        routed_up_weight[0],
        routed_down_weight[0],
        common_gate_weight,
        common_up_weight,
        common_down_weight,
    )


def solution(mesh):
    finer = Mesh(mesh.devices.reshape(4, 4, 4, mesh.shape["tp"]), AXES)
    in_specs = (
        P(SP, "tp"),
        P(SP, "tp"),
        P(SP, "tp"),
        P(SP, "tp"),
        P(SP, "tp"),
        P(SP, "tp"),
        P("tp"),
        P(SP, "tp"),
        P(),
        P(),
        P(AXES, None),
        P(),
        P(AXES, None),
        P(AXES, None),
        P(AXES, None, None),
        P(AXES, None, None),
        P(AXES, None, None),
        P(),
        P(),
        P(),
    )
    return jax.shard_map(
        shards, mesh=finer, in_specs=in_specs, out_specs=P(AXES, None), check_vma=False
    )
```

```python
import functools

import jax
import jax.numpy as jnp
from jax import lax
from jax.experimental import pallas as pl
from jax.experimental.pallas import tpu as pltpu
from jax.sharding import Mesh
from jax.sharding import PartitionSpec as P

TOP_K = 4
SPAN = 64
CAP = 12
HD = 128
AXES = ("sp_0", "sp_1", "sp_2", "tp")
SP = AXES[:3]
EPS = 1e-06
F32, BF16 = jnp.float32, jnp.bfloat16
HIGH = lax.Precision.HIGHEST
MESH = pl.DeviceIdType.MESH
VMEM = pl.BlockSpec(memory_space=pltpu.VMEM)
OFFSETS = (2, 1, 3)
ORDERS = ((2, 1, 0), (1, 0, 2), (0, 2, 1))
STATE_TYPE = BF16


def params(**kw):
    return pltpu.CompilerParams(vmem_limit_bytes=62 * 2**20, **kw)


def mm(a, b, dims=((1,), (0,))):
    return lax.dot_general(a, b, (dims, ((), ())), preferred_element_type=F32)


def halves(x):
    high = x.astype(BF16)
    return high, (x - high.astype(F32)).astype(BF16)


def mm3(a, b, dims=((1,), (0,))):
    high, low = a
    both = mm2(a, b[0], dims)
    return both + mm(high, b[1], dims)


def mm2(a, b, dims=((1,), (0,))):
    rows = a[0].shape[0]
    if a[0].shape[1] == HD:
        return mm(jnp.concatenate(a, 1), jnp.concatenate([b, b], dims[1][0]), dims)
    both = mm(jnp.concatenate(a, 0), b, dims)
    return both[:rows] + both[rows:]


def silu(x):
    return (0.5 * x) * (1.0 + jnp.tanh(0.5 * x))


def iota(shape, dim):
    return lax.broadcasted_iota(jnp.int32, shape, dim)


def along(dim, off):
    at = [lax.axis_index(a) for a in AXES]
    at[dim] = lax.rem(at[dim] + off, 4)
    return tuple(at)


def partner():
    at = [lax.axis_index(a) for a in AXES]
    at[3] = 1 - at[3]
    return tuple(at)


def arrive(dims, pair):
    barrier = pltpu.get_barrier_semaphore()
    count = 0
    for dim in dims:
        for off in OFFSETS:
            pl.semaphore_signal(barrier, inc=1, device_id=along(dim, off), device_id_type=MESH)
            count += 1
    if pair:
        pl.semaphore_signal(barrier, inc=1, device_id=partner(), device_id_type=MESH)
        count += 1
    return count


def attention_kernel(
    q_ref, k_ref, v_ref, strength_ref, input_ref, extra_ref, rate_ref, gate_hbm, gain_ref, out_w_hbm, residual_hbm,
    norm_ref, ids_ref, weight_ref,
    attended_ref, normed_ref, both_meta_ref, code_ref,
    beta_s, g_s, row_s, low_s, decay_s, inv_s, right_s, kk_s, wu_s, kdt_s, qp_s, step_s, pair_s, pre_s, span_s, z_s, h_s, map_s, meta_s,
    gate_s, out_w_s, residual_s, lit_s, rows_in, plane_in, all_in, row_total, plane_total, state_out, state_in,
    mix_s, mix_in, acc_s, send_sem, recv_sem, share_send, share_recv, load_sem,
):
    heads, tokens = 4, q_ref.shape[0]
    blocks = tokens // SPAN
    loads = [
        pltpu.make_async_copy(src, dst, load_sem.at[i])
        for i, (src, dst) in enumerate(((gate_hbm, gate_s), (residual_hbm, residual_s), (out_w_hbm, out_w_s)))
    ]
    for load in loads:
        load.start()
    greeted = arrive((0, 1, 2), True)
    z, y, x, c = (lax.axis_index(a) for a in AXES)
    meta_s[0:TOP_K, :] = ids_ref[...].astype(F32)
    meta_s[TOP_K : 2 * TOP_K, :] = weight_ref[...]

    i256, j256 = iota((256, 256), 0), iota((256, 256), 1)
    same = (i256 // SPAN) == (j256 // SPAN)
    tri_t = jnp.where(same & (i256 <= j256), 1.0, 0.0)
    ones = jnp.where(same, 1.0, 0.0)

    def high(a, b):
        return lax.dot_general(a, b, (((1,), (0,)), ((), ())), precision=HIGH, preferred_element_type=F32)

    rate = jnp.where(iota((heads, heads), 0) == iota((heads, heads), 1), jnp.exp(rate_ref[...]), 0.0)
    rate = jnp.sum(rate, axis=1, keepdims=True)
    grown = input_ref[...].astype(F32) - 6.0
    tail = jnp.exp(-jnp.abs(grown))
    up = 1.0 + tail
    log_up = jnp.where(up == 1.0, tail, jnp.log(up) * tail / jnp.where(up == 1.0, 1.0, up - 1.0))
    decay = extra_ref[...] - rate * (jnp.maximum(grown, 0.0) + log_up)
    beta = 1.0 / (1.0 + jnp.exp(-strength_ref[...].astype(F32)))
    g_row = jnp.concatenate([high(decay[:, 256 * i : 256 * i + 256], tri_t) for i in range(2)], 1)
    total_row = jnp.concatenate([high(decay[:, 256 * i : 256 * i + 256], ones) for i in range(2)], 1)
    row_s[0:heads, :] = g_row
    row_s[heads : 2 * heads, :] = total_row
    cols = jnp.concatenate([beta, g_row], 0).T
    for h in range(heads):
        beta_s[h] = jnp.broadcast_to(cols[:, h : h + 1], (tokens, HD))
        g_s[h] = jnp.broadcast_to(cols[:, heads + h : heads + h + 1], (tokens, HD))

    row, lane = iota((SPAN, 128), 0), iota((SPAN, 128), 1)
    first = lane < SPAN
    place = lane % SPAN
    causal, strict = row >= place, row > place
    pair_masks = [jnp.where(first, 1.0, 0.0).astype(BF16), jnp.where(first, 0.0, 1.0).astype(BF16)]
    first_wide = iota((128, 128), 1) < SPAN
    eye = jnp.where(iota((128, 128), 0) == iota((128, 128), 1), 1.0, 0.0)

    def prepare(h, _):
        lanes = pl.ds(pl.multiple_of(h * HD, HD), HD)
        k = silu(k_ref[:, lanes].astype(F32))
        k = k * lax.rsqrt(jnp.sum(k * k, axis=-1, keepdims=True) + EPS)
        v = silu(v_ref[:, lanes].astype(F32))
        b_h, g_h = beta_s[h], g_s[h]
        grown = jnp.exp(g_h)
        kb = k * b_h
        right_s[h, :, :HD] = (kb * grown).astype(BF16)
        right_s[h, :, HD:] = (v * b_h).astype(BF16)
        gr = row_s[pl.ds(h, 1), :]
        kdt_s[h] = k.T * jnp.exp(row_s[pl.ds(h + heads, 1), :] - gr)
        ks, kbs = halves(k), halves(kb)
        kk_s[h, :, :HD] = ks[0]
        kk_s[h, :, HD:] = ks[1]
        for j in range(tokens // 128):
            rows = slice(128 * j, 128 * j + 128)
            both = mm3(tuple(a[rows] for a in kbs), tuple(a[rows] for a in ks), ((1,), (1,)))
            inner = jnp.where(first, both[0:64], both[64:128])
            gi = jnp.where(first, g_h[128 * j : 128 * j + 64], g_h[128 * j + 64 : 128 * j + 128])
            spread = jnp.where(causal, gi - gr[:, rows], 0.0)
            decay = jnp.where(causal, jnp.exp(spread), 0.0)
            low_s[h, :, rows] = jnp.where(strict, inner * decay, 0.0)
            decay_s[h, :, rows] = decay
        return 0

    lax.fori_loop(0, heads, prepare, 0)

    r4, l4 = iota((SPAN, 256), 0), iota((SPAN, 256), 1)
    p4 = l4 % SPAN
    quad_masks = [jnp.where(l4 // SPAN == n, 1.0, 0.0).astype(BF16) for n in range(4)]
    eye4 = jnp.where(r4 == p4, 1.0, 0.0)

    def diag4(x):
        return jnp.concatenate([x * m for m in quad_masks], 0)

    def times(a, b):
        return mm3(a, tuple(diag4(x) for x in b))

    def times2(a, b):
        return mm2(a, diag4(b.astype(BF16)))

    def invert():
        mine = [(i // 2, slice(256 * (i % 2), 256 * (i % 2) + 256)) for i in range(8)]
        lows = [low_s[h, :, s] for h, s in mine]
        small = r4 // 8 == p4 // 8
        d1 = [jnp.where(small, x, 0.0) for x in lows]
        d1s = [halves(x) for x in d1]
        d2s = [halves(times(x, x)) for x in d1s]
        x1 = [eye4 - x for x in d1]
        x2 = [x + times(halves(x), d) for x, d in zip(x1, d2s)]
        d4s = [halves(times(d, d)) for d in d2s]
        inv = [x + times(halves(x), d) for x, d in zip(x2, d4s)]
        for size in (8, 16, 32):
            off = (r4 // (2 * size) == p4 // (2 * size)) & (r4 // size != p4 // size)
            ex = [times2(halves(jnp.where(off, x, 0.0)), y) for x, y in zip(lows, inv)]
            inv = [x - times2(halves(x), e) for x, e in zip(inv, ex)]
        for (h, s), x in zip(mine, inv):
            inv_s[h, :, s] = x

    invert()

    def diag2(x):
        return jnp.concatenate([x * m for m in pair_masks], 0)

    def apply(h, _):
        for j in range(tokens // 128):
            rows = slice(128 * j, 128 * j + 128)
            inv = tuple(diag2(x) for x in halves(inv_s[h, :, rows]))
            wu = mm2(inv, right_s[h, rows, :]).astype(BF16)
            wu_s[h, rows, :] = wu
            kdt = kdt_s[h, :, rows]
            kdt = halves(jnp.concatenate([jnp.where(first_wide, kdt, 0.0), jnp.where(first_wide, 0.0, kdt)], 0))
            change = mm2(kdt, wu)
            for i in range(2):
                n = 2 * j + i
                factor = jnp.exp(g_s[h, n * SPAN + SPAN - 1 : n * SPAN + SPAN, :])
                step_s[h, n, :, :HD] = eye * factor - change[128 * i : 128 * i + 128, :HD]
                step_s[h, n, :, HD:] = change[128 * i : 128 * i + 128, HD:]
        return 0

    lax.fori_loop(0, heads, apply, 0)

    def compose(later, earlier):
        moved = mm3(halves(later[:, :HD]), halves(earlier))
        return jnp.concatenate([moved[:, :HD], moved[:, HD:] + later[:, HD:]], 1)

    def pairs(i, _):
        for h in range(heads):
            pair_s[i, h] = compose(step_s[h, 2 * i + 1], step_s[h, 2 * i])
        return 0

    lax.fori_loop(0, 4, pairs, 0)
    for h in range(heads):
        pre_s[4, h] = compose(pair_s[1, h], pair_s[0, h])
        pair_s[4, h] = compose(pair_s[3, h], pair_s[2, h])
    for h in range(heads):
        map_s[h] = compose(pair_s[4, h], pre_s[4, h]).astype(STATE_TYPE)

    def send(stage, dim, source, target):
        copies = []
        here = lax.axis_index(AXES[dim])
        for n, off in enumerate(OFFSETS):
            copies.append(
                pltpu.make_async_remote_copy(
                    src_ref=source(lax.rem(here + off, 4)),
                    dst_ref=target.at[here],
                    send_sem=send_sem.at[stage, n],
                    recv_sem=recv_sem.at[stage, n],
                    device_id=along(dim, off),
                    device_id_type=MESH,
                )
            )
        for n in range(3):
            copies[n].start()
        return copies

    def moved_by(step, carried):
        high, low = halves(carried)
        moved = mm(step[:, :HD], jnp.concatenate([high, low], 1))
        width = carried.shape[1]
        moved = moved[:, :width] + moved[:, width:]
        if width == HD:
            return moved + step[:, HD:].astype(F32)
        return jnp.concatenate([moved[:, :HD], moved[:, HD:] + step[:, HD:].astype(F32)], 1)

    def scores(h, _):
        lanes = pl.ds(pl.multiple_of(h * HD, HD), HD)
        q = silu(q_ref[:, lanes].astype(F32))
        q = q * lax.rsqrt(jnp.sum(q * q, axis=-1, keepdims=True) + EPS)
        qd = q * jnp.exp(g_s[h])
        qs = halves(q)
        for j in range(tokens // 128):
            rows = slice(128 * j, 128 * j + 128)
            ks = (kk_s[h, rows, :HD], kk_s[h, rows, HD:])
            both = mm3(tuple(a[rows] for a in qs), ks, ((1,), (1,)))
            score = jnp.where(first, both[0:64], both[64:128]) * decay_s[h, :, rows]
            both = mm2(tuple(diag2(x) for x in halves(score)), wu_s[h, rows, :])
            qp_s[h, rows, :] = qd[rows] - both[:, :HD]
            h_s[h, rows, :] = both[:, HD:]
        return 0

    def outputs(h):
        pre_s[1, h] = step_s[h, 0]
        pre_s[2, h] = pair_s[0, h]
        pre_s[3, h] = compose(step_s[h, 2], pair_s[0, h])
        pre_s[5, h] = compose(step_s[h, 4], pre_s[4, h])
        pre_s[6, h] = compose(pair_s[2, h], pre_s[4, h])
        pre_s[7, h] = compose(step_s[h, 6], pre_s[6, h])
        z_s[h, 0:SPAN, :] = qp_s[h, 0:SPAN, :]
        for n in range(1, blocks):
            rows = slice(SPAN * n, SPAN * n + SPAN)
            moved = mm2(halves(qp_s[h, rows, :]), pre_s[n, h].astype(BF16))
            z_s[h, rows, :] = moved[:, :HD]
            h_s[h, rows, :] = h_s[h, rows, :] + moved[:, HD:]

    def light(h):
        lanes = slice(h * HD, h * HD + HD)
        lit_s[:, lanes] = silu(gate_s[:, lanes].astype(F32)) * gain_ref[...]

    sent = []
    pl.semaphore_wait(pltpu.get_barrier_semaphore(), greeted)
    copies = send(0, 2, lambda t: map_s.at[t], rows_in)
    tell = pltpu.make_async_remote_copy(
        src_ref=meta_s,
        dst_ref=both_meta_ref.at[c],
        send_sem=send_sem.at[4, 2],
        recv_sem=recv_sem.at[4, 2],
        device_id=partner(),
        device_id_type=MESH,
    )
    tell.start()
    both_meta_ref[c] = meta_s[...]
    rows_in[x] = map_s[x]
    lax.fori_loop(0, heads, scores, 0)
    for copy in copies:
        copy.wait_recv()
    sent += copies
    low_pair = moved_by(rows_in[1], rows_in[0].astype(F32))
    high_pair = moved_by(rows_in[3], rows_in[2].astype(F32))
    span_s[2] = low_pair
    row_total[...] = compose(high_pair, low_pair).astype(STATE_TYPE)
    copies = send(1, 1, lambda t: row_total, plane_in)
    plane_in[y] = row_total[...]
    span_s[1] = rows_in[0].astype(F32)
    span_s[3] = moved_by(rows_in[2], span_s[2])
    loads[0].wait()
    for h in range(heads):
        light(h)
        outputs(h)
    for copy in copies:
        copy.wait_recv()
    sent += copies
    low_pair = moved_by(plane_in[1], plane_in[0].astype(F32))
    high_pair = moved_by(plane_in[3], plane_in[2].astype(F32))
    plane_total[...] = compose(high_pair, low_pair).astype(STATE_TYPE)
    copies = send(2, 0, lambda t: plane_total, all_in)
    all_in[z] = plane_total[...]
    entry = jnp.where(y == 1, plane_in[0].astype(F32), jnp.concatenate([eye, jnp.zeros((HD, HD), F32)], 1))
    entry = jnp.where(y == 2, low_pair, entry)
    entry = jnp.where(y == 3, moved_by(plane_in[2], low_pair), entry)
    span_s[0] = entry
    for i in range(1, 4):
        span_s[i] = compose(span_s[i], entry)

    tell.wait()
    chips = code_ref.shape[0]
    expert = (2 * iota((chips, 1), 0) + c).astype(F32)
    chosen = jnp.zeros((chips, tokens), F32)
    for j in range(TOP_K):
        ids = jnp.concatenate([both_meta_ref[0, j : j + 1, :], both_meta_ref[1, j : j + 1, :]], 1)
        chosen = chosen + jnp.where(ids == expert, 1.0, 0.0)
    i512, j512 = iota((tokens, tokens), 0), iota((tokens, tokens), 1)
    half = tokens // 2
    before = jnp.where((i512 // half == j512 // half) & (i512 < j512), 1.0, 0.0).astype(BF16)
    slot = mm(chosen.astype(BF16), before)
    shift = jnp.where(iota((chips, tokens), 1) < half, 0.0, float(CAP))
    code_ref[...] = jnp.where(chosen > 0.0, slot + shift, -1.0)

    for copy in copies:
        copy.wait_recv()
    sent += copies
    state = jnp.where(z > 0, all_in[0, :, HD:].astype(F32), 0.0)
    for i in range(1, 3):
        state = jnp.where(i < z, moved_by(all_in[i], state), state)
    state = halves(state)
    for i in range(4):
        entering = mm3(halves(span_s[i, :, :HD]), state) + span_s[i, :, HD:]
        state_out[i] = entering.astype(STATE_TYPE)
    copies = send(3, 2, lambda t: state_out.at[t], state_in)
    state_in[x] = state_out[x]
    for copy in copies:
        copy.wait_recv()
    sent += copies

    for h in range(heads):
        lanes = slice(h * HD, h * HD + HD)
        mix = h_s[h] + mm2(halves(z_s[h]), state_in[h])
        mix = mix * lax.rsqrt(jnp.mean(mix * mix, axis=-1, keepdims=True) + EPS) * lit_s[:, lanes]
        mix_s[:, lanes] = mix.astype(BF16)
    width = mix_s.shape[1]
    other = 1 - c
    swap = pltpu.make_async_remote_copy(
        src_ref=mix_s.at[pl.ds(pl.multiple_of(other * half, half), half)],
        dst_ref=mix_in,
        send_sem=send_sem.at[4, 0],
        recv_sem=recv_sem.at[4, 0],
        device_id=partner(),
        device_id_type=MESH,
    )
    swap.start()
    for load in loads[1:]:
        load.wait()
    own = pl.ds(pl.multiple_of(c * half, half), half)
    own_w = pl.ds(pl.multiple_of(c * width, width), width)
    other_w = pl.ds(pl.multiple_of(other * width, width), width)
    model = out_w_s.shape[1]
    for n in range(model // 512):
        cols = slice(512 * n, 512 * n + 512)
        acc_s[:, cols] = residual_s[:, cols].astype(F32) + mm(mix_s[own, :], out_w_s[own_w, cols])
    swap.wait()
    squares = jnp.zeros((half, 1), F32)
    for n in range(model // 512):
        cols = slice(512 * n, 512 * n + 512)
        piece = acc_s[:, cols] + mm(mix_in[...], out_w_s[other_w, cols])
        piece = piece.astype(BF16)
        attended_ref[:, cols] = piece
        wide = piece.astype(F32)
        acc_s[:, cols] = wide
        squares = squares + jnp.sum(wide * wide, axis=-1, keepdims=True)
    scale = lax.rsqrt(squares / model + EPS)
    shares = []
    for n in range(model // 512):
        cols = slice(512 * n, 512 * n + 512)
        normed_ref[own, cols] = (acc_s[:, cols] * scale * norm_ref[:, cols]).astype(BF16)
        share = pltpu.make_async_remote_copy(
            src_ref=normed_ref.at[own, cols],
            dst_ref=normed_ref.at[own, cols],
            send_sem=share_send.at[n],
            recv_sem=share_recv.at[n],
            device_id=partner(),
            device_id_type=MESH,
        )
        share.start()
        shares.append(share)
    for share in shares:
        share.wait()
    for copy in sent:
        copy.wait_send()


def attention(q, k, v, strength, inputs, extra, rate, gate, gain, out_w, residual, norm_gain, ids, weight):
    half, model = residual.shape
    tokens, heads, blocks = 2 * half, 4, 2 * half // SPAN
    hbm = pl.BlockSpec(memory_space=pl.ANY)
    per_head = pltpu.VMEM((heads, tokens, HD), F32)
    side = pltpu.VMEM((heads, SPAN, tokens), F32)
    maps = pltpu.VMEM((4, HD, 2 * HD), STATE_TYPE)
    return pl.pallas_call(
        attention_kernel,
        out_shape=(
            jax.ShapeDtypeStruct((half, model), BF16),
            jax.ShapeDtypeStruct((tokens, model), BF16),
            jax.ShapeDtypeStruct((2, 2 * TOP_K, half), F32),
            jax.ShapeDtypeStruct((64, tokens), F32),
        ),
        in_specs=[VMEM] * 7 + [hbm, VMEM, hbm, hbm] + [VMEM] * 3,
        out_specs=(VMEM,) * 4,
        scratch_shapes=[
            per_head,
            per_head,
            pltpu.VMEM((8, tokens), F32),
            side,
            side,
            side,
            pltpu.VMEM((heads, tokens, 2 * HD), BF16),
            pltpu.VMEM((heads, tokens, 2 * HD), BF16),
            pltpu.VMEM((heads, tokens, 2 * HD), BF16),
            pltpu.VMEM((heads, HD, tokens), F32),
            per_head,
            pltpu.VMEM((heads, blocks, HD, 2 * HD), F32),
            pltpu.VMEM((5, heads, HD, 2 * HD), F32),
            pltpu.VMEM((blocks, heads, HD, 2 * HD), F32),
            pltpu.VMEM((4, HD, 2 * HD), F32),
            per_head,
            per_head,
            maps,
            pltpu.VMEM((2 * TOP_K, half), F32),
            pltpu.VMEM((tokens, heads * HD), BF16),
            pltpu.VMEM((2 * heads * HD, model), BF16),
            pltpu.VMEM((half, model), BF16),
            pltpu.VMEM((tokens, heads * HD), F32),
            maps,
            maps,
            maps,
            pltpu.VMEM((HD, 2 * HD), STATE_TYPE),
            pltpu.VMEM((HD, 2 * HD), STATE_TYPE),
            pltpu.VMEM((4, HD, HD), STATE_TYPE),
            pltpu.VMEM((4, HD, HD), STATE_TYPE),
            pltpu.VMEM((tokens, heads * HD), BF16),
            pltpu.VMEM((half, heads * HD), BF16),
            pltpu.VMEM((half, model), F32),
            pltpu.SemaphoreType.DMA((5, 3)),
            pltpu.SemaphoreType.DMA((5, 3)),
            pltpu.SemaphoreType.DMA((4,)),
            pltpu.SemaphoreType.DMA((4,)),
            pltpu.SemaphoreType.DMA((3,)),
        ],
        compiler_params=params(collective_id=0, has_side_effects=True),
        name="attention",
    )(q, k, v, strength, inputs, extra, rate, gate, gain, out_w, residual, norm_gain, ids, weight)


def at(ref, fixed):
    return ref.at[tuple(fixed.get(d, slice(None)) for d in range(3))]


def experts_kernel(
    normed_ref, attended_hbm, meta_ref, code_ref, gate_hbm, up_hbm, down_hbm, common_gate_hbm, common_up_hbm, common_down_hbm,
    out_ref,
    buf0, buf1, buf2, buf3, buf4, gate_w, up_w, down_w, common_gate_w, common_up_w, common_down_w,
    attended_s, pick_s, acc_s, away_s, here_s,
    send1, recv1, send2, recv2, send3, recv3, free_sem, swap_send, swap_recv, load_sem,
):
    tokens, model = normed_ref.shape
    half = tokens // 2
    chips = 64
    c = lax.axis_index("tp")
    loads = [
        pltpu.make_async_copy(a, b, load_sem.at[i])
        for i, (a, b) in enumerate(
            (
                (attended_hbm, attended_s),
                (common_gate_hbm, common_gate_w),
                (common_up_hbm, common_up_w),
                (common_down_hbm, common_down_w),
                (gate_hbm, gate_w),
                (up_hbm, up_w),
                (down_hbm, down_w),
            )
        )
    ]
    for load in loads:
        load.start()

    greeted = arrive((0, 1, 2), True)
    coord = [lax.axis_index(a) for a in SP]
    away = [[lax.rem(coord[d] + off, 4) for off in OFFSETS] for d in range(3)]
    back = [[lax.rem(coord[d] + 4 - off, 4) for off in OFFSETS] for d in range(3)]
    forward = (buf0, buf1, buf2, buf3)
    backward = (buf3, buf4, buf1, buf0)

    def dims(way, k):
        return ORDERS[k] if way == 0 else ORDERS[k][::-1]

    def remote(src, dst, send, recv, dim, n):
        return pltpu.make_async_remote_copy(
            src_ref=src,
            dst_ref=dst,
            send_sem=send,
            recv_sem=recv,
            device_id=along(dim, OFFSETS[n]),
            device_id_type=MESH,
        )

    def keep(source, target):
        for i in range(4):
            target[i] = source[i]

    def first(way, k, n):
        bufs = forward if way == 0 else backward
        d1 = dims(way, k)[0]
        return remote(
            at(bufs[0].at[k], {d1: away[d1][n]}),
            at(bufs[1].at[k], {d1: coord[d1]}),
            send1.at[way, k, n],
            recv1.at[way, k, n],
            d1,
            n,
        )

    def second(way, k, m, n):
        bufs = forward if way == 0 else backward
        d1, d2, _ = dims(way, k)
        source = bufs[0] if m == 0 else bufs[1]
        place = coord[d1] if m == 0 else back[d1][m - 1]
        return remote(
            at(source.at[k], {d1: place, d2: away[d2][n]}),
            at(bufs[2].at[k], {d1: place, d2: coord[d2]}),
            send2.at[way, k, m, n],
            recv2.at[way, k, m, n],
            d2,
            n,
        )

    def third(way, k, m, n):
        bufs = forward if way == 0 else backward
        _, d2, d3 = dims(way, k)
        place = coord[d2] if m == 0 else back[d2][m - 1]
        return remote(
            at(bufs[2].at[k], {d2: place, d3: away[d3][n]}),
            at(bufs[3].at[k], {d2: place, d3: coord[d3]}),
            send3.at[way, k, m, n],
            recv3.at[way, k, m, n],
            d3,
            n,
        )

    def start_second(way, k, m):
        bufs = forward if way == 0 else backward
        d1, d2, _ = dims(way, k)
        for n in range(3):
            second(way, k, m, n).start()
        source = bufs[0] if m == 0 else bufs[1]
        place = coord[d1] if m == 0 else back[d1][m - 1]
        keep(at(source.at[k], {d1: place, d2: coord[d2]}), at(bufs[2].at[k], {d1: place, d2: coord[d2]}))

    def start_third(way, k, m):
        bufs = forward if way == 0 else backward
        _, d2, d3 = dims(way, k)
        for n in range(3):
            third(way, k, m, n).start()
        place = coord[d2] if m == 0 else back[d2][m - 1]
        keep(at(bufs[2].at[k], {d2: place, d3: coord[d3]}), at(bufs[3].at[k], {d2: place, d3: coord[d3]}))

    for k in (0, 2, 1):
        low = 0 if k < 2 else half
        high = half if k == 0 else tokens
        wanted = (iota((chips, 8, high - low), 1) + 8 * k).astype(F32)
        pick = jnp.where(code_ref[:, low:high][:, None, :] == wanted, 1.0, 0.0)
        pick = pick.reshape(8 * chips, high - low).astype(BF16)
        for n in range(model // 512):
            cols = slice(512 * n, 512 * n + 512)
            rows = mm(pick, normed_ref[low:high, cols]).astype(BF16)
            buf0[k, :, :, :, :, cols] = rows.reshape(4, 4, 4, 8, 512)
        if k == 0:
            pl.semaphore_wait(pltpu.get_barrier_semaphore(), greeted)
        for n in range(3):
            first(0, k, n).start()
    for k in range(3):
        start_second(0, k, 0)

    for load in loads[:4]:
        load.wait()
    own = pl.ds(pl.multiple_of(c * half, half), half)
    hidden = silu(mm(normed_ref[own, :], common_gate_w[...])) * mm(normed_ref[own, :], common_up_w[...])
    hidden = hidden.astype(BF16)
    for n in range(model // 512):
        cols = slice(512 * n, 512 * n + 512)
        acc_s[:, cols] = attended_s[:, cols].astype(F32) + mm(hidden, common_down_w[:, cols])

    for n in range(3):
        for k in range(3):
            first(0, k, n).wait_recv()
            start_second(0, k, n + 1)
    for k in range(3):
        start_third(0, k, 0)

    meta = jnp.concatenate([meta_ref[0], meta_ref[1]], 1).T
    expert = (2 * iota((1, chips), 1) + c).astype(F32)
    chosen = jnp.zeros((tokens, chips), F32)
    weight = jnp.zeros((tokens, chips), F32)
    for q in range(TOP_K):
        hit = meta[:, q : q + 1] == expert
        chosen = chosen + jnp.where(hit, 1.0, 0.0)
        weight = weight + jnp.where(hit, meta[:, TOP_K + q : TOP_K + q + 1], 0.0)
    i, j = iota((tokens, tokens), 0), iota((tokens, tokens), 1)
    before = jnp.where((i // half == j // half) & (j < i), 1.0, 0.0).astype(BF16)
    slot = mm(before, chosen.astype(BF16))
    shift = jnp.where(iota((tokens, chips), 0) < half, 0.0, float(CAP))
    code = jnp.where(chosen > 0.0, slot + shift, -1.0).astype(BF16)
    spread = jnp.where(iota((chips, 8 * chips), 1) // 8 == iota((chips, 8 * chips), 0), 1.0, 0.0).astype(BF16)
    code = mm(code, spread)
    weight = mm(weight.astype(BF16), spread)
    place = (iota((tokens, 8 * chips), 1) % 8).astype(F32)
    for k in range(3):
        pick_s[k] = jnp.where(code == place + 8.0 * k, weight, 0.0).astype(BF16)

    for n in range(3):
        for k in range(3):
            for m in range(4):
                second(0, k, m, n).wait_recv()
            start_third(0, k, n + 1)
    for k in range(3):
        for n in range(3):
            first(0, k, n).wait_send()
        for m in range(4):
            for n in range(3):
                second(0, k, m, n).wait_send()
        d1, d2, _ = ORDERS[k]
        for off in OFFSETS:
            pl.semaphore_signal(free_sem.at[0, k], inc=1, device_id=along(d2, off), device_id_type=MESH)
            pl.semaphore_signal(free_sem.at[1, k], inc=1, device_id=along(d1, off), device_id_type=MESH)
    for load in loads[4:]:
        load.wait()

    def serve(places):
        views = [at(buf3.at[k], {ORDERS[k][2]: places[k]}) for k in range(3)]
        rows = jnp.concatenate([v[...].reshape(128, model) for v in views], 0)
        hidden = (silu(mm(rows, gate_w[...])) * mm(rows, up_w[...])).astype(BF16)
        for n in range(model // 512):
            cols = slice(512 * n, 512 * n + 512)
            result = mm(hidden, down_w[:, cols]).astype(BF16)
            for k in range(3):
                views[k][:, :, :, cols] = result[128 * k : 128 * k + 128].reshape(4, 4, 8, 512)

    last = [ORDERS[k][2] for k in range(3)]
    serve([coord[d] for d in last])
    for k in range(3):
        pl.semaphore_wait(free_sem.at[0, k], 3)
        start_second(1, k, 0)
    for n in range(3):
        for k in range(3):
            for m in range(4):
                third(0, k, m, n).wait_recv()
        serve([back[d][n] for d in last])
        turned = OFFSETS.index(4 - OFFSETS[n])
        for k in range(3):
            first(1, k, turned).start()
    for n in range(3):
        for k in range(3):
            first(1, k, n).wait_recv()
            start_second(1, k, n + 1)
    for k in range(3):
        pl.semaphore_wait(free_sem.at[1, k], 3)
        start_third(1, k, 0)
    for n in range(3):
        for k in range(3):
            for m in range(4):
                second(1, k, m, n).wait_recv()
            start_third(1, k, n + 1)
    for n in range(3):
        for k in range(3):
            for m in range(4):
                third(1, k, m, n).wait_recv()

    def partial(core, cols):
        rows = pl.ds(pl.multiple_of(core * half, half), half)
        total = mm(pick_s[1, rows, :], buf0[1, :, :, :, :, cols].reshape(8 * chips, 512))
        return total + mm(pick_s[2 * core, rows, :], buf0[2 * core, :, :, :, :, cols].reshape(8 * chips, 512))

    swaps = []
    for n in range(model // 512):
        away_s[n] = partial(1 - c, slice(512 * n, 512 * n + 512))
        swap = pltpu.make_async_remote_copy(
            src_ref=away_s.at[n],
            dst_ref=here_s.at[n],
            send_sem=swap_send.at[n],
            recv_sem=swap_recv.at[n],
            device_id=partner(),
            device_id_type=MESH,
        )
        swap.start()
        swaps.append(swap)
    for n in range(model // 512):
        cols = slice(512 * n, 512 * n + 512)
        acc_s[:, cols] = acc_s[:, cols] + partial(c, cols)
    for n in range(model // 512):
        cols = slice(512 * n, 512 * n + 512)
        swaps[n].wait()
        out_ref[:, cols] = (acc_s[:, cols] + here_s[n]).astype(BF16)

    for k in range(3):
        for m in range(4):
            for n in range(3):
                third(0, k, m, n).wait_send()
                second(1, k, m, n).wait_send()
                third(1, k, m, n).wait_send()
        for n in range(3):
            first(1, k, n).wait_send()


def run_experts(normed, attended, meta, code, gate, up, down, common_gate, common_up, common_down):
    half, model = attended.shape
    buffer = pltpu.VMEM((3, 4, 4, 4, 8, model), BF16)
    hbm = pl.BlockSpec(memory_space=pl.ANY)
    return pl.pallas_call(
        experts_kernel,
        out_shape=jax.ShapeDtypeStruct((half, model), BF16),
        in_specs=[VMEM, hbm, VMEM, VMEM] + [hbm] * 6,
        out_specs=VMEM,
        scratch_shapes=[buffer] * 5
        + [pltpu.VMEM(w.shape, BF16) for w in (gate, up, down, common_gate, common_up, common_down)]
        + [
            pltpu.VMEM((half, model), BF16),
            pltpu.VMEM((3, 2 * half, 512), BF16),
            pltpu.VMEM((half, model), F32),
            pltpu.VMEM((model // 512, half, 512), F32),
            pltpu.VMEM((model // 512, half, 512), F32),
        ]
        + [pltpu.SemaphoreType.DMA((2, 3, 3))] * 2
        + [pltpu.SemaphoreType.DMA((2, 3, 4, 3))] * 4
        + [
            pltpu.SemaphoreType.REGULAR((2, 3)),
            pltpu.SemaphoreType.DMA((model // 512,)),
            pltpu.SemaphoreType.DMA((model // 512,)),
            pltpu.SemaphoreType.DMA((7,)),
        ],
        compiler_params=params(collective_id=1, has_side_effects=True),
        name="experts",
    )(normed, attended, meta, code, gate, up, down, common_gate, common_up, common_down)


def settle_kernel(src_ref, dst_ref, held, in_sem, out_sem):
    step = held.shape[1]
    loads, stores = [], []
    for i in range(held.shape[0]):
        rows = slice(step * i, step * i + step)
        loads.append(pltpu.make_async_copy(src_ref.at[rows], held.at[i], in_sem.at[i]))
        stores.append(pltpu.make_async_copy(held.at[i], dst_ref.at[rows], out_sem.at[i]))
    for load in loads:
        load.start()
    for load, store in zip(loads, stores):
        load.wait()
        store.start()
    for store in stores:
        store.wait()


def settle(out):
    rows, model = out.shape
    hbm = pl.BlockSpec(memory_space=pl.ANY)
    return pl.pallas_call(
        settle_kernel,
        out_shape=jax.ShapeDtypeStruct(out.shape, out.dtype),
        in_specs=[hbm],
        out_specs=hbm,
        scratch_shapes=[
            pltpu.VMEM((4, rows // 4, model), out.dtype),
            pltpu.SemaphoreType.DMA((4,)),
            pltpu.SemaphoreType.DMA((4,)),
        ],
        compiler_params=params(),
        name="settle",
    )(out)


def shards(
    projected_queries,
    projected_keys,
    projected_values,
    output_gate_values,
    write_strength_logits,
    decay_input_logits,
    head_rate_logarithm,
    extra_log_decay,
    per_head_norm_gain,
    output_matrix,
    residual,
    mixture_norm_gain,
    selected_expert_index,
    routing_weight,
    routed_gate_weight,
    routed_up_weight,
    routed_down_weight,
    common_gate_weight,
    common_up_weight,
    common_down_weight,
):
    attended, normed, meta, code = attention(
        projected_queries,
        projected_keys,
        projected_values,
        write_strength_logits.T,
        decay_input_logits.T,
        extra_log_decay.T,
        head_rate_logarithm[None, :],
        output_gate_values,
        per_head_norm_gain[None, :],
        output_matrix,
        residual,
        mixture_norm_gain[None, :],
        selected_expert_index.T,
        routing_weight.T,
    )
    out = run_experts(
        normed,
        attended,
        meta,
        code,
        routed_gate_weight[0],
        routed_up_weight[0],
        routed_down_weight[0],
        common_gate_weight,
        common_up_weight,
        common_down_weight,
    )
    return settle(out)


def solution(mesh):
    finer = Mesh(mesh.devices.reshape(4, 4, 4, mesh.shape["tp"]), AXES)
    in_specs = (
        P(SP, "tp"),
        P(SP, "tp"),
        P(SP, "tp"),
        P(SP, "tp"),
        P(SP, "tp"),
        P(SP, "tp"),
        P("tp"),
        P(SP, "tp"),
        P(),
        P(),
        P(AXES, None),
        P(),
        P(AXES, None),
        P(AXES, None),
        P(AXES, None, None),
        P(AXES, None, None),
        P(AXES, None, None),
        P(),
        P(),
        P(),
    )
    return jax.shard_map(
        shards, mesh=finer, in_specs=in_specs, out_specs=P(AXES, None), check_vma=False
    )
```
